32 devices in a mesh: rep: 2 (over x), fs: 8 (over z, y), tp: 2 (over core).
Axes of the slice: x: 2, y: 2, z: 4, core: 2. Of those that a mesh axis runs over, the one named last changes fastest.
Arguments:
- tokens: bfloat16 [6144, 2048], P(('rep', 'fs'), 'tp'), may hold values from -6 to 6
- mix_gain: float32 [2048], replicated, may hold values from 0.1 to 1.9
- w_u: bfloat16 [2048, 2048], P('fs', 'tp'), may hold values from -0.125 to 0.125
- w_v: bfloat16 [2048, 2048], P('fs', 'tp'), may hold values from -0.125 to 0.125
- norm_gain: float32 [2048], P('tp'), may hold values from 0.1 to 1.9
- mix_weight: bfloat16 [16, 128, 128], P('tp'), may hold values from -0.5 to 0.5
- mix_bias: float32 [16, 128], P('tp'), may hold values from 0.1 to 1.9
- w_mix_out: bfloat16 [2048, 2048], P('tp', 'fs'), may hold values from -0.125 to 0.125
- ffn_gain: float32 [2048], replicated, may hold values from 0.1 to 1.9
- w_gate: bfloat16 [2048, 3072], P('fs', 'tp'), may hold values from -0.125 to 0.125
- w_value: bfloat16 [2048, 3072], P('fs', 'tp'), may hold values from -0.125 to 0.125
- taps_gate: bfloat16 [3, 3072], P(None, 'tp'), may hold values from -3.5 to 3.5
- taps_value: bfloat16 [3, 3072], P(None, 'tp'), may hold values from -3.5 to 3.5
- w_down: bfloat16 [3072, 2048], P('tp', 'fs'), may hold values from -0.109375 to 0.109375
Outputs:
- layer_out: bfloat16 [6144, 2048], P(('rep', 'fs'), 'tp')
The draws below stay inside these ranges and needn't reach their ends.
All inputs are finite; a program needn't handle non-finite values.
Results may differ from the reference program's by a relative error of at most 0.017.
Values may be sent and summed in bfloat16 or wider, within the bound.
A program may use at most 64 MiB of HBM per device.

```python
import jax
import jax.numpy as jnp
from jax import lax

D = 2048
GROUPS = 16
MIX_WIDTH = 2048
FF = 3072
BLOCK = 128
CONV = 3
TOK_DEV = 384
TOKENS = 6144
N_TP = 2


def level_of(rng, extent, split, low, top_value):
    level, own = 1.0, jax.random.fold_in(rng, 6)
    for dim, blocks in split:
        draws = jnp.exp(jax.random.uniform(jax.random.fold_in(own, dim), (blocks,), jnp.float32, low / len(split), top_value / len(split)))
        level = level * jnp.repeat(draws, extent[dim] // blocks).reshape([-1 if axis == dim else 1 for axis in range(len(extent))])
    return level


def scatter_about(own_key, extent, deviation, most, pieces=(), kind=jnp.bfloat16):
    drawn = jax.random.normal(own_key, extent, jnp.float32) * deviation
    if len(pieces) > 0:
        drawn = level_of(own_key, extent, pieces, -0.22, 0.18) * drawn
    return jnp.clip(drawn, min=-most, max=most).astype(kind)


def setup_inputs(seed: int = 0) -> dict:
    key_of = jax.random.split(jax.random.key(seed), 15)
    tokens = scatter_about(key_of[0], (TOKENS, D), 1.0, 6.0, ((0, 16), (1, 2)))
    mix_gain = jnp.clip(1.0 + 0.18 * jax.random.normal(key_of[1], (D,), jnp.float32), 0.1, 1.9)
    w_u = scatter_about(key_of[2], (D, MIX_WIDTH), D ** -0.5, 0.125, ((0, 8), (1, 2)))
    w_v = scatter_about(key_of[3], (D, MIX_WIDTH), D ** -0.5, 0.125, ((0, 8), (1, 2)))
    norm_gain = jnp.clip(1.0 + 0.18 * jax.random.normal(key_of[4], (MIX_WIDTH,), jnp.float32), 0.1, 1.9)
    mix_weight = scatter_about(key_of[5], (GROUPS, BLOCK, BLOCK), BLOCK ** -0.5, 0.5, ((0, 2),))
    mix_bias = jnp.clip(1.0 + 0.18 * jax.random.normal(key_of[6], (GROUPS, BLOCK), jnp.float32), 0.1, 1.9)
    w_mix_out = scatter_about(key_of[7], (MIX_WIDTH, D), MIX_WIDTH ** -0.5, 0.125, ((0, 2), (1, 8)))
    ffn_gain = jnp.clip(1.0 + 0.18 * jax.random.normal(key_of[8], (D,), jnp.float32), 0.1, 1.9)
    w_gate = scatter_about(key_of[9], (D, FF), D ** -0.5, 0.125, ((0, 8), (1, 2)))
    w_value = scatter_about(key_of[10], (D, FF), D ** -0.5, 0.125, ((0, 8), (1, 2)))
    taps_gate = scatter_about(key_of[11], (CONV, FF), CONV ** -0.5, 3.5, ((1, 2),))
    taps_value = scatter_about(key_of[12], (CONV, FF), CONV ** -0.5, 3.5, ((1, 2),))
    w_down = scatter_about(key_of[13], (FF, D), FF ** -0.5, 0.109375, ((0, 2), (1, 8)))
    return {"tokens": tokens, "mix_gain": mix_gain, "w_u": w_u, "w_v": w_v, "norm_gain": norm_gain, "mix_weight": mix_weight, "mix_bias": mix_bias, "w_mix_out": w_mix_out, "ffn_gain": ffn_gain, "w_gate": w_gate, "w_value": w_value, "taps_gate": taps_gate, "taps_value": taps_value, "w_down": w_down}


EPS_RMS = 1e-06
EPS_LN = 1e-05

def rms_scale(features, gain_vec):
    values = features.astype(jnp.float32)
    scaled = values * lax.rsqrt(lax.optimization_barrier(jnp.mean(values * values, axis=-1, keepdims=True)) + EPS_RMS)
    return (scaled * gain_vec).astype(jnp.bfloat16)

def spatial_mix(u_pre, v_pre, norm_gain, mix_weight, mix_bias):
    row_count = u_pre.shape[0]
    groups = mix_weight.shape[0]
    block_len = mix_weight.shape[1]
    group_width = v_pre.shape[1] // groups
    activated = jax.nn.gelu(v_pre).reshape(row_count, groups, group_width)
    average = lax.optimization_barrier(jnp.mean(activated, axis=-1, keepdims=True))
    spread_sq = lax.optimization_barrier(jnp.mean(jnp.square(activated - average), axis=-1, keepdims=True))
    v_norm = ((activated - average) * lax.rsqrt(spread_sq + EPS_LN) * norm_gain.reshape(groups, group_width)).astype(jnp.bfloat16)
    blocks = v_norm.reshape(row_count // block_len, block_len, groups, group_width)
    lower_mask = jnp.arange(block_len)[:, None] >= jnp.arange(block_len)[None, :]
    masked = jnp.where(lower_mask[None], mix_weight, jnp.zeros_like(mix_weight))
    mixed_rows = jnp.einsum('gts,nsgc->ntgc', masked.astype(jnp.float32), blocks.astype(jnp.float32))
    mixed_rows = mixed_rows + jnp.transpose(mix_bias)[None, :, :, None]
    mixed_rows = mixed_rows.reshape(row_count, groups * group_width)
    return (jax.nn.gelu(u_pre) * mixed_rows).astype(jnp.bfloat16)

def causal_taps(values, tap_weights, seq_len):
    row_count, channels = values.shape
    conv_len = tap_weights.shape[0]
    sequences = values.reshape(row_count // seq_len, seq_len, channels)
    padded = jnp.pad(sequences, ((0, 0), (conv_len - 1, 0), (0, 0)))
    summed_terms = jnp.zeros_like(sequences)
    for tap_index in range(conv_len):
        summed_terms = summed_terms + tap_weights[tap_index].astype(jnp.float32) * padded[:, tap_index:tap_index + seq_len]
    return summed_terms.reshape(row_count, channels)

def split_sum(operand, weight):
    share_width = operand.shape[1] // N_TP
    summed_terms = jnp.zeros((operand.shape[0], weight.shape[1]), jnp.float32)
    for member in range(N_TP):
        partial_value = jnp.dot(operand[:, member * share_width:(member + 1) * share_width], weight[member * share_width:(member + 1) * share_width], preferred_element_type=jnp.float32)
        rounded = lax.optimization_barrier(partial_value.astype(jnp.bfloat16))
        summed_terms = summed_terms + rounded.astype(jnp.float32)
    return summed_terms

def reference(tokens, mix_gain, w_u, w_v, norm_gain, mix_weight, mix_bias, w_mix_out, ffn_gain, w_gate, w_value, taps_gate, taps_value, w_down):
    normed = rms_scale(tokens, mix_gain)
    u_pre = jnp.dot(normed, w_u, preferred_element_type=jnp.float32)
    v_pre = jnp.dot(normed, w_v, preferred_element_type=jnp.float32)
    hidden = spatial_mix(u_pre, v_pre, norm_gain, mix_weight, mix_bias)
    middle = (tokens.astype(jnp.float32) + split_sum(hidden, w_mix_out)).astype(jnp.bfloat16)
    normed_mid = rms_scale(middle, ffn_gain)
    gate_pre = jnp.dot(normed_mid, w_gate, preferred_element_type=jnp.float32)
    value_pre = jnp.dot(normed_mid, w_value, preferred_element_type=jnp.float32)
    gate_conv = causal_taps(gate_pre, taps_gate, TOK_DEV)
    value_conv = causal_taps(value_pre, taps_value, TOK_DEV)
    activation = (jax.nn.gelu(gate_conv) * value_conv).astype(jnp.bfloat16)
    return (middle.astype(jnp.float32) + split_sum(activation, w_down)).astype(jnp.bfloat16)
```

```python
import functools

import jax
import jax.numpy as jnp
from jax import lax
from jax.experimental import pallas as pl
from jax.experimental.pallas import tpu as pltpu
from jax.sharding import PartitionSpec as P

EPS_RMS = 1e-06
EPS_LN = 1e-05
F32 = jnp.float32
BF16 = jnp.bfloat16
MESH = pl.DeviceIdType.MESH


def own_half(array, axis):
    share = array.shape[axis] // lax.axis_size("rep")
    return lax.dynamic_slice_in_dim(array, lax.axis_index("rep") * share, share, axis)


def layer_kernel(
    n, nr, nt,
    tok, mix_gain, w_in, norm_gain, mixw, bias, w_out, ffn_gain, w_up, taps_g, taps_v, w_dn,
    out,
    g_in, g_out, g_up, g_dn, feat, feat2, normed, uv, hidden, gv, act, part1, part2, got1, got2,
    w_send, w_recv, w_local, f_send, f_recv, p_send, p_recv,
):
    rep, fs, tp = lax.axis_index("rep"), lax.axis_index("fs"), lax.axis_index("tp")
    seq, own_width = tok.shape
    nz = n // 2
    z, y = fs // 2, fs % 2
    per = n // nt
    depth = normed.shape[2]
    mine = (w_in, w_out, w_up, w_dn)
    gathered = (g_in, g_out, g_up, g_dn)
    offsets = [(a, b) for a in range(nr) for b in range(nt) if (a, b) != (0, 0)]

    def peer(a, b):
        return {"rep": lax.rem(rep + a, nr), "tp": lax.rem(tp + b, nt)}

    barrier = pltpu.get_barrier_semaphore()
    line = (lax.rem(z + 1, nz), lax.rem(z + nz - 1, nz))
    greeted = [{"fs": z * 2 + 1 - y}] + [{"fs": at * 2 + y} for at in line]
    greeted += [peer(a, b) for a, b in offsets]
    for target in greeted:
        pl.semaphore_signal(barrier, inc=1, device_id=target, device_id_type=MESH)
    pl.semaphore_wait(barrier, len(greeted))

    def hop(stage, block, way):
        target = (fs + 2, fs - 2, z * 2 + 1 - y)[way]
        return pltpu.make_async_remote_copy(
            src_ref=gathered[stage].at[block],
            dst_ref=gathered[stage].at[block],
            send_sem=w_send.at[stage, way, block],
            recv_sem=w_recv.at[stage, block],
            device_id={"fs": target},
            device_id_type=MESH,
        )

    def ways(src):
        return (
            jnp.logical_and(src <= z, z < nz - 1),
            jnp.logical_and(src >= z, z > 0),
        )

    def forward(stage, src):
        block = src * 2 + y
        hop(stage, block, 2).start()
        for way, used in enumerate(ways(src)):
            @pl.when(used)
            def _():
                hop(stage, block, way).start()

    def arrived(stage, block):
        hop(stage, block, 2).wait_recv()

    def order(i):
        near = jnp.minimum(z, nz - 1 - z)
        swing = z + ((i + 1) // 2) * (1 - 2 * (i % 2))
        rest = jnp.where(z < nz - 1 - z, i, nz - 1 - i)
        return jnp.where(i <= 2 * near, swing, rest)

    def stage_loop(stage, compute, begin, middle):
        def step(i, _):
            src = order(i)

            @pl.when(i > 0)
            def _():
                arrived(stage, src * 2 + y)
                forward(stage, src)

            compute(src * 2 + y)

            @pl.when(i > 0)
            def _():
                other = order(i - 1) * 2 + 1 - y
                arrived(stage, other)
                compute(other)

            return 0

        lax.fori_loop(begin, nz, step, 0)
        middle()
        last = order(nz - 1) * 2 + 1 - y
        arrived(stage, last)
        compute(last)

    locals_ = [
        pltpu.make_async_copy(mine[k], gathered[k].at[fs], w_local.at[k]) for k in range(4)
    ]
    own_tok = pltpu.make_async_copy(tok, feat.at[rep, tp], w_local.at[4])
    for copy in locals_ + [own_tok]:
        copy.start()

    def share(turn, slabs):
        copies = []
        for k, (a, b) in enumerate(offsets):
            copies.append(
                pltpu.make_async_remote_copy(
                    src_ref=slabs.at[rep, tp],
                    dst_ref=slabs.at[rep, tp],
                    send_sem=f_send.at[turn, k],
                    recv_sem=f_recv.at[turn, k],
                    device_id=peer(a, b),
                    device_id_type=MESH,
                )
            )
        return copies

    def share_wait(turn, slabs):
        for k, (a, b) in enumerate(offsets):
            slab = slabs.at[lax.rem(rep + nr - a, nr), lax.rem(tp + nt - b, nt)]
            pltpu.make_async_remote_copy(
                src_ref=slab, dst_ref=slab, send_sem=f_send.at[turn, k],
                recv_sem=f_recv.at[turn, k], device_id=peer(a, b), device_id_type=MESH,
            ).wait_recv()

    def norm(slabs, gain):
        for r in range(nr):
            total = jnp.zeros((seq, 1), F32)
            for t in range(nt):
                values = slabs[r, t].astype(F32)
                total += jnp.sum(values * values, axis=1, keepdims=True)
            scale = lax.rsqrt(total / (nt * own_width) + EPS_RMS)
            for t in range(nt):
                for j in range(per):
                    values = slabs[r, t, :, j * depth : (j + 1) * depth].astype(F32)
                    normed[t * per + j, r * seq : (r + 1) * seq, :] = (
                        values * scale * gain[t * per + j]
                    ).astype(BF16)

    def piece(turn, part, got, block, r):
        return pltpu.make_async_remote_copy(
            src_ref=part.at[block, r],
            dst_ref=got.at[rep * nt + tp, block % per],
            send_sem=p_send.at[turn, block, r],
            recv_sem=p_recv.at[turn, rep * nt + tp, block % per],
            device_id={"rep": r, "tp": block // per},
            device_id_type=MESH,
        )

    def abroad(block, r):
        return jnp.logical_or(block // per != tp, r != rep)

    def project(turn, left, gathered_w, part, got, block):
        for r in range(nr):
            part[block, r] = jnp.dot(
                left[r], gathered_w[block], preferred_element_type=F32
            ).astype(BF16)

            @pl.when(abroad(block, r))
            def _():
                piece(turn, part, got, block, r).start()

    def collect(turn, part, got, base, emit):
        for j in range(per):
            total = part[tp * per + j, rep].astype(F32)
            for a, b in offsets:
                slot = lax.rem(rep + a, nr) * nt + lax.rem(tp + b, nt)
                landing = got.at[slot, j]
                pltpu.make_async_remote_copy(
                    src_ref=landing, dst_ref=landing, send_sem=p_send.at[turn, 0, 0],
                    recv_sem=p_recv.at[turn, slot, j], device_id=peer(a, b),
                    device_id_type=MESH,
                ).wait_recv()
                total += got[slot, j].astype(F32)
            width = total.shape[1]
            span = slice(j * width, (j + 1) * width)
            emit(span, (base(span).astype(F32) + total).astype(BF16))

    for copy in locals_ + [own_tok]:
        copy.wait()
    for copy in share(0, feat):
        copy.start()
    forward(0, z)
    forward(1, z)
    forward(2, z)
    uv[...] = jnp.zeros_like(uv)
    gv[...] = jnp.zeros_like(gv)
    share_wait(0, feat)
    norm(feat, mix_gain)

    def in_block(block):
        for r in range(nr):
            rows = slice(r * seq, (r + 1) * seq)
            uv[rows, :] += jnp.dot(
                normed[block, rows, :], g_in[block], preferred_element_type=F32
            )

    stage_loop(0, in_block, 0, lambda: forward(3, z))

    groups, block_len = mixw.shape[0], mixw.shape[1]
    group_width = uv.shape[1] // 2 // groups

    for r in range(nr):
        def mix_rows(i, _):
            start = pl.multiple_of(i * block_len, block_len)
            rows = pl.ds(pl.multiple_of(r * seq + i * block_len, block_len), block_len)
            for g in range(groups):
                at = g * group_width
                half = groups * group_width
                activated = jax.nn.gelu(uv[rows, half + at : half + at + group_width])
                centred = activated - jnp.mean(activated, axis=1, keepdims=True)
                spread = jnp.mean(centred * centred, axis=1, keepdims=True)
                v_norm = (
                    centred * lax.rsqrt(spread + EPS_LN) * norm_gain[:, at : at + group_width]
                ).astype(BF16)
                mixed = jnp.dot(mixw[g], v_norm, preferred_element_type=F32) + bias[g]
                hidden[r, pl.ds(start, block_len), at : at + group_width] = (
                    jax.nn.gelu(uv[rows, at : at + group_width]) * mixed
                ).astype(BF16)
            return 0

        lax.fori_loop(0, seq // block_len, mix_rows, 0)

    stage_loop(
        1, functools.partial(project, 0, hidden, g_out, part1, got1), 0, lambda: None
    )

    def relay(stage, begin, end):
        def step(i, _):
            arrived(stage, order(i) * 2 + y)
            forward(stage, order(i))
            return 0

        lax.fori_loop(begin, end, step, 0)

    def put_middle(span, value):
        feat2[rep, tp, :, span] = value

    relay(2, 1, nz // 2)
    collect(0, part1, got1, lambda span: tok[:, span], put_middle)
    for copy in share(1, feat2):
        copy.start()
    relay(2, nz // 2, nz)
    share_wait(1, feat2)
    norm(feat2, ffn_gain)

    def up_block(block):
        for r in range(nr):
            gv[r, 8:, :] += jnp.dot(
                normed[block, r * seq : (r + 1) * seq, :],
                g_up[block],
                preferred_element_type=F32,
            )

    def up_step(i, _):
        up_block(order(i) * 2 + y)

        @pl.when(i > 0)
        def _():
            arrived(3, order(i) * 2 + y)
            forward(3, order(i))

        other = order(i) * 2 + 1 - y
        arrived(2, other)
        up_block(other)
        return 0

    lax.fori_loop(0, nz, up_step, 0)

    units = act.shape[2]
    taps_len = taps_g.shape[0]
    chunk = 128 if units % 128 == 0 else units
    for r in range(nr):
        for at in range(0, units, chunk):
            gate = jnp.zeros((seq, chunk), F32)
            value = jnp.zeros((seq, chunk), F32)
            for k in range(taps_len):
                first = 8 - (taps_len - 1) + k
                gate += taps_g[k : k + 1, at : at + chunk] * gv[r, first : first + seq, at : at + chunk]
                value += (
                    taps_v[k : k + 1, at : at + chunk]
                    * gv[r, first : first + seq, units + at : units + at + chunk]
                )
            act[r, :, at : at + chunk] = (jax.nn.gelu(gate) * value).astype(BF16)

    down = functools.partial(project, 1, act, g_dn, part2, got2)

    def down_own(i, _):
        down(order(i) * 2 + y)
        return 0

    def down_other(i, _):
        arrived(3, order(i) * 2 + 1 - y)
        down(order(i) * 2 + 1 - y)
        return 0

    lax.fori_loop(0, nz, down_own, 0)
    lax.fori_loop(0, nz, down_other, 0)

    def put_out(span, value):
        out[:, span] = value

    collect(1, part2, got2, lambda span: feat2[rep, tp, :, span], put_out)

    for turn, slabs in enumerate((feat, feat2)):
        for copy in share(turn, slabs):
            copy.wait_send()

    def drain_pieces(block, _):
        for r in range(nr):
            @pl.when(abroad(block, r))
            def _():
                piece(0, part1, got1, block, r).wait_send()
                piece(1, part2, got2, block, r).wait_send()
        return 0

    lax.fori_loop(0, n, drain_pieces, 0)

    def drain_hops(src, _):
        for stage in range(4):
            hop(stage, src * 2 + y, 2).wait_send()
            for way, used in enumerate(ways(src)):
                @pl.when(used)
                def _():
                    hop(stage, src * 2 + y, way).wait_send()
        return 0

    lax.fori_loop(0, nz, drain_hops, 0)


def on_device(
    tokens,
    mix_gain,
    w_u,
    w_v,
    norm_gain,
    mix_weight,
    mix_bias,
    w_mix_out,
    ffn_gain,
    w_gate,
    w_value,
    taps_gate,
    taps_value,
    w_down,
):
    n, nr, nt = lax.axis_size("fs"), lax.axis_size("rep"), lax.axis_size("tp")
    seq, own_width = tokens.shape
    depth, per = own_width * nt // n, n // nt
    block_len = mix_weight.shape[1]
    lower_mask = jnp.arange(block_len)[:, None] >= jnp.arange(block_len)[None, :]
    mixw = own_half(mix_weight, 0)
    mixw = jnp.where(lower_mask[None], mixw, jnp.zeros_like(mixw))
    w_in = jnp.concatenate((own_half(w_u, 1), own_half(w_v, 1)), 1)
    w_up = jnp.concatenate((own_half(w_gate, 1), own_half(w_value, 1)), 1)
    w_out, w_dn = own_half(w_mix_out, 0), own_half(w_down, 0)
    operands = (
        tokens,
        mix_gain.reshape(n, 1, depth),
        w_in,
        own_half(norm_gain, 0)[None, :],
        mixw,
        own_half(mix_bias, 0)[:, :, None],
        w_out,
        ffn_gain.reshape(n, 1, depth),
        w_up,
        own_half(taps_gate, 1).astype(F32),
        own_half(taps_value, 1).astype(F32),
        w_dn,
    )
    vmem, sem = pltpu.VMEM, pltpu.SemaphoreType.DMA
    others = nr * nt - 1
    return pl.pallas_call(
        functools.partial(layer_kernel, n, nr, nt),
        out_shape=jax.ShapeDtypeStruct((seq, own_width), BF16),
        in_specs=[pl.BlockSpec(memory_space=vmem)] * len(operands),
        out_specs=pl.BlockSpec(memory_space=vmem),
        scratch_shapes=[
            vmem((n,) + w_in.shape, BF16),
            vmem((n,) + w_out.shape, BF16),
            vmem((n,) + w_up.shape, BF16),
            vmem((n,) + w_dn.shape, BF16),
            vmem((nr, nt, seq, own_width), BF16),
            vmem((nr, nt, seq, own_width), BF16),
            vmem((n, nr * seq, depth), BF16),
            vmem((nr * seq, w_in.shape[1]), F32),
            vmem((nr, seq, w_out.shape[0]), BF16),
            vmem((nr, seq + 8, w_up.shape[1]), F32),
            vmem((nr, seq, w_dn.shape[0]), BF16),
            vmem((n, nr, seq, depth), BF16),
            vmem((n, nr, seq, depth), BF16),
            vmem((nr * nt, per, seq, depth), BF16),
            vmem((nr * nt, per, seq, depth), BF16),
            sem((4, 3, n)),
            sem((4, n)),
            sem((5,)),
            sem((2, others)),
            sem((2, others)),
            sem((2, n, nr)),
            sem((2, nr * nt, per)),
        ],
        compiler_params=pltpu.CompilerParams(
            collective_id=0, has_side_effects=True, vmem_limit_bytes=67043328
        ),
    )(*operands)


def plane_kernel(
    n, nr, nt,
    tok, mix_gain, w_u, w_v, norm_gain, mixw, bias, w_out, ffn_gain, w_gate, w_value, taps_g, taps_v, w_dn,
    out,
    g_in, g_out, g_up, g_dn, feat, feat2, mid, normed, uv, hidden, gv, act,
    part1, part2, inc1, inc2, got1, got2, raw_mix, mix_low, gain_v, bias_all, bias_col, tg, tv,
    l_sem, y_send, y_recv, z_send, z_recv, d_send, d_recv, s_local, s_send, s_recv,
    a_send, a_recv, f_send, r_send, i_recv, t_recv,
):
    rep, fs, tp = lax.axis_index("rep"), lax.axis_index("fs"), lax.axis_index("tp")
    seq, own_width = tok.shape
    ny, nz = 2, n // 2
    z, y = fs // ny, fs % ny
    per = n // nt
    width = own_width // per
    quarter = rep * ny + y
    other_quarter = rep * ny + 1 - y
    fs_y = z * ny + 1 - y
    home = rep == tp
    away = rep != tp
    cu, cf = g_out.shape[2], g_dn.shape[2]
    mid_rows = (tok, mid)
    feats = (feat, feat2)

    barrier = pltpu.get_barrier_semaphore()
    greeted = [{"tp": 1 - tp}]
    greeted += [{"rep": 1 - rep, "tp": t} for t in range(nt)]
    greeted += [{"fs": fs_y, "tp": t} for t in range(nt)]
    greeted += [{"fs": lax.rem(z + k, nz) * ny + y} for k in range(1, nz)]

    def item(k, block, half):
        if k == 0:
            return g_in.at[half, block]
        if k == 1:
            return g_out.at[block, half]
        if k == 2:
            return g_up.at[half, block]
        return g_dn.at[block, half]

    def pieces(k, which, block):
        whole = item(k, block, tp)
        if k in (0, 2):
            first, second, size = (w_u, w_v, cu) if k == 0 else (w_gate, w_value, cf)
            cols = pl.ds(pl.multiple_of(which * size, 128), size)
            return (
                (first.at[:, cols], whole.at[:, pl.ds(0, size)]),
                (second.at[:, cols], whole.at[:, pl.ds(size, size)]),
            )
        source, size = (w_out, cu) if k == 1 else (w_dn, cf)
        rows = pl.ds(pl.multiple_of(which * size, 128), size)
        return ((source.at[rows, :], whole),)

    def own_load(k):
        return [
            pltpu.make_async_copy(src, dst, l_sem.at[k, i])
            for i, (src, dst) in enumerate(pieces(k, quarter, fs))
        ]

    def across(k, block):
        return [
            pltpu.make_async_remote_copy(
                src_ref=src, dst_ref=dst, send_sem=y_send.at[k, i], recv_sem=y_recv.at[k, i],
                device_id={"fs": fs_y}, device_id_type=MESH,
            )
            for i, (src, dst) in enumerate(pieces(k, other_quarter, block))
        ]

    def z_copy(k, block, step):
        return pltpu.make_async_remote_copy(
            src_ref=item(k, block, tp), dst_ref=item(k, block, tp),
            send_sem=z_send.at[k, block, step + 2], recv_sem=z_recv.at[k, block],
            device_id={"fs": fs + ny * step}, device_id_type=MESH,
        )

    def d_copy(k, block):
        return pltpu.make_async_remote_copy(
            src_ref=item(k, block, tp), dst_ref=item(k, block, tp),
            send_sem=d_send.at[k, block], recv_sem=d_recv.at[k, block],
            device_id={"tp": 1 - tp}, device_id_type=MESH,
        )

    def inside(step):
        return jnp.logical_and(z + step >= 0, z + step < nz)

    def spread(k, block):
        for step in (2, -2, 1, -1):
            @pl.when(inside(step))
            def _():
                z_copy(k, block, step).start()
        d_copy(k, block).start()

    def arrive(k, block):
        landing = item(k, block, tp)
        pltpu.make_async_remote_copy(
            src_ref=landing, dst_ref=landing, send_sem=z_send.at[k, block, 2],
            recv_sem=z_recv.at[k, block], device_id={"tp": 1 - tp}, device_id_type=MESH,
        ).wait_recv()
        d_copy(k, block).start()

    def cross_over(k):
        for copy in across(k, fs_y):
            copy.wait_recv()
        spread(k, fs_y)

    def relays():
        return [
            (sign, z - sign * far, jnp.logical_and(inside(sign), inside(-sign * far)))
            for sign in (1, -1)
            for far in range(2, nz)
        ]

    def relay(k):
        for at in range(ny):
            for sign, source, used in relays():
                @pl.when(used)
                def _():
                    arrive(k, source * ny + at)
                    z_copy(k, source * ny + at, sign).start()

    def relayed(source):
        up = jnp.logical_and(z - source >= 2, inside(1))
        down = jnp.logical_and(source - z >= 2, inside(-1))
        return jnp.logical_or(up, down)

    def need(k, block):
        source = block // ny
        @pl.when(jnp.logical_and(source != z, jnp.logical_not(relayed(source))))
        def _():
            arrive(k, block)

    def partner_wait(k, block):
        landing = item(k, block, 1 - tp)
        pltpu.make_async_remote_copy(
            src_ref=landing, dst_ref=landing, send_sem=d_send.at[k, block],
            recv_sem=d_recv.at[k, block], device_id={"tp": 1 - tp}, device_id_type=MESH,
        ).wait_recv()

    def order(i):
        near = jnp.minimum(z, nz - 1 - z)
        swing = z + ((i + 1) // 2) * (1 - 2 * (i % 2))
        rest = jnp.where(z < nz - 1 - z, i, nz - 1 - i)
        return jnp.where(i <= 2 * near, swing, rest)

    def near_block(i):
        return order(i // ny) * ny + lax.rem(y + i, ny)

    def plain_block(i):
        return order(i // ny) * ny + lax.rem(i, ny)

    small = [
        (mixw.at[pl.ds(quarter * raw_mix.shape[1], raw_mix.shape[1])], raw_mix.at[tp]),
        (norm_gain.at[:, pl.ds(pl.multiple_of(quarter * cu, 128), cu)], gain_v.at[tp]),
        (bias, bias_all.at[tp]),
        (taps_g.at[:, pl.ds(pl.multiple_of(quarter * cf, 128), cf)], tg.at[tp]),
        (taps_v.at[:, pl.ds(pl.multiple_of(quarter * cf, 128), cf)], tv.at[tp]),
    ]
    small_local = [
        pltpu.make_async_copy(src, dst, s_local.at[i]) for i, (src, dst) in enumerate(small)
    ]
    small_away = [
        pltpu.make_async_remote_copy(
            src_ref=src, dst_ref=dst, send_sem=s_send.at[i], recv_sem=s_recv.at[i],
            device_id={"tp": 1 - tp}, device_id_type=MESH,
        )
        for i, (src, dst) in enumerate(small)
    ]

    def ag_source(turn, i):
        if turn == 0:
            return tok.at[:, pl.ds(pl.multiple_of(i * width, 128), width)]
        return mid.at[i]

    def ag_copy(turn, i, way):
        block = tp * per + i
        device = ({"rep": 1 - rep, "tp": rep}, {"fs": fs_y, "tp": rep}, {"tp": 1 - tp})[way]
        return pltpu.make_async_remote_copy(
            src_ref=ag_source(turn, i), dst_ref=feats[turn].at[y, block],
            send_sem=a_send.at[turn, way, i], recv_sem=a_recv.at[turn, y, block],
            device_id=device, device_id_type=MESH,
        )

    def ag_send(turn, i):
        ag_copy(turn, i, 0).start()
        ag_copy(turn, i, 1).start()

        @pl.when(away)
        def _():
            ag_copy(turn, i, 2).start()

        @pl.when(home)
        def _():
            feats[turn][y, tp * per + i] = ag_source(turn, i)[...]

    def ag_pass(turn, i):
        slot = jnp.where(home, 1 - y, y)
        block = jnp.where(home, (nt - 1) * per, 0) + i
        return pltpu.make_async_remote_copy(
            src_ref=feats[turn].at[slot, block], dst_ref=feats[turn].at[slot, block],
            send_sem=f_send.at[turn, i], recv_sem=a_recv.at[turn, slot, block],
            device_id={
                "rep": jnp.where(home, 1 - rep, rep),
                "fs": jnp.where(home, fs, fs_y),
            },
            device_id_type=MESH,
        )

    def ag_landed(turn, slot, block):
        landing = feats[turn].at[slot, block]
        pltpu.make_async_remote_copy(
            src_ref=landing, dst_ref=landing, send_sem=f_send.at[turn, 0],
            recv_sem=a_recv.at[turn, slot, block], device_id={"tp": 1 - tp}, device_id_type=MESH,
        ).wait_recv()

    def ag_forward(turn):
        def step(i, _):
            slot = jnp.where(home, 1 - y, y)
            ag_landed(turn, slot, jnp.where(home, (nt - 1) * per, 0) + i)
            ag_pass(turn, i).start()
            return 0

        lax.fori_loop(0, per, step, 0)

    def ag_wait(turn, slot):
        def step(block, _):
            half = block // per
            local = jnp.logical_and(home, jnp.logical_and(slot == y, half == tp))
            passed_home = jnp.logical_and(home, jnp.logical_and(slot != y, half == nt - 1))
            passed_away = jnp.logical_and(away, jnp.logical_and(slot == y, half == 0))
            done = jnp.logical_or(local, jnp.logical_or(passed_home, passed_away))

            @pl.when(jnp.logical_not(done))
            def _():
                ag_landed(turn, slot, block)

            return 0

        lax.fori_loop(0, n, step, 0)

    def norm(turn, slot, gain):
        slabs = feats[turn]

        def add(block, total):
            values = slabs[slot, block].astype(F32)
            return total + jnp.sum(values * values, axis=1, keepdims=True)

        total = lax.fori_loop(0, n, add, jnp.zeros((seq, 1), F32))
        scale = lax.rsqrt(total / (n * width) + EPS_RMS)

        def put(block, _):
            values = slabs[slot, block].astype(F32)
            cols = pl.ds(pl.multiple_of(block * width, 128), width)
            normed[block, slot] = (values * scale * gain[:, cols]).astype(BF16)
            return 0

        lax.fori_loop(0, n, put, 0)

    def gathered_loop(k, multiply):
        def step(i, _):
            block = near_block(i)
            need(k, block)
            multiply(block, tp)

            @pl.when(i > 0)
            def _():
                before = near_block(i - 1)
                partner_wait(k, before)
                multiply(before, 1 - tp)

            return 0

        lax.fori_loop(0, n, step, 0)
        last = near_block(n - 1)
        partner_wait(k, last)
        multiply(last, 1 - tp)

    def even(block):
        return lax.rem(block, 2) == 0

    def both(*conditions):
        return functools.reduce(jnp.logical_and, conditions)

    parts, incs, gots = (part1, part2), (inc1, inc2), (got1, got2)

    def r_copy(turn, r, block, kind):
        slot = lax.rem(y + r, 2)
        core, at = block // per, lax.rem(block, per)
        got, inc = gots[turn], incs[turn]
        dst, sem, device = {
            "diag_x": (inc.at[block], i_recv.at[turn, block], {"rep": 1 - rep}),
            "diag_y": (inc.at[block], i_recv.at[turn, block], {"fs": fs_y}),
            "pair": (got.at[0, at], t_recv.at[turn, 0, at], {"tp": 1 - tp}),
            "x": (got.at[1, at], t_recv.at[turn, 1, at], {"rep": 1 - rep, "tp": core}),
            "y": (got.at[2, at], t_recv.at[turn, 2, at], {"fs": fs_y, "tp": core}),
        }[kind]
        return pltpu.make_async_remote_copy(
            src_ref=parts[turn].at[slot, block], dst_ref=dst, send_sem=r_send.at[turn, r, block],
            recv_sem=sem, device_id=device, device_id_type=MESH,
        )

    def cases(block):
        return (
            (1, "diag_x", both(away, even(block)), True),
            (1, "diag_y", both(away, jnp.logical_not(even(block))), True),
            (1, "y", both(home, jnp.logical_not(even(block))), True),
            (0, "pair", both(home, block // per != tp), True),
            (0, "x", both(away, even(block)), True),
            (1, "y", both(home, even(block)), False),
            (0, "x", both(away, jnp.logical_not(even(block))), False),
        )

    def project(turn, left, weight, block):
        size = weight.shape[1] * weight.shape[2]
        right = weight[block].reshape(size, weight.shape[3])
        for r in (1, 0):
            slot = lax.rem(y + r, 2)
            parts[turn][slot, block] = jnp.dot(
                left[slot], right, preferred_element_type=F32
            ).astype(BF16)
            for row, kind, used, now in cases(block):
                if row == r and now:
                    @pl.when(used)
                    def _():
                        r_copy(turn, r, block, kind).start()

        @pl.when(both(home, block // per == tp))
        def _():
            gots[turn][0, lax.rem(block, per)] = parts[turn][y, block]

    def join(turn, block):
        for r, kind, used, now in cases(block):
            if not now:
                @pl.when(used)
                def _():
                    landing = incs[turn].at[block]
                    pltpu.make_async_remote_copy(
                        src_ref=landing, dst_ref=landing, send_sem=r_send.at[turn, 0, 0],
                        recv_sem=i_recv.at[turn, block], device_id={"rep": 1 - rep},
                        device_id_type=MESH,
                    ).wait_recv()
                    slot = lax.rem(y + r, 2)
                    parts[turn][slot, block] = (
                        parts[turn][slot, block].astype(F32) + incs[turn][block].astype(F32)
                    ).astype(BF16)
                    r_copy(turn, r, block, kind).start()

    def landed(turn, kind, at):
        landing = gots[turn].at[kind, at]
        pltpu.make_async_remote_copy(
            src_ref=landing, dst_ref=landing, send_sem=r_send.at[turn, 0, 0],
            recv_sem=t_recv.at[turn, kind, at], device_id={"rep": 1 - rep}, device_id_type=MESH,
        ).wait_recv()

    def collect(turn, block):
        at = lax.rem(block, per)

        @pl.when(away)
        def _():
            landed(turn, 0, at)

        landed(turn, 1, at)
        landed(turn, 2, at)
        got = gots[turn]
        total = got[0, at].astype(F32) + got[1, at].astype(F32) + got[2, at].astype(F32)
        cols = pl.ds(pl.multiple_of(at * width, 128), width)
        if turn == 0:
            mid[at] = (tok[:, cols].astype(F32) + total).astype(BF16)
            ag_send(1, at)
        else:
            out[:, cols] = (mid[at].astype(F32) + total).astype(BF16)

    def scatter_loop(k, turn, left, weight):
        def step(i, _):
            @pl.when(i < n)
            def _():
                need(k, plain_block(i))

            @pl.when(both(i >= 1, i < n + 1))
            def _():
                block = plain_block(i - 1)
                partner_wait(k, block)
                project(turn, left, weight, block)

            @pl.when(both(i >= 3, i < n + 3))
            def _():
                join(turn, plain_block(i - 3))

            @pl.when(i >= 5)
            def _():
                block = plain_block(i - 5)

                @pl.when(block // per == tp)
                def _():
                    collect(turn, block)

            return 0

        lax.fori_loop(0, n + 5, step, 0)

    for k in range(4):
        for copy in own_load(k):
            copy.start()
    for copy in small_local:
        copy.start()
    for target in greeted:
        pl.semaphore_signal(barrier, inc=1, device_id=target, device_id_type=MESH)
    pl.semaphore_wait(barrier, len(greeted))

    for copy in across(0, fs):
        copy.start()
    for i in range(per):
        ag_send(0, i)
    for k in range(2):
        for copy in own_load(k):
            copy.wait()
        spread(k, fs)
    for copy in across(1, fs) + small_away:
        copy.start()
    cross_over(0)
    for k in (2, 3):
        for copy in own_load(k):
            copy.wait()
    ag_forward(0)
    cross_over(1)
    for k in (2, 3):
        for copy in across(k, fs):
            copy.start()
    uv[...] = jnp.zeros_like(uv)
    gv[...] = jnp.zeros_like(gv)
    relay(0)
    for r in range(2):
        slot = lax.rem(y + r, 2)
        ag_wait(0, slot)
        norm(0, slot, mix_gain)
    spread(2, fs)

    def in_block(block, half):
        for slot in range(2):
            uv[half, slot] += jnp.dot(
                normed[block, slot], g_in[half, block], preferred_element_type=F32
            )

    gathered_loop(0, in_block)
    relay(1)
    cross_over(2)

    for copy in small_local:
        copy.wait()
    for i, (_, dst) in enumerate(small):
        landing = (raw_mix, gain_v, bias_all, tg, tv)[i].at[1 - tp]
        pltpu.make_async_remote_copy(
            src_ref=landing, dst_ref=landing, send_sem=s_send.at[i], recv_sem=s_recv.at[i],
            device_id={"tp": 1 - tp}, device_id_type=MESH,
        ).wait_recv()
    per_half, block_len = raw_mix.shape[1], raw_mix.shape[2]
    group_width = cu // per_half
    at_row = lax.broadcasted_iota(jnp.int32, (block_len, block_len), 0)
    at_col = lax.broadcasted_iota(jnp.int32, (block_len, block_len), 1)
    for half in range(nt):
        turned = bias_all[half].T
        lane = lax.broadcasted_iota(jnp.int32, turned.shape, 1)
        for g in range(per_half):
            mix_low[half, g] = jnp.where(
                at_row >= at_col, raw_mix[half, g].astype(F32), 0.0
            ).astype(BF16)
            bias_col[half, g] = jnp.sum(
                jnp.where(lane == quarter * per_half + g, turned, 0.0), axis=1, keepdims=True
            )

    for slot in range(2):
        def mix_rows(i, _):
            rows = pl.ds(pl.multiple_of(i * block_len, block_len), block_len)
            for half in range(nt):
                for g in range(per_half):
                    at = g * group_width
                    activated = jax.nn.gelu(uv[half, slot, rows, cu + at : cu + at + group_width])
                    centred = activated - jnp.mean(activated, axis=1, keepdims=True)
                    spread_sq = jnp.mean(centred * centred, axis=1, keepdims=True)
                    v_norm = (
                        centred
                        * lax.rsqrt(spread_sq + EPS_LN)
                        * gain_v[half, :, at : at + group_width]
                    ).astype(BF16)
                    mixed = (
                        jnp.dot(mix_low[half, g], v_norm, preferred_element_type=F32)
                        + bias_col[half, g]
                    )
                    hidden[slot, rows, half * cu + at : half * cu + at + group_width] = (
                        jax.nn.gelu(uv[half, slot, rows, at : at + group_width]) * mixed
                    ).astype(BF16)
            return 0

        lax.fori_loop(0, seq // block_len, mix_rows, 0)

    scatter_loop(1, 0, hidden, g_out)
    relay(2)
    spread(3, fs)
    cross_over(3)
    ag_forward(1)
    for r in range(2):
        slot = lax.rem(y + r, 2)
        ag_wait(1, slot)
        norm(1, slot, ffn_gain)
    relay(3)

    def up_block(block, half):
        for slot in range(2):
            gv[half, slot, 8:, :] += jnp.dot(
                normed[block, slot], g_up[half, block], preferred_element_type=F32
            )

    gathered_loop(2, up_block)

    taps_len = tg.shape[1]
    chunk = 128
    for slot in range(2):
        for half in range(nt):
            for at in range(0, cf, chunk):
                gate = jnp.zeros((seq, chunk), F32)
                value = jnp.zeros((seq, chunk), F32)
                for k in range(taps_len):
                    first = 8 - (taps_len - 1) + k
                    rows = slice(first, first + seq)
                    gate += tg[half, k : k + 1, at : at + chunk].astype(F32) * gv[
                        half, slot, rows, at : at + chunk
                    ]
                    value += tv[half, k : k + 1, at : at + chunk].astype(F32) * gv[
                        half, slot, rows, cf + at : cf + at + chunk
                    ]
                act[slot, :, half * cf + at : half * cf + at + chunk] = (
                    jax.nn.gelu(gate) * value
                ).astype(BF16)

    scatter_loop(3, 1, act, g_dn)

    for k in range(4):
        for copy in across(k, fs):
            copy.wait_send()
    for copy in small_away:
        copy.wait_send()

    def drain_block(block, _):
        for k in range(4):
            d_copy(k, block).wait_send()
        for turn in range(2):
            for r, kind, used, _now in cases(block):
                @pl.when(used)
                def _():
                    r_copy(turn, r, block, kind).wait_send()
        return 0

    lax.fori_loop(0, n, drain_block, 0)

    def drain_gather(i, _):
        for turn in range(2):
            ag_copy(turn, i, 0).wait_send()
            ag_copy(turn, i, 1).wait_send()
            ag_pass(turn, i).wait_send()

            @pl.when(away)
            def _():
                ag_copy(turn, i, 2).wait_send()
        return 0

    lax.fori_loop(0, per, drain_gather, 0)

    def drain_line(at, _):
        for k in range(4):
            for step in (2, -2, 1, -1):
                @pl.when(inside(step))
                def _():
                    z_copy(k, z * ny + at, step).wait_send()
            for sign, source, used in relays():
                @pl.when(used)
                def _():
                    z_copy(k, source * ny + at, sign).wait_send()
        return 0

    lax.fori_loop(0, ny, drain_line, 0)


def on_plane(
    tokens,
    mix_gain,
    w_u,
    w_v,
    norm_gain,
    mix_weight,
    mix_bias,
    w_mix_out,
    ffn_gain,
    w_gate,
    w_value,
    taps_gate,
    taps_value,
    w_down,
):
    n, nr, nt = lax.axis_size("fs"), lax.axis_size("rep"), lax.axis_size("tp")
    seq, own_width = tokens.shape
    per = n // nt
    width = own_width // per
    depth = w_u.shape[0]
    share = nr * 2
    cu, cf = w_u.shape[1] // share, w_gate.shape[1] // share
    groups, block_len = mix_weight.shape[0], mix_weight.shape[1]
    taps_len = taps_gate.shape[0]
    vmem, sem, hbm = pltpu.VMEM, pltpu.SemaphoreType.DMA, pl.ANY
    operands = (
        (tokens, vmem),
        (mix_gain[None, :], vmem),
        (w_u, hbm),
        (w_v, hbm),
        (norm_gain[None, :], hbm),
        (mix_weight, hbm),
        (mix_bias, hbm),
        (w_mix_out, hbm),
        (ffn_gain[None, :], vmem),
        (w_gate, hbm),
        (w_value, hbm),
        (taps_gate, hbm),
        (taps_value, hbm),
        (w_down, hbm),
    )
    return pl.pallas_call(
        functools.partial(plane_kernel, n, nr, nt),
        out_shape=jax.ShapeDtypeStruct((seq, own_width), BF16),
        in_specs=[pl.BlockSpec(memory_space=space) for _, space in operands],
        out_specs=pl.BlockSpec(memory_space=vmem),
        scratch_shapes=[
            vmem((nt, n, depth, 2 * cu), BF16),
            vmem((n, nt, cu, width), BF16),
            vmem((nt, n, depth, 2 * cf), BF16),
            vmem((n, nt, cf, width), BF16),
            vmem((2, n, seq, width), BF16),
            vmem((2, n, seq, width), BF16),
            vmem((per, seq, width), BF16),
            vmem((n, 2, seq, width), BF16),
            vmem((nt, 2, seq, 2 * cu), F32),
            vmem((2, seq, nt * cu), BF16),
            vmem((nt, 2, seq + 8, 2 * cf), F32),
            vmem((2, seq, nt * cf), BF16),
            vmem((2, n, seq, width), BF16),
            vmem((2, n, seq, width), BF16),
            vmem((n, seq, width), BF16),
            vmem((n, seq, width), BF16),
            vmem((3, per, seq, width), BF16),
            vmem((3, per, seq, width), BF16),
            vmem((nt, groups // share, block_len, block_len), BF16),
            vmem((nt, groups // share, block_len, block_len), BF16),
            vmem((nt, 1, cu), F32),
            vmem((nt, groups, block_len), F32),
            vmem((nt, groups // share, block_len, 1), F32),
            vmem((nt, taps_len, cf), BF16),
            vmem((nt, taps_len, cf), BF16),
            sem((4, 2)),
            sem((4, 2)),
            sem((4, 2)),
            sem((4, n, 5)),
            sem((4, n)),
            sem((4, n)),
            sem((4, n)),
            sem((5,)),
            sem((5,)),
            sem((5,)),
            sem((2, 3, per)),
            sem((2, 2, n)),
            sem((2, per)),
            sem((2, 2, n)),
            sem((2, n)),
            sem((2, 3, per)),
        ],
        compiler_params=pltpu.CompilerParams(
            collective_id=0, has_side_effects=True, vmem_limit_bytes=67043328
        ),
    )(*(array for array, _ in operands))


def by_shape(*arrays):
    n, nr, nt = lax.axis_size("fs"), lax.axis_size("rep"), lax.axis_size("tp")
    groups, units = arrays[5].shape[0], arrays[9].shape[1]
    share = nr * 2
    fits = nr == 2 and nt == 2 and n % 2 == 0 and groups % share == 0 and units % (share * 128) == 0
    return on_plane(*arrays) if fits else on_device(*arrays)


def solution(mesh):
    placed = (
        P(("rep", "fs"), "tp"),
        P(),
        P("fs", "tp"),
        P("fs", "tp"),
        P("tp"),
        P("tp", None, None),
        P("tp", None),
        P("tp", "fs"),
        P(),
        P("fs", "tp"),
        P("fs", "tp"),
        P(None, "tp"),
        P(None, "tp"),
        P("tp", "fs"),
    )
    return jax.shard_map(
        by_shape, mesh=mesh, in_specs=placed, out_specs=P(("rep", "fs"), "tp"), check_vma=False
    )
```

```python
import functools

import jax
import jax.numpy as jnp
from jax import lax
from jax.experimental import pallas as pl
from jax.experimental.pallas import tpu as pltpu
from jax.sharding import PartitionSpec as P

EPS_RMS = 1e-06
EPS_LN = 1e-05
F32 = jnp.float32
BF16 = jnp.bfloat16
MESH = pl.DeviceIdType.MESH


def own_half(array, axis):
    share = array.shape[axis] // lax.axis_size("rep")
    return lax.dynamic_slice_in_dim(array, lax.axis_index("rep") * share, share, axis)


def layer_kernel(
    n, nr, nt,
    tok, mix_gain, w_in, norm_gain, mixw, bias, w_out, ffn_gain, w_up, taps_g, taps_v, w_dn,
    out,
    g_in, g_out, g_up, g_dn, feat, feat2, normed, uv, hidden, gv, act, part1, part2, got1, got2,
    w_send, w_recv, w_local, f_send, f_recv, p_send, p_recv,
):
    rep, fs, tp = lax.axis_index("rep"), lax.axis_index("fs"), lax.axis_index("tp")
    seq, own_width = tok.shape
    nz = n // 2
    z, y = fs // 2, fs % 2
    per = n // nt
    depth = normed.shape[2]
    mine = (w_in, w_out, w_up, w_dn)
    gathered = (g_in, g_out, g_up, g_dn)
    offsets = [(a, b) for a in range(nr) for b in range(nt) if (a, b) != (0, 0)]

    def peer(a, b):
        return {"rep": lax.rem(rep + a, nr), "tp": lax.rem(tp + b, nt)}

    barrier = pltpu.get_barrier_semaphore()
    line = (lax.rem(z + 1, nz), lax.rem(z + nz - 1, nz))
    greeted = [{"fs": z * 2 + 1 - y}] + [{"fs": at * 2 + y} for at in line]
    greeted += [peer(a, b) for a, b in offsets]
    for target in greeted:
        pl.semaphore_signal(barrier, inc=1, device_id=target, device_id_type=MESH)
    pl.semaphore_wait(barrier, len(greeted))

    def hop(stage, block, way):
        target = (fs + 2, fs - 2, z * 2 + 1 - y)[way]
        return pltpu.make_async_remote_copy(
            src_ref=gathered[stage].at[block],
            dst_ref=gathered[stage].at[block],
            send_sem=w_send.at[stage, way, block],
            recv_sem=w_recv.at[stage, block],
            device_id={"fs": target},
            device_id_type=MESH,
        )

    def ways(src):
        return (
            jnp.logical_and(src <= z, z < nz - 1),
            jnp.logical_and(src >= z, z > 0),
        )

    def forward(stage, src):
        block = src * 2 + y
        hop(stage, block, 2).start()
        for way, used in enumerate(ways(src)):
            @pl.when(used)
            def _():
                hop(stage, block, way).start()

    def arrived(stage, block):
        hop(stage, block, 2).wait_recv()

    def order(i):
        near = jnp.minimum(z, nz - 1 - z)
        swing = z + ((i + 1) // 2) * (1 - 2 * (i % 2))
        rest = jnp.where(z < nz - 1 - z, i, nz - 1 - i)
        return jnp.where(i <= 2 * near, swing, rest)

    def stage_loop(stage, compute, begin, middle):
        def step(i, _):
            src = order(i)

            @pl.when(i > 0)
            def _():
                arrived(stage, src * 2 + y)
                forward(stage, src)

            compute(src * 2 + y)

            @pl.when(i > 0)
            def _():
                other = order(i - 1) * 2 + 1 - y
                arrived(stage, other)
                compute(other)

            return 0

        lax.fori_loop(begin, nz, step, 0)
        middle()
        last = order(nz - 1) * 2 + 1 - y
        arrived(stage, last)
        compute(last)

    locals_ = [
        pltpu.make_async_copy(mine[k], gathered[k].at[fs], w_local.at[k]) for k in range(4)
    ]
    own_tok = pltpu.make_async_copy(tok, feat.at[rep, tp], w_local.at[4])
    for copy in locals_ + [own_tok]:
        copy.start()

    def share(turn, slabs):
        copies = []
        for k, (a, b) in enumerate(offsets):
            copies.append(
                pltpu.make_async_remote_copy(
                    src_ref=slabs.at[rep, tp],
                    dst_ref=slabs.at[rep, tp],
                    send_sem=f_send.at[turn, k],
                    recv_sem=f_recv.at[turn, k],
                    device_id=peer(a, b),
                    device_id_type=MESH,
                )
            )
        return copies

    def share_wait(turn, slabs):
        for k, (a, b) in enumerate(offsets):
            slab = slabs.at[lax.rem(rep + nr - a, nr), lax.rem(tp + nt - b, nt)]
            pltpu.make_async_remote_copy(
                src_ref=slab, dst_ref=slab, send_sem=f_send.at[turn, k],
                recv_sem=f_recv.at[turn, k], device_id=peer(a, b), device_id_type=MESH,
            ).wait_recv()

    def norm(slabs, gain):
        for r in range(nr):
            total = jnp.zeros((seq, 1), F32)
            for t in range(nt):
                values = slabs[r, t].astype(F32)
                total += jnp.sum(values * values, axis=1, keepdims=True)
            scale = lax.rsqrt(total / (nt * own_width) + EPS_RMS)
            for t in range(nt):
                for j in range(per):
                    values = slabs[r, t, :, j * depth : (j + 1) * depth].astype(F32)
                    normed[t * per + j, r * seq : (r + 1) * seq, :] = (
                        values * scale * gain[t * per + j]
                    ).astype(BF16)

    def piece(turn, part, got, block, r):
        return pltpu.make_async_remote_copy(
            src_ref=part.at[block, r],
            dst_ref=got.at[rep * nt + tp, block % per],
            send_sem=p_send.at[turn, block, r],
            recv_sem=p_recv.at[turn, rep * nt + tp, block % per],
            device_id={"rep": r, "tp": block // per},
            device_id_type=MESH,
        )

    def abroad(block, r):
        return jnp.logical_or(block // per != tp, r != rep)

    def project(turn, left, gathered_w, part, got, block):
        for r in range(nr):
            part[block, r] = jnp.dot(
                left[r], gathered_w[block], preferred_element_type=F32
            ).astype(BF16)

            @pl.when(abroad(block, r))
            def _():
                piece(turn, part, got, block, r).start()

    def collect(turn, part, got, base, emit):
        for j in range(per):
            total = part[tp * per + j, rep].astype(F32)
            for a, b in offsets:
                slot = lax.rem(rep + a, nr) * nt + lax.rem(tp + b, nt)
                landing = got.at[slot, j]
                pltpu.make_async_remote_copy(
                    src_ref=landing, dst_ref=landing, send_sem=p_send.at[turn, 0, 0],
                    recv_sem=p_recv.at[turn, slot, j], device_id=peer(a, b),
                    device_id_type=MESH,
                ).wait_recv()
                total += got[slot, j].astype(F32)
            width = total.shape[1]
            span = slice(j * width, (j + 1) * width)
            emit(span, (base(span).astype(F32) + total).astype(BF16))

    for copy in locals_ + [own_tok]:
        copy.wait()
    for copy in share(0, feat):
        copy.start()
    forward(0, z)
    forward(1, z)
    forward(2, z)
    uv[...] = jnp.zeros_like(uv)
    gv[...] = jnp.zeros_like(gv)
    share_wait(0, feat)
    norm(feat, mix_gain)

    def in_block(block):
        for r in range(nr):
            rows = slice(r * seq, (r + 1) * seq)
            uv[rows, :] += jnp.dot(
                normed[block, rows, :], g_in[block], preferred_element_type=F32
            )

    stage_loop(0, in_block, 0, lambda: forward(3, z))

    groups, block_len = mixw.shape[0], mixw.shape[1]
    group_width = uv.shape[1] // 2 // groups

    for r in range(nr):
        def mix_rows(i, _):
            start = pl.multiple_of(i * block_len, block_len)
            rows = pl.ds(pl.multiple_of(r * seq + i * block_len, block_len), block_len)
            for g in range(groups):
                at = g * group_width
                half = groups * group_width
                activated = jax.nn.gelu(uv[rows, half + at : half + at + group_width])
                centred = activated - jnp.mean(activated, axis=1, keepdims=True)
                spread = jnp.mean(centred * centred, axis=1, keepdims=True)
                v_norm = (
                    centred * lax.rsqrt(spread + EPS_LN) * norm_gain[:, at : at + group_width]
                ).astype(BF16)
                mixed = jnp.dot(mixw[g], v_norm, preferred_element_type=F32) + bias[g]
                hidden[r, pl.ds(start, block_len), at : at + group_width] = (
                    jax.nn.gelu(uv[rows, at : at + group_width]) * mixed
                ).astype(BF16)
            return 0

        lax.fori_loop(0, seq // block_len, mix_rows, 0)

    stage_loop(
        1, functools.partial(project, 0, hidden, g_out, part1, got1), 0, lambda: None
    )

    def relay(stage, begin, end):
        def step(i, _):
            arrived(stage, order(i) * 2 + y)
            forward(stage, order(i))
            return 0

        lax.fori_loop(begin, end, step, 0)

    def put_middle(span, value):
        feat2[rep, tp, :, span] = value

    relay(2, 1, nz // 2)
    collect(0, part1, got1, lambda span: tok[:, span], put_middle)
    for copy in share(1, feat2):
        copy.start()
    relay(2, nz // 2, nz)
    share_wait(1, feat2)
    norm(feat2, ffn_gain)

    def up_block(block):
        for r in range(nr):
            gv[r, 8:, :] += jnp.dot(
                normed[block, r * seq : (r + 1) * seq, :],
                g_up[block],
                preferred_element_type=F32,
            )

    def up_step(i, _):
        up_block(order(i) * 2 + y)

        @pl.when(i > 0)
        def _():
            arrived(3, order(i) * 2 + y)
            forward(3, order(i))

        other = order(i) * 2 + 1 - y
        arrived(2, other)
        up_block(other)
        return 0

    lax.fori_loop(0, nz, up_step, 0)

    units = act.shape[2]
    taps_len = taps_g.shape[0]
    chunk = 128 if units % 128 == 0 else units
    for r in range(nr):
        for at in range(0, units, chunk):
            gate = jnp.zeros((seq, chunk), F32)
            value = jnp.zeros((seq, chunk), F32)
            for k in range(taps_len):
                first = 8 - (taps_len - 1) + k
                gate += taps_g[k : k + 1, at : at + chunk] * gv[r, first : first + seq, at : at + chunk]
                value += (
                    taps_v[k : k + 1, at : at + chunk]
                    * gv[r, first : first + seq, units + at : units + at + chunk]
                )
            act[r, :, at : at + chunk] = (jax.nn.gelu(gate) * value).astype(BF16)

    down = functools.partial(project, 1, act, g_dn, part2, got2)

    def down_own(i, _):
        down(order(i) * 2 + y)
        return 0

    def down_other(i, _):
        arrived(3, order(i) * 2 + 1 - y)
        down(order(i) * 2 + 1 - y)
        return 0

    lax.fori_loop(0, nz, down_own, 0)
    lax.fori_loop(0, nz, down_other, 0)

    def put_out(span, value):
        out[:, span] = value

    collect(1, part2, got2, lambda span: feat2[rep, tp, :, span], put_out)

    for turn, slabs in enumerate((feat, feat2)):
        for copy in share(turn, slabs):
            copy.wait_send()

    def drain_pieces(block, _):
        for r in range(nr):
            @pl.when(abroad(block, r))
            def _():
                piece(0, part1, got1, block, r).wait_send()
                piece(1, part2, got2, block, r).wait_send()
        return 0

    lax.fori_loop(0, n, drain_pieces, 0)

    def drain_hops(src, _):
        for stage in range(4):
            hop(stage, src * 2 + y, 2).wait_send()
            for way, used in enumerate(ways(src)):
                @pl.when(used)
                def _():
                    hop(stage, src * 2 + y, way).wait_send()
        return 0

    lax.fori_loop(0, nz, drain_hops, 0)


def on_device(
    tokens,
    mix_gain,
    w_u,
    w_v,
    norm_gain,
    mix_weight,
    mix_bias,
    w_mix_out,
    ffn_gain,
    w_gate,
    w_value,
    taps_gate,
    taps_value,
    w_down,
):
    n, nr, nt = lax.axis_size("fs"), lax.axis_size("rep"), lax.axis_size("tp")
    seq, own_width = tokens.shape
    depth, per = own_width * nt // n, n // nt
    block_len = mix_weight.shape[1]
    lower_mask = jnp.arange(block_len)[:, None] >= jnp.arange(block_len)[None, :]
    mixw = own_half(mix_weight, 0)
    mixw = jnp.where(lower_mask[None], mixw, jnp.zeros_like(mixw))
    w_in = jnp.concatenate((own_half(w_u, 1), own_half(w_v, 1)), 1)
    w_up = jnp.concatenate((own_half(w_gate, 1), own_half(w_value, 1)), 1)
    w_out, w_dn = own_half(w_mix_out, 0), own_half(w_down, 0)
    operands = (
        tokens,
        mix_gain.reshape(n, 1, depth),
        w_in,
        own_half(norm_gain, 0)[None, :],
        mixw,
        own_half(mix_bias, 0)[:, :, None],
        w_out,
        ffn_gain.reshape(n, 1, depth),
        w_up,
        own_half(taps_gate, 1).astype(F32),
        own_half(taps_value, 1).astype(F32),
        w_dn,
    )
    vmem, sem = pltpu.VMEM, pltpu.SemaphoreType.DMA
    others = nr * nt - 1
    return pl.pallas_call(
        functools.partial(layer_kernel, n, nr, nt),
        out_shape=jax.ShapeDtypeStruct((seq, own_width), BF16),
        in_specs=[pl.BlockSpec(memory_space=vmem)] * len(operands),
        out_specs=pl.BlockSpec(memory_space=vmem),
        scratch_shapes=[
            vmem((n,) + w_in.shape, BF16),
            vmem((n,) + w_out.shape, BF16),
            vmem((n,) + w_up.shape, BF16),
            vmem((n,) + w_dn.shape, BF16),
            vmem((nr, nt, seq, own_width), BF16),
            vmem((nr, nt, seq, own_width), BF16),
            vmem((n, nr * seq, depth), BF16),
            vmem((nr * seq, w_in.shape[1]), F32),
            vmem((nr, seq, w_out.shape[0]), BF16),
            vmem((nr, seq + 8, w_up.shape[1]), F32),
            vmem((nr, seq, w_dn.shape[0]), BF16),
            vmem((n, nr, seq, depth), BF16),
            vmem((n, nr, seq, depth), BF16),
            vmem((nr * nt, per, seq, depth), BF16),
            vmem((nr * nt, per, seq, depth), BF16),
            sem((4, 3, n)),
            sem((4, n)),
            sem((5,)),
            sem((2, others)),
            sem((2, others)),
            sem((2, n, nr)),
            sem((2, nr * nt, per)),
        ],
        compiler_params=pltpu.CompilerParams(
            collective_id=0, has_side_effects=True, vmem_limit_bytes=67043328
        ),
    )(*operands)


def plane_kernel(
    n, nr, nt,
    tok, mix_gain, w_u, w_v, norm_gain, mixw, bias, w_out, ffn_gain, w_gate, w_value, taps_g, taps_v, w_dn,
    out,
    g_in, g_out, g_up, g_dn, feat, feat2, mid, normed, uv, hidden, gv, act,
    row_scale, squares, part1, part2, inc1, inc2, got1, got2, raw_mix, mix_low, gain_v, bias_all, bias_col, tg, tv,
    l_sem, y_send, y_recv, z_send, z_recv, d_send, d_recv, s_local, s_send, s_recv,
    a_send, a_recv, f_send, r_send, i_recv, t_recv,
):
    rep, fs, tp = lax.axis_index("rep"), lax.axis_index("fs"), lax.axis_index("tp")
    seq, own_width = tok.shape
    ny, nz = 2, n // 2
    z, y = fs // ny, fs % ny
    per = n // nt
    width = own_width // per
    quarter = rep * ny + y
    other_quarter = rep * ny + 1 - y
    fs_y = z * ny + 1 - y
    home = rep == tp
    away = rep != tp
    cu, cf = g_out.shape[2], g_dn.shape[2]
    few = max(1, per // 4)
    feats = (feat, feat2)

    def both(*conditions):
        return functools.reduce(jnp.logical_and, conditions)

    barrier = pltpu.get_barrier_semaphore()
    greeted = [{"tp": 1 - tp}]
    greeted += [{"rep": 1 - rep, "tp": t} for t in range(nt)]
    greeted += [{"fs": fs_y, "tp": t} for t in range(nt)]
    greeted += [{"fs": lax.rem(z + k, nz) * ny + y} for k in range(1, nz)]

    def item(k, block, half):
        if k == 0:
            return g_in.at[half, block]
        if k == 1:
            return g_out.at[block, half]
        if k == 2:
            return g_up.at[half, block]
        return g_dn.at[block, half]

    def pieces(k, which, block):
        whole = item(k, block, tp)
        if k in (0, 2):
            first, second, size = (w_u, w_v, cu) if k == 0 else (w_gate, w_value, cf)
            cols = pl.ds(pl.multiple_of(which * size, 128), size)
            return (
                (first.at[:, cols], whole.at[:, pl.ds(0, size)]),
                (second.at[:, cols], whole.at[:, pl.ds(size, size)]),
            )
        source, size = (w_out, cu) if k == 1 else (w_dn, cf)
        rows = pl.ds(pl.multiple_of(which * size, 128), size)
        return ((source.at[rows, :], whole),)

    def own_load(k):
        return [
            pltpu.make_async_copy(src, dst, l_sem.at[k, i])
            for i, (src, dst) in enumerate(pieces(k, quarter, fs))
        ]

    def across(k, block):
        return [
            pltpu.make_async_remote_copy(
                src_ref=src, dst_ref=dst, send_sem=y_send.at[k, i], recv_sem=y_recv.at[k, i],
                device_id={"fs": fs_y}, device_id_type=MESH,
            )
            for i, (src, dst) in enumerate(pieces(k, other_quarter, block))
        ]

    def z_copy(k, block, step):
        return pltpu.make_async_remote_copy(
            src_ref=item(k, block, tp), dst_ref=item(k, block, tp),
            send_sem=z_send.at[k, block, step + 2], recv_sem=z_recv.at[k, block],
            device_id={"fs": fs + ny * step}, device_id_type=MESH,
        )

    def d_copy(k, block):
        return pltpu.make_async_remote_copy(
            src_ref=item(k, block, tp), dst_ref=item(k, block, tp),
            send_sem=d_send.at[k, block], recv_sem=d_recv.at[k, block],
            device_id={"tp": 1 - tp}, device_id_type=MESH,
        )

    def inside(step):
        return jnp.logical_and(z + step >= 0, z + step < nz)

    def reach(k):
        return (1, -1) if k == 0 else (2, -2, 1, -1)

    def spread(k, block):
        for step in reach(k):
            @pl.when(inside(step))
            def _():
                z_copy(k, block, step).start()
        d_copy(k, block).start()

    def arrive(k, block):
        landing = item(k, block, tp)
        pltpu.make_async_remote_copy(
            src_ref=landing, dst_ref=landing, send_sem=z_send.at[k, block, 2],
            recv_sem=z_recv.at[k, block], device_id={"tp": 1 - tp}, device_id_type=MESH,
        ).wait_recv()
        d_copy(k, block).start()

    def cross_over(k):
        for copy in across(k, fs_y):
            copy.wait_recv()
        spread(k, fs_y)

    def relays(k, far):
        return [
            (sign, z - sign * far, jnp.logical_and(inside(sign), inside(-sign * far)))
            for sign in (1, -1)
        ]

    def nearest(k):
        return 1 if k == 0 else 2

    def relay(k, far, at):
        for sign, source, used in relays(k, far):
            @pl.when(used)
            def _():
                arrive(k, source * ny + at)
                z_copy(k, source * ny + at, sign).start()

    def relay_all(k):
        for far in range(nearest(k), nz - 1):
            for at in range(ny):
                relay(k, far, at)

    def relayed(k, source):
        up = jnp.logical_and(z - source >= nearest(k), inside(1))
        down = jnp.logical_and(source - z >= nearest(k), inside(-1))
        return jnp.logical_or(up, down)

    def need(k, block):
        source = block // ny
        @pl.when(jnp.logical_and(source != z, jnp.logical_not(relayed(k, source))))
        def _():
            arrive(k, block)

    def partner_wait(k, block):
        landing = item(k, block, 1 - tp)
        pltpu.make_async_remote_copy(
            src_ref=landing, dst_ref=landing, send_sem=d_send.at[k, block],
            recv_sem=d_recv.at[k, block], device_id={"tp": 1 - tp}, device_id_type=MESH,
        ).wait_recv()

    def order(i):
        near = jnp.minimum(z, nz - 1 - z)
        swing = z + ((i + 1) // 2) * (1 - 2 * (i % 2))
        rest = jnp.where(z < nz - 1 - z, i, nz - 1 - i)
        return jnp.where(i <= 2 * near, swing, rest)

    def near_block(i):
        return order(i // ny) * ny + lax.rem(y + i, ny)

    def plain_block(i):
        return order(i // ny) * ny + lax.rem(i, ny)

    small = [
        (mixw.at[pl.ds(quarter * raw_mix.shape[1], raw_mix.shape[1])], raw_mix.at[tp]),
        (norm_gain.at[:, pl.ds(pl.multiple_of(quarter * cu, 128), cu)], gain_v.at[tp]),
        (bias, bias_all.at[tp]),
        (taps_g.at[:, pl.ds(pl.multiple_of(quarter * cf, 128), cf)], tg.at[tp]),
        (taps_v.at[:, pl.ds(pl.multiple_of(quarter * cf, 128), cf)], tv.at[tp]),
    ]
    small_local = [
        pltpu.make_async_copy(src, dst, s_local.at[i]) for i, (src, dst) in enumerate(small)
    ]
    small_away = [
        pltpu.make_async_remote_copy(
            src_ref=src, dst_ref=dst, send_sem=s_send.at[i], recv_sem=s_recv.at[i],
            device_id={"tp": 1 - tp}, device_id_type=MESH,
        )
        for i, (src, dst) in enumerate(small)
    ]

    def ag_source(turn, i):
        if turn == 0:
            return tok.at[:, pl.ds(pl.multiple_of(i * width, 128), width)]
        return mid.at[i]

    def ag_copy(turn, i, way):
        block = tp * per + i
        device = ({"rep": 1 - rep, "tp": rep}, {"fs": fs_y, "tp": rep}, {"tp": 1 - tp})[way]
        return pltpu.make_async_remote_copy(
            src_ref=ag_source(turn, i), dst_ref=feats[turn].at[y, block],
            send_sem=a_send.at[turn, way, i], recv_sem=a_recv.at[turn, y, block],
            device_id=device, device_id_type=MESH,
        )

    def ag_send(turn, i):
        ag_copy(turn, i, 0).start()
        ag_copy(turn, i, 1).start()

        @pl.when(away)
        def _():
            ag_copy(turn, i, 2).start()

        @pl.when(home)
        def _():
            feats[turn][y, tp * per + i] = ag_source(turn, i)[...]

    def passed(block):
        at = lax.rem(block, per)
        return jnp.logical_or(
            jnp.logical_and(home, at >= few), jnp.logical_and(away, at < few)
        )

    def ag_pass(turn, block):
        slot = jnp.where(home, 1 - y, y)
        return pltpu.make_async_remote_copy(
            src_ref=feats[turn].at[slot, block], dst_ref=feats[turn].at[slot, block],
            send_sem=f_send.at[turn, block], recv_sem=a_recv.at[turn, slot, block],
            device_id={
                "rep": jnp.where(home, 1 - rep, rep),
                "fs": jnp.where(home, fs, fs_y),
            },
            device_id_type=MESH,
        )

    def ag_landed(turn, slot, block):
        landing = feats[turn].at[slot, block]
        pltpu.make_async_remote_copy(
            src_ref=landing, dst_ref=landing, send_sem=f_send.at[turn, 0],
            recv_sem=a_recv.at[turn, slot, block], device_id={"tp": 1 - tp}, device_id_type=MESH,
        ).wait_recv()

    def ag_forward(turn, block):
        @pl.when(passed(block))
        def _():
            ag_landed(turn, jnp.where(home, 1 - y, y), block)
            ag_pass(turn, block).start()

    def ag_wait(turn, slot, block):
        local = both(home, slot == y, block // per == tp)
        sent_on = jnp.logical_and(passed(block), slot == jnp.where(home, 1 - y, y))

        @pl.when(jnp.logical_not(jnp.logical_or(local, sent_on)))
        def _():
            ag_landed(turn, slot, block)

    def weigh(turn, gain, block):
        gains = gain[:, pl.ds(pl.multiple_of(block * width, 128), width)]
        for r in range(2):
            slot = lax.rem(y + r, 2)
            ag_wait(turn, slot, block)
            values = feats[turn][slot, block].astype(F32)
            normed[block, slot] = (values * gains).astype(BF16)
            for at in range(0, width, 128):
                piece = values[:, at : at + 128]
                squares[slot] += piece * piece

    def finish_scale():
        for slot in range(2):
            total = jnp.sum(squares[slot], axis=1, keepdims=True)
            row_scale[slot, 8:, :] = lax.rsqrt(total / (n * width) + EPS_RMS)

    def gathered_loop(k, turn, gain, multiply):
        def step(i, _):
            block = near_block(i)
            weigh(turn, gain, block)
            need(k, block)
            multiply(block, tp)

            @pl.when(i > 0)
            def _():
                before = near_block(i - 1)
                partner_wait(k, before)
                multiply(before, 1 - tp)

            return 0

        lax.fori_loop(0, n, step, 0)
        last = near_block(n - 1)
        partner_wait(k, last)
        multiply(last, 1 - tp)
        finish_scale()

    def even(block):
        return lax.rem(block, 2) == 0

    parts, incs, gots = (part1, part2), (inc1, inc2), (got1, got2)

    def r_copy(turn, r, block, kind):
        slot = lax.rem(y + r, 2)
        core, at = block // per, lax.rem(block, per)
        got, inc = gots[turn], incs[turn]
        dst, sem, device = {
            "diag_x": (inc.at[block], i_recv.at[turn, block], {"rep": 1 - rep}),
            "diag_y": (inc.at[block], i_recv.at[turn, block], {"fs": fs_y}),
            "pair": (got.at[0, at], t_recv.at[turn, 0, at], {"tp": 1 - tp}),
            "x": (got.at[1, at], t_recv.at[turn, 1, at], {"rep": 1 - rep, "tp": core}),
            "y": (got.at[2, at], t_recv.at[turn, 2, at], {"fs": fs_y, "tp": core}),
        }[kind]
        return pltpu.make_async_remote_copy(
            src_ref=parts[turn].at[slot, block], dst_ref=dst, send_sem=r_send.at[turn, r, block],
            recv_sem=sem, device_id=device, device_id_type=MESH,
        )

    def cases(block):
        return (
            (1, "diag_x", both(away, even(block)), True),
            (1, "diag_y", both(away, jnp.logical_not(even(block))), True),
            (1, "y", both(home, jnp.logical_not(even(block))), True),
            (0, "pair", both(home, block // per != tp), True),
            (0, "x", both(away, even(block)), True),
            (1, "y", both(home, even(block)), False),
            (0, "x", both(away, jnp.logical_not(even(block))), False),
        )

    def project(turn, left, weight, block):
        size = weight.shape[1] * weight.shape[2]
        right = weight[block].reshape(size, weight.shape[3])
        for r in (1, 0):
            slot = lax.rem(y + r, 2)
            parts[turn][slot, block] = jnp.dot(
                left[slot], right, preferred_element_type=F32
            ).astype(BF16)
            for row, kind, used, now in cases(block):
                if row == r and now:
                    @pl.when(used)
                    def _():
                        r_copy(turn, r, block, kind).start()

        @pl.when(both(home, block // per == tp))
        def _():
            gots[turn][0, lax.rem(block, per)] = parts[turn][y, block]

    def join(turn, block):
        for r, kind, used, now in cases(block):
            if not now:
                @pl.when(used)
                def _():
                    landing = incs[turn].at[block]
                    pltpu.make_async_remote_copy(
                        src_ref=landing, dst_ref=landing, send_sem=r_send.at[turn, 0, 0],
                        recv_sem=i_recv.at[turn, block], device_id={"rep": 1 - rep},
                        device_id_type=MESH,
                    ).wait_recv()
                    slot = lax.rem(y + r, 2)
                    parts[turn][slot, block] = (
                        parts[turn][slot, block].astype(F32) + incs[turn][block].astype(F32)
                    ).astype(BF16)
                    r_copy(turn, r, block, kind).start()

    def landed(turn, kind, at):
        landing = gots[turn].at[kind, at]
        pltpu.make_async_remote_copy(
            src_ref=landing, dst_ref=landing, send_sem=r_send.at[turn, 0, 0],
            recv_sem=t_recv.at[turn, kind, at], device_id={"rep": 1 - rep}, device_id_type=MESH,
        ).wait_recv()

    def collect(turn, block):
        at = lax.rem(block, per)

        @pl.when(away)
        def _():
            landed(turn, 0, at)

        landed(turn, 1, at)
        landed(turn, 2, at)
        got = gots[turn]
        total = got[0, at].astype(F32) + got[1, at].astype(F32) + got[2, at].astype(F32)
        cols = pl.ds(pl.multiple_of(at * width, 128), width)
        if turn == 0:
            mid[at] = (tok[:, cols].astype(F32) + total).astype(BF16)
            ag_send(1, at)
        else:
            out[:, cols] = (mid[at].astype(F32) + total).astype(BF16)

    def scatter_loop(k, turn, left, weight, beside):
        def step(i, _):
            @pl.when(i < n)
            def _():
                need(k, plain_block(i))

            @pl.when(both(i >= 1, i < n + 1))
            def _():
                block = plain_block(i - 1)
                partner_wait(k, block)
                project(turn, left, weight, block)

            @pl.when(both(i >= 3, i < n + 3))
            def _():
                join(turn, plain_block(i - 3))

            for at, action in beside:
                pl.when(i == at)(action)

            @pl.when(i >= 5)
            def _():
                block = plain_block(i - 5)

                @pl.when(block // per == tp)
                def _():
                    collect(turn, block)

            return 0

        lax.fori_loop(0, n + 5, step, 0)

    for k in range(4):
        for copy in own_load(k):
            copy.start()
    for copy in small_local:
        copy.start()
    for target in greeted:
        pl.semaphore_signal(barrier, inc=1, device_id=target, device_id_type=MESH)
    pl.semaphore_wait(barrier, len(greeted))

    for copy in across(0, fs):
        copy.start()
    for i in range(per):
        ag_send(0, i)
    for copy in own_load(0):
        copy.wait()
    spread(0, fs)
    for copy in across(1, fs) + small_away:
        copy.start()
    uv[...] = jnp.zeros_like(uv)
    gv[...] = jnp.zeros_like(gv)
    squares[...] = jnp.zeros_like(squares)
    row_scale[...] = jnp.zeros_like(row_scale)
    cross_over(0)
    for k in range(1, 4):
        for copy in own_load(k):
            copy.wait()
    turns = [(far, at) for far in range(1, nz - 1) for at in (y, 1 - y)]
    for i in range(max(per, len(turns))):
        if i < len(turns):
            relay(0, *turns[i])
        if i == 2:
            spread(1, fs)
        if i < per:
            for half in range(nt):
                ag_forward(0, half * per + i)
    cross_over(1)
    for k in (2, 3):
        for copy in across(k, fs):
            copy.start()

    def in_block(block, half):
        for slot in range(2):
            uv[half, slot] += jnp.dot(
                normed[block, slot], g_in[half, block], preferred_element_type=F32
            )

    gathered_loop(0, 0, mix_gain, in_block)

    for copy in small_local:
        copy.wait()
    for i, (_, dst) in enumerate(small):
        landing = (raw_mix, gain_v, bias_all, tg, tv)[i].at[1 - tp]
        pltpu.make_async_remote_copy(
            src_ref=landing, dst_ref=landing, send_sem=s_send.at[i], recv_sem=s_recv.at[i],
            device_id={"tp": 1 - tp}, device_id_type=MESH,
        ).wait_recv()
    per_half, block_len = raw_mix.shape[1], raw_mix.shape[2]
    group_width = cu // per_half
    at_row = lax.broadcasted_iota(jnp.int32, (block_len, block_len), 0)
    at_col = lax.broadcasted_iota(jnp.int32, (block_len, block_len), 1)
    for half in range(nt):
        turned = bias_all[half].T
        lane = lax.broadcasted_iota(jnp.int32, turned.shape, 1)
        for g in range(per_half):
            mix_low[half, g] = jnp.where(
                at_row >= at_col, raw_mix[half, g].astype(F32), 0.0
            ).astype(BF16)
            bias_col[half, g] = jnp.sum(
                jnp.where(lane == quarter * per_half + g, turned, 0.0), axis=1, keepdims=True
            )

    for slot in range(2):
        def mix_rows(i, _):
            rows = pl.ds(pl.multiple_of(i * block_len, block_len), block_len)
            scale = row_scale[slot, pl.ds(pl.multiple_of(i * block_len + 8, 8), block_len), :]
            for half in range(nt):
                for g in range(per_half):
                    at = g * group_width
                    activated = jax.nn.gelu(
                        uv[half, slot, rows, cu + at : cu + at + group_width] * scale
                    )
                    centred = activated - jnp.mean(activated, axis=1, keepdims=True)
                    spread_sq = jnp.mean(centred * centred, axis=1, keepdims=True)
                    v_norm = (
                        centred
                        * lax.rsqrt(spread_sq + EPS_LN)
                        * gain_v[half, :, at : at + group_width]
                    ).astype(BF16)
                    mixed = (
                        jnp.dot(mix_low[half, g], v_norm, preferred_element_type=F32)
                        + bias_col[half, g]
                    )
                    hidden[slot, rows, half * cu + at : half * cu + at + group_width] = (
                        jax.nn.gelu(uv[half, slot, rows, at : at + group_width] * scale) * mixed
                    ).astype(BF16)
            return 0

        lax.fori_loop(0, seq // block_len, mix_rows, 0)

    relay_all(1)
    spread(2, fs)
    cross_over(2)
    squares[...] = jnp.zeros_like(squares)

    def start_down():
        spread(3, fs)
        cross_over(3)

    scatter_loop(1, 0, hidden, g_out, ((n + 2, lambda: relay_all(2)), (n + 3, start_down)))
    lax.fori_loop(0, n, lambda i, _: (ag_forward(1, plain_block(i)), 0)[1], 0)

    def up_block(block, half):
        for slot in range(2):
            gv[half, slot, 8:, :] += jnp.dot(
                normed[block, slot], g_up[half, block], preferred_element_type=F32
            )

    gathered_loop(2, 1, ffn_gain, up_block)
    relay_all(3)

    taps_len = tg.shape[1]
    chunk = 128
    for slot in range(2):
        for half in range(nt):
            for at in range(0, cf, chunk):
                gate = jnp.zeros((seq, chunk), F32)
                value = jnp.zeros((seq, chunk), F32)
                for k in range(taps_len):
                    first = 8 - (taps_len - 1) + k
                    rows = slice(first, first + seq)
                    scale = row_scale[slot, rows, :]
                    gate += tg[half, k : k + 1, at : at + chunk].astype(F32) * (
                        gv[half, slot, rows, at : at + chunk] * scale
                    )
                    value += tv[half, k : k + 1, at : at + chunk].astype(F32) * (
                        gv[half, slot, rows, cf + at : cf + at + chunk] * scale
                    )
                act[slot, :, half * cf + at : half * cf + at + chunk] = (
                    jax.nn.gelu(gate) * value
                ).astype(BF16)

    scatter_loop(3, 1, act, g_dn, ())

    for k in range(4):
        for copy in across(k, fs):
            copy.wait_send()
    for copy in small_away:
        copy.wait_send()

    def drain_block(block, _):
        for k in range(4):
            d_copy(k, block).wait_send()
        for turn in range(2):
            for r, kind, used, _now in cases(block):
                @pl.when(used)
                def _():
                    r_copy(turn, r, block, kind).wait_send()

            @pl.when(passed(block))
            def _():
                ag_pass(turn, block).wait_send()
        return 0

    lax.fori_loop(0, n, drain_block, 0)

    def drain_gather(i, _):
        for turn in range(2):
            ag_copy(turn, i, 0).wait_send()
            ag_copy(turn, i, 1).wait_send()

            @pl.when(away)
            def _():
                ag_copy(turn, i, 2).wait_send()
        return 0

    lax.fori_loop(0, per, drain_gather, 0)

    def drain_line(at, _):
        for k in range(4):
            for step in reach(k):
                @pl.when(inside(step))
                def _():
                    z_copy(k, z * ny + at, step).wait_send()
            for far in range(nearest(k), nz - 1):
                for sign, source, used in relays(k, far):
                    @pl.when(used)
                    def _():
                        z_copy(k, source * ny + at, sign).wait_send()
        return 0

    lax.fori_loop(0, ny, drain_line, 0)


def on_plane(
    tokens,
    mix_gain,
    w_u,
    w_v,
    norm_gain,
    mix_weight,
    mix_bias,
    w_mix_out,
    ffn_gain,
    w_gate,
    w_value,
    taps_gate,
    taps_value,
    w_down,
):
    n, nr, nt = lax.axis_size("fs"), lax.axis_size("rep"), lax.axis_size("tp")
    seq, own_width = tokens.shape
    per = n // nt
    width = own_width // per
    depth = w_u.shape[0]
    share = nr * 2
    cu, cf = w_u.shape[1] // share, w_gate.shape[1] // share
    groups, block_len = mix_weight.shape[0], mix_weight.shape[1]
    taps_len = taps_gate.shape[0]
    vmem, sem, hbm = pltpu.VMEM, pltpu.SemaphoreType.DMA, pl.ANY
    operands = (
        (tokens, vmem),
        (mix_gain[None, :], vmem),
        (w_u, hbm),
        (w_v, hbm),
        (norm_gain[None, :], hbm),
        (mix_weight, hbm),
        (mix_bias, hbm),
        (w_mix_out, hbm),
        (ffn_gain[None, :], vmem),
        (w_gate, hbm),
        (w_value, hbm),
        (taps_gate, hbm),
        (taps_value, hbm),
        (w_down, hbm),
    )
    return pl.pallas_call(
        functools.partial(plane_kernel, n, nr, nt),
        out_shape=jax.ShapeDtypeStruct((seq, own_width), BF16),
        in_specs=[pl.BlockSpec(memory_space=space) for _, space in operands],
        out_specs=pl.BlockSpec(memory_space=vmem),
        scratch_shapes=[
            vmem((nt, n, depth, 2 * cu), BF16),
            vmem((n, nt, cu, width), BF16),
            vmem((nt, n, depth, 2 * cf), BF16),
            vmem((n, nt, cf, width), BF16),
            vmem((2, n, seq, width), BF16),
            vmem((2, n, seq, width), BF16),
            vmem((per, seq, width), BF16),
            vmem((n, 2, seq, width), BF16),
            vmem((nt, 2, seq, 2 * cu), F32),
            vmem((2, seq, nt * cu), BF16),
            vmem((nt, 2, seq + 8, 2 * cf), F32),
            vmem((2, seq, nt * cf), BF16),
            vmem((2, seq + 8, 1), F32),
            vmem((2, seq, 128), F32),
            vmem((2, n, seq, width), BF16),
            vmem((2, n, seq, width), BF16),
            vmem((n, seq, width), BF16),
            vmem((n, seq, width), BF16),
            vmem((3, per, seq, width), BF16),
            vmem((3, per, seq, width), BF16),
            vmem((nt, groups // share, block_len, block_len), BF16),
            vmem((nt, groups // share, block_len, block_len), BF16),
            vmem((nt, 1, cu), F32),
            vmem((nt, groups, block_len), F32),
            vmem((nt, groups // share, block_len, 1), F32),
            vmem((nt, taps_len, cf), BF16),
            vmem((nt, taps_len, cf), BF16),
            sem((4, 2)),
            sem((4, 2)),
            sem((4, 2)),
            sem((4, n, 5)),
            sem((4, n)),
            sem((4, n)),
            sem((4, n)),
            sem((5,)),
            sem((5,)),
            sem((5,)),
            sem((2, 3, per)),
            sem((2, 2, n)),
            sem((2, n)),
            sem((2, 2, n)),
            sem((2, n)),
            sem((2, 3, per)),
        ],
        compiler_params=pltpu.CompilerParams(
            collective_id=0, has_side_effects=True, vmem_limit_bytes=67043328
        ),
    )(*(array for array, _ in operands))


def by_shape(*arrays):
    n, nr, nt = lax.axis_size("fs"), lax.axis_size("rep"), lax.axis_size("tp")
    groups, units = arrays[5].shape[0], arrays[9].shape[1]
    share = nr * 2
    fits = nr == 2 and nt == 2 and n % 2 == 0 and groups % share == 0 and units % (share * 128) == 0
    return on_plane(*arrays) if fits else on_device(*arrays)


def solution(mesh):
    placed = (
        P(("rep", "fs"), "tp"),
        P(),
        P("fs", "tp"),
        P("fs", "tp"),
        P("tp"),
        P("tp", None, None),
        P("tp", None),
        P("tp", "fs"),
        P(),
        P("fs", "tp"),
        P("fs", "tp"),
        P(None, "tp"),
        P(None, "tp"),
        P("tp", "fs"),
    )
    return jax.shard_map(
        by_shape, mesh=mesh, in_specs=placed, out_specs=P(("rep", "fs"), "tp"), check_vma=False
    )
```

```python
import functools

import jax
import jax.numpy as jnp
from jax import lax
from jax.experimental import pallas as pl
from jax.experimental.pallas import tpu as pltpu
from jax.sharding import PartitionSpec as P

EPS_RMS = 1e-06
EPS_LN = 1e-05
F32 = jnp.float32
BF16 = jnp.bfloat16
MESH = pl.DeviceIdType.MESH


def own_half(array, axis):
    share = array.shape[axis] // lax.axis_size("rep")
    return lax.dynamic_slice_in_dim(array, lax.axis_index("rep") * share, share, axis)


def layer_kernel(
    n, nr, nt,
    tok, mix_gain, w_in, norm_gain, mixw, bias, w_out, ffn_gain, w_up, taps_g, taps_v, w_dn,
    out,
    g_in, g_out, g_up, g_dn, feat, feat2, normed, uv, hidden, gv, act, part1, part2, got1, got2,
    w_send, w_recv, w_local, f_send, f_recv, p_send, p_recv,
):
    rep, fs, tp = lax.axis_index("rep"), lax.axis_index("fs"), lax.axis_index("tp")
    seq, own_width = tok.shape
    nz = n // 2
    z, y = fs // 2, fs % 2
    per = n // nt
    depth = normed.shape[2]
    mine = (w_in, w_out, w_up, w_dn)
    gathered = (g_in, g_out, g_up, g_dn)
    offsets = [(a, b) for a in range(nr) for b in range(nt) if (a, b) != (0, 0)]

    def peer(a, b):
        return {"rep": lax.rem(rep + a, nr), "tp": lax.rem(tp + b, nt)}

    barrier = pltpu.get_barrier_semaphore()
    line = (lax.rem(z + 1, nz), lax.rem(z + nz - 1, nz))
    greeted = [{"fs": z * 2 + 1 - y}] + [{"fs": at * 2 + y} for at in line]
    greeted += [peer(a, b) for a, b in offsets]
    for target in greeted:
        pl.semaphore_signal(barrier, inc=1, device_id=target, device_id_type=MESH)
    pl.semaphore_wait(barrier, len(greeted))

    def hop(stage, block, way):
        target = (fs + 2, fs - 2, z * 2 + 1 - y)[way]
        return pltpu.make_async_remote_copy(
            src_ref=gathered[stage].at[block],
            dst_ref=gathered[stage].at[block],
            send_sem=w_send.at[stage, way, block],
            recv_sem=w_recv.at[stage, block],
            device_id={"fs": target},
            device_id_type=MESH,
        )

    def ways(src):
        return (
            jnp.logical_and(src <= z, z < nz - 1),
            jnp.logical_and(src >= z, z > 0),
        )

    def forward(stage, src):
        block = src * 2 + y
        hop(stage, block, 2).start()
        for way, used in enumerate(ways(src)):
            @pl.when(used)
            def _():
                hop(stage, block, way).start()

    def arrived(stage, block):
        hop(stage, block, 2).wait_recv()

    def order(i):
        near = jnp.minimum(z, nz - 1 - z)
        swing = z + ((i + 1) // 2) * (1 - 2 * (i % 2))
        rest = jnp.where(z < nz - 1 - z, i, nz - 1 - i)
        return jnp.where(i <= 2 * near, swing, rest)

    def stage_loop(stage, compute, begin, middle):
        def step(i, _):
            src = order(i)

            @pl.when(i > 0)
            def _():
                arrived(stage, src * 2 + y)
                forward(stage, src)

            compute(src * 2 + y)

            @pl.when(i > 0)
            def _():
                other = order(i - 1) * 2 + 1 - y
                arrived(stage, other)
                compute(other)

            return 0

        lax.fori_loop(begin, nz, step, 0)
        middle()
        last = order(nz - 1) * 2 + 1 - y
        arrived(stage, last)
        compute(last)

    locals_ = [
        pltpu.make_async_copy(mine[k], gathered[k].at[fs], w_local.at[k]) for k in range(4)
    ]
    own_tok = pltpu.make_async_copy(tok, feat.at[rep, tp], w_local.at[4])
    for copy in locals_ + [own_tok]:
        copy.start()

    def share(turn, slabs):
        copies = []
        for k, (a, b) in enumerate(offsets):
            copies.append(
                pltpu.make_async_remote_copy(
                    src_ref=slabs.at[rep, tp],
                    dst_ref=slabs.at[rep, tp],
                    send_sem=f_send.at[turn, k],
                    recv_sem=f_recv.at[turn, k],
                    device_id=peer(a, b),
                    device_id_type=MESH,
                )
            )
        return copies

    def share_wait(turn, slabs):
        for k, (a, b) in enumerate(offsets):
            slab = slabs.at[lax.rem(rep + nr - a, nr), lax.rem(tp + nt - b, nt)]
            pltpu.make_async_remote_copy(
                src_ref=slab, dst_ref=slab, send_sem=f_send.at[turn, k],
                recv_sem=f_recv.at[turn, k], device_id=peer(a, b), device_id_type=MESH,
            ).wait_recv()

    def norm(slabs, gain):
        for r in range(nr):
            total = jnp.zeros((seq, 1), F32)
            for t in range(nt):
                values = slabs[r, t].astype(F32)
                total += jnp.sum(values * values, axis=1, keepdims=True)
            scale = lax.rsqrt(total / (nt * own_width) + EPS_RMS)
            for t in range(nt):
                for j in range(per):
                    values = slabs[r, t, :, j * depth : (j + 1) * depth].astype(F32)
                    normed[t * per + j, r * seq : (r + 1) * seq, :] = (
                        values * scale * gain[t * per + j]
                    ).astype(BF16)

    def piece(turn, part, got, block, r):
        return pltpu.make_async_remote_copy(
            src_ref=part.at[block, r],
            dst_ref=got.at[rep * nt + tp, block % per],
            send_sem=p_send.at[turn, block, r],
            recv_sem=p_recv.at[turn, rep * nt + tp, block % per],
            device_id={"rep": r, "tp": block // per},
            device_id_type=MESH,
        )

    def abroad(block, r):
        return jnp.logical_or(block // per != tp, r != rep)

    def project(turn, left, gathered_w, part, got, block):
        for r in range(nr):
            part[block, r] = jnp.dot(
                left[r], gathered_w[block], preferred_element_type=F32
            ).astype(BF16)

            @pl.when(abroad(block, r))
            def _():
                piece(turn, part, got, block, r).start()

    def collect(turn, part, got, base, emit):
        for j in range(per):
            total = part[tp * per + j, rep].astype(F32)
            for a, b in offsets:
                slot = lax.rem(rep + a, nr) * nt + lax.rem(tp + b, nt)
                landing = got.at[slot, j]
                pltpu.make_async_remote_copy(
                    src_ref=landing, dst_ref=landing, send_sem=p_send.at[turn, 0, 0],
                    recv_sem=p_recv.at[turn, slot, j], device_id=peer(a, b),
                    device_id_type=MESH,
                ).wait_recv()
                total += got[slot, j].astype(F32)
            width = total.shape[1]
            span = slice(j * width, (j + 1) * width)
            emit(span, (base(span).astype(F32) + total).astype(BF16))

    for copy in locals_ + [own_tok]:
        copy.wait()
    for copy in share(0, feat):
        copy.start()
    forward(0, z)
    forward(1, z)
    forward(2, z)
    uv[...] = jnp.zeros_like(uv)
    gv[...] = jnp.zeros_like(gv)
    share_wait(0, feat)
    norm(feat, mix_gain)

    def in_block(block):
        for r in range(nr):
            rows = slice(r * seq, (r + 1) * seq)
            uv[rows, :] += jnp.dot(
                normed[block, rows, :], g_in[block], preferred_element_type=F32
            )

    stage_loop(0, in_block, 0, lambda: forward(3, z))

    groups, block_len = mixw.shape[0], mixw.shape[1]
    group_width = uv.shape[1] // 2 // groups

    for r in range(nr):
        def mix_rows(i, _):
            start = pl.multiple_of(i * block_len, block_len)
            rows = pl.ds(pl.multiple_of(r * seq + i * block_len, block_len), block_len)
            for g in range(groups):
                at = g * group_width
                half = groups * group_width
                activated = jax.nn.gelu(uv[rows, half + at : half + at + group_width])
                centred = activated - jnp.mean(activated, axis=1, keepdims=True)
                spread = jnp.mean(centred * centred, axis=1, keepdims=True)
                v_norm = (
                    centred * lax.rsqrt(spread + EPS_LN) * norm_gain[:, at : at + group_width]
                ).astype(BF16)
                mixed = jnp.dot(mixw[g], v_norm, preferred_element_type=F32) + bias[g]
                hidden[r, pl.ds(start, block_len), at : at + group_width] = (
                    jax.nn.gelu(uv[rows, at : at + group_width]) * mixed
                ).astype(BF16)
            return 0

        lax.fori_loop(0, seq // block_len, mix_rows, 0)

    stage_loop(
        1, functools.partial(project, 0, hidden, g_out, part1, got1), 0, lambda: None
    )

    def relay(stage, begin, end):
        def step(i, _):
            arrived(stage, order(i) * 2 + y)
            forward(stage, order(i))
            return 0

        lax.fori_loop(begin, end, step, 0)

    def put_middle(span, value):
        feat2[rep, tp, :, span] = value

    relay(2, 1, nz // 2)
    collect(0, part1, got1, lambda span: tok[:, span], put_middle)
    for copy in share(1, feat2):
        copy.start()
    relay(2, nz // 2, nz)
    share_wait(1, feat2)
    norm(feat2, ffn_gain)

    def up_block(block):
        for r in range(nr):
            gv[r, 8:, :] += jnp.dot(
                normed[block, r * seq : (r + 1) * seq, :],
                g_up[block],
                preferred_element_type=F32,
            )

    def up_step(i, _):
        up_block(order(i) * 2 + y)

        @pl.when(i > 0)
        def _():
            arrived(3, order(i) * 2 + y)
            forward(3, order(i))

        other = order(i) * 2 + 1 - y
        arrived(2, other)
        up_block(other)
        return 0

    lax.fori_loop(0, nz, up_step, 0)

    units = act.shape[2]
    taps_len = taps_g.shape[0]
    chunk = 128 if units % 128 == 0 else units
    for r in range(nr):
        for at in range(0, units, chunk):
            gate = jnp.zeros((seq, chunk), F32)
            value = jnp.zeros((seq, chunk), F32)
            for k in range(taps_len):
                first = 8 - (taps_len - 1) + k
                gate += taps_g[k : k + 1, at : at + chunk] * gv[r, first : first + seq, at : at + chunk]
                value += (
                    taps_v[k : k + 1, at : at + chunk]
                    * gv[r, first : first + seq, units + at : units + at + chunk]
                )
            act[r, :, at : at + chunk] = (jax.nn.gelu(gate) * value).astype(BF16)

    down = functools.partial(project, 1, act, g_dn, part2, got2)

    def down_own(i, _):
        down(order(i) * 2 + y)
        return 0

    def down_other(i, _):
        arrived(3, order(i) * 2 + 1 - y)
        down(order(i) * 2 + 1 - y)
        return 0

    lax.fori_loop(0, nz, down_own, 0)
    lax.fori_loop(0, nz, down_other, 0)

    def put_out(span, value):
        out[:, span] = value

    collect(1, part2, got2, lambda span: feat2[rep, tp, :, span], put_out)

    for turn, slabs in enumerate((feat, feat2)):
        for copy in share(turn, slabs):
            copy.wait_send()

    def drain_pieces(block, _):
        for r in range(nr):
            @pl.when(abroad(block, r))
            def _():
                piece(0, part1, got1, block, r).wait_send()
                piece(1, part2, got2, block, r).wait_send()
        return 0

    lax.fori_loop(0, n, drain_pieces, 0)

    def drain_hops(src, _):
        for stage in range(4):
            hop(stage, src * 2 + y, 2).wait_send()
            for way, used in enumerate(ways(src)):
                @pl.when(used)
                def _():
                    hop(stage, src * 2 + y, way).wait_send()
        return 0

    lax.fori_loop(0, nz, drain_hops, 0)


def on_device(
    tokens,
    mix_gain,
    w_u,
    w_v,
    norm_gain,
    mix_weight,
    mix_bias,
    w_mix_out,
    ffn_gain,
    w_gate,
    w_value,
    taps_gate,
    taps_value,
    w_down,
):
    n, nr, nt = lax.axis_size("fs"), lax.axis_size("rep"), lax.axis_size("tp")
    seq, own_width = tokens.shape
    depth, per = own_width * nt // n, n // nt
    block_len = mix_weight.shape[1]
    lower_mask = jnp.arange(block_len)[:, None] >= jnp.arange(block_len)[None, :]
    mixw = own_half(mix_weight, 0)
    mixw = jnp.where(lower_mask[None], mixw, jnp.zeros_like(mixw))
    w_in = jnp.concatenate((own_half(w_u, 1), own_half(w_v, 1)), 1)
    w_up = jnp.concatenate((own_half(w_gate, 1), own_half(w_value, 1)), 1)
    w_out, w_dn = own_half(w_mix_out, 0), own_half(w_down, 0)
    operands = (
        tokens,
        mix_gain.reshape(n, 1, depth),
        w_in,
        own_half(norm_gain, 0)[None, :],
        mixw,
        own_half(mix_bias, 0)[:, :, None],
        w_out,
        ffn_gain.reshape(n, 1, depth),
        w_up,
        own_half(taps_gate, 1).astype(F32),
        own_half(taps_value, 1).astype(F32),
        w_dn,
    )
    vmem, sem = pltpu.VMEM, pltpu.SemaphoreType.DMA
    others = nr * nt - 1
    return pl.pallas_call(
        functools.partial(layer_kernel, n, nr, nt),
        out_shape=jax.ShapeDtypeStruct((seq, own_width), BF16),
        in_specs=[pl.BlockSpec(memory_space=vmem)] * len(operands),
        out_specs=pl.BlockSpec(memory_space=vmem),
        scratch_shapes=[
            vmem((n,) + w_in.shape, BF16),
            vmem((n,) + w_out.shape, BF16),
            vmem((n,) + w_up.shape, BF16),
            vmem((n,) + w_dn.shape, BF16),
            vmem((nr, nt, seq, own_width), BF16),
            vmem((nr, nt, seq, own_width), BF16),
            vmem((n, nr * seq, depth), BF16),
            vmem((nr * seq, w_in.shape[1]), F32),
            vmem((nr, seq, w_out.shape[0]), BF16),
            vmem((nr, seq + 8, w_up.shape[1]), F32),
            vmem((nr, seq, w_dn.shape[0]), BF16),
            vmem((n, nr, seq, depth), BF16),
            vmem((n, nr, seq, depth), BF16),
            vmem((nr * nt, per, seq, depth), BF16),
            vmem((nr * nt, per, seq, depth), BF16),
            sem((4, 3, n)),
            sem((4, n)),
            sem((5,)),
            sem((2, others)),
            sem((2, others)),
            sem((2, n, nr)),
            sem((2, nr * nt, per)),
        ],
        compiler_params=pltpu.CompilerParams(
            collective_id=0, has_side_effects=True, vmem_limit_bytes=67043328
        ),
    )(*operands)


def plane_kernel(
    n, nr, nt,
    tok, mix_gain, w_u, w_v, norm_gain, mixw, bias, w_out, ffn_gain, w_gate, w_value, taps_g, taps_v, w_dn,
    out,
    g_in, g_out, g_up, g_dn, feat, feat2, mid, normed, uv, hidden, gv, act,
    row_scale, squares, part1, part2, inc1, inc2, got1, got2, raw_mix, mix_low, gain_v, bias_all, bias_col, tg, tv,
    l_sem, y_send, y_recv, z_send, z_recv, d_send, d_recv, s_local, s_send, s_recv,
    a_send, a_recv, f_send, r_send, i_recv, t_recv,
):
    rep, fs, tp = lax.axis_index("rep"), lax.axis_index("fs"), lax.axis_index("tp")
    seq, own_width = tok.shape
    ny, nz = 2, n // 2
    z, y = fs // ny, fs % ny
    per = n // nt
    width = own_width // per
    quarter = rep * ny + y
    other_quarter = rep * ny + 1 - y
    fs_y = z * ny + 1 - y
    home = rep == tp
    away = rep != tp
    cu, cf = g_out.shape[2], g_dn.shape[2]
    depth = w_u.shape[0]
    few = (max(1, per // 4), max(1, per // 2))
    feats = (feat, feat2)

    def both(*conditions):
        return functools.reduce(jnp.logical_and, conditions)

    barrier = pltpu.get_barrier_semaphore()
    greeted = [{"tp": 1 - tp}]
    greeted += [{"rep": 1 - rep, "tp": t} for t in range(nt)]
    greeted += [{"fs": fs_y, "tp": t} for t in range(nt)]
    greeted += [{"fs": lax.rem(z + k, nz) * ny + y} for k in range(1, nz)]

    def item(k, block, half):
        if k in (0, 2):
            rows = pl.ds(pl.multiple_of(block * depth, 128), depth)
            return (g_in if k == 0 else g_up).at[half, rows]
        if k == 1:
            return g_out.at[block, half]
        return g_dn.at[block, half]

    def pieces(k, which, block):
        whole = item(k, block, tp)
        if k in (0, 2):
            first, second, size = (w_u, w_v, cu) if k == 0 else (w_gate, w_value, cf)
            cols = pl.ds(pl.multiple_of(which * size, 128), size)
            return (
                (first.at[:, cols], whole.at[:, pl.ds(0, size)]),
                (second.at[:, cols], whole.at[:, pl.ds(size, size)]),
            )
        source, size = (w_out, cu) if k == 1 else (w_dn, cf)
        rows = pl.ds(pl.multiple_of(which * size, 128), size)
        return ((source.at[rows, :], whole),)

    def own_load(k):
        return [
            pltpu.make_async_copy(src, dst, l_sem.at[k, i])
            for i, (src, dst) in enumerate(pieces(k, quarter, fs))
        ]

    def across(k, block):
        return [
            pltpu.make_async_remote_copy(
                src_ref=src, dst_ref=dst, send_sem=y_send.at[k, i], recv_sem=y_recv.at[k, i],
                device_id={"fs": fs_y}, device_id_type=MESH,
            )
            for i, (src, dst) in enumerate(pieces(k, other_quarter, block))
        ]

    def z_copy(k, block, step):
        return pltpu.make_async_remote_copy(
            src_ref=item(k, block, tp), dst_ref=item(k, block, tp),
            send_sem=z_send.at[k, block, (step + 1) // 2], recv_sem=z_recv.at[k, block],
            device_id={"fs": fs + ny * step}, device_id_type=MESH,
        )

    def d_copy(k, block):
        return pltpu.make_async_remote_copy(
            src_ref=item(k, block, tp), dst_ref=item(k, block, tp),
            send_sem=d_send.at[k, block], recv_sem=d_recv.at[k, block],
            device_id={"tp": 1 - tp}, device_id_type=MESH,
        )

    def inside(step):
        return jnp.logical_and(z + step >= 0, z + step < nz)

    def spread(k, block):
        for step in (1, -1):
            @pl.when(inside(step))
            def _():
                z_copy(k, block, step).start()
        d_copy(k, block).start()

    def arrive(k, block):
        landing = item(k, block, tp)
        pltpu.make_async_remote_copy(
            src_ref=landing, dst_ref=landing, send_sem=z_send.at[k, block, 0],
            recv_sem=z_recv.at[k, block], device_id={"tp": 1 - tp}, device_id_type=MESH,
        ).wait_recv()
        d_copy(k, block).start()

    def cross_over(k):
        for copy in across(k, fs_y):
            copy.wait_recv()
        spread(k, fs_y)

    def relays(far):
        return [
            (sign, z - sign * far, jnp.logical_and(inside(sign), inside(-sign * far)))
            for sign in (1, -1)
        ]

    def relay(k, far, at):
        for sign, source, used in relays(far):
            @pl.when(used)
            def _():
                arrive(k, source * ny + at)
                z_copy(k, source * ny + at, sign).start()

    def relay_from(k, first, last):
        for far in range(first, last):
            for at in (y, 1 - y):
                relay(k, far, at)

    def relayed(source):
        up = jnp.logical_and(z > source, inside(1))
        down = jnp.logical_and(source > z, inside(-1))
        return jnp.logical_or(up, down)

    def need(k, block):
        source = block // ny
        @pl.when(jnp.logical_and(source != z, jnp.logical_not(relayed(source))))
        def _():
            arrive(k, block)

    def partner_wait(k, block):
        landing = item(k, block, 1 - tp)
        pltpu.make_async_remote_copy(
            src_ref=landing, dst_ref=landing, send_sem=d_send.at[k, block],
            recv_sem=d_recv.at[k, block], device_id={"tp": 1 - tp}, device_id_type=MESH,
        ).wait_recv()

    def order(i):
        near = jnp.minimum(z, nz - 1 - z)
        swing = z + ((i + 1) // 2) * (1 - 2 * (i % 2))
        rest = jnp.where(z < nz - 1 - z, i, nz - 1 - i)
        return jnp.where(i <= 2 * near, swing, rest)

    def plain_block(i):
        return order(i // ny) * ny + lax.rem(i, ny)

    small = [
        (mixw.at[pl.ds(quarter * raw_mix.shape[1], raw_mix.shape[1])], raw_mix.at[tp]),
        (norm_gain.at[:, pl.ds(pl.multiple_of(quarter * cu, 128), cu)], gain_v.at[tp]),
        (bias, bias_all.at[tp]),
        (taps_g.at[:, pl.ds(pl.multiple_of(quarter * cf, 128), cf)], tg.at[tp]),
        (taps_v.at[:, pl.ds(pl.multiple_of(quarter * cf, 128), cf)], tv.at[tp]),
    ]
    small_local = [
        pltpu.make_async_copy(src, dst, s_local.at[i]) for i, (src, dst) in enumerate(small)
    ]
    small_away = [
        pltpu.make_async_remote_copy(
            src_ref=src, dst_ref=dst, send_sem=s_send.at[i], recv_sem=s_recv.at[i],
            device_id={"tp": 1 - tp}, device_id_type=MESH,
        )
        for i, (src, dst) in enumerate(small)
    ]

    def ag_source(turn, i):
        if turn == 0:
            return tok.at[:, pl.ds(pl.multiple_of(i * width, 128), width)]
        return mid.at[i]

    def ag_copy(turn, i, way):
        block = tp * per + i
        device = ({"rep": 1 - rep, "tp": rep}, {"fs": fs_y, "tp": rep}, {"tp": 1 - tp})[way]
        return pltpu.make_async_remote_copy(
            src_ref=ag_source(turn, i), dst_ref=feats[turn].at[y, block],
            send_sem=a_send.at[turn, way, i], recv_sem=a_recv.at[turn, y, block],
            device_id=device, device_id_type=MESH,
        )

    def ag_send(turn, i):
        ag_copy(turn, i, 0).start()
        ag_copy(turn, i, 1).start()

        @pl.when(away)
        def _():
            ag_copy(turn, i, 2).start()

        @pl.when(home)
        def _():
            feats[turn][y, tp * per + i] = ag_source(turn, i)[...]

    def passed(turn, block):
        at = lax.rem(block, per)
        return jnp.logical_or(
            jnp.logical_and(home, at >= few[turn]), jnp.logical_and(away, at < few[turn])
        )

    def ag_pass(turn, block):
        slot = jnp.where(home, 1 - y, y)
        return pltpu.make_async_remote_copy(
            src_ref=feats[turn].at[slot, block], dst_ref=feats[turn].at[slot, block],
            send_sem=f_send.at[turn, block], recv_sem=a_recv.at[turn, slot, block],
            device_id={
                "rep": jnp.where(home, 1 - rep, rep),
                "fs": jnp.where(home, fs, fs_y),
            },
            device_id_type=MESH,
        )

    def ag_landed(turn, slot, block):
        landing = feats[turn].at[slot, block]
        pltpu.make_async_remote_copy(
            src_ref=landing, dst_ref=landing, send_sem=f_send.at[turn, 0],
            recv_sem=a_recv.at[turn, slot, block], device_id={"tp": 1 - tp}, device_id_type=MESH,
        ).wait_recv()

    def ag_forward(turn, block):
        @pl.when(passed(turn, block))
        def _():
            ag_landed(turn, jnp.where(home, 1 - y, y), block)
            ag_pass(turn, block).start()

    def ag_wait(turn, slot, block):
        local = both(home, slot == y, block // per == tp)
        sent_on = jnp.logical_and(passed(turn, block), slot == jnp.where(home, 1 - y, y))

        @pl.when(jnp.logical_not(jnp.logical_or(local, sent_on)))
        def _():
            ag_landed(turn, slot, block)

    def weigh(turn, gain, block):
        gains = gain[:, pl.ds(pl.multiple_of(block * width, 128), width)]
        for r in range(2):
            slot = lax.rem(y + r, 2)
            ag_wait(turn, slot, block)
            values = feats[turn][slot, block].astype(F32)
            rows = pl.ds(pl.multiple_of(slot * seq, 8), seq)
            normed[rows, pl.ds(pl.multiple_of(block * width, 128), width)] = (
                values * gains
            ).astype(BF16)
            for at in range(0, width, 128):
                piece = values[:, at : at + 128]
                squares[slot] += piece * piece

    def finish_scale():
        for slot in range(2):
            total = jnp.sum(squares[slot], axis=1, keepdims=True)
            row_scale[slot, 8:, :] = lax.rsqrt(total / (n * width) + EPS_RMS)

    def gathered_loop(k, turn, gain, multiply, lead, beside):
        def arrived(source, half):
            if half is tp:
                for at in range(ny):
                    weigh(turn, gain, source * ny + at)
                for at in (y, 1 - y):
                    need(k, source * ny + at)
            else:
                for at in (y, 1 - y):
                    partner_wait(k, source * ny + at)
            cols = pl.ds(pl.multiple_of(source * ny * depth, 128), ny * depth)
            multiply(cols, half)

        def step(i, _):
            if lead:
                @pl.when(i < nz)
                def _():
                    for at in range(ny):
                        ag_forward(turn, order(i) * ny + at)

            for at, action in beside:
                pl.when(i == at)(action)

            @pl.when(both(i >= lead, i < nz + lead))
            def _():
                arrived(order(i - lead), tp)

            @pl.when(i >= lead + 1)
            def _():
                arrived(order(i - lead - 1), 1 - tp)

            return 0

        lax.fori_loop(0, nz + lead + 1, step, 0)
        finish_scale()

    def even(block):
        return lax.rem(block, 2) == 0

    parts, incs, gots = (part1, part2), (inc1, inc2), (got1, got2)

    def r_copy(turn, r, block, kind):
        slot = lax.rem(y + r, 2)
        core, at = block // per, lax.rem(block, per)
        got, inc = gots[turn], incs[turn]
        dst, sem, device = {
            "diag_x": (inc.at[block], i_recv.at[turn, block], {"rep": 1 - rep}),
            "diag_y": (inc.at[block], i_recv.at[turn, block], {"fs": fs_y}),
            "pair": (got.at[0, at], t_recv.at[turn, 0, at], {"tp": 1 - tp}),
            "x": (got.at[1, at], t_recv.at[turn, 1, at], {"rep": 1 - rep, "tp": core}),
            "y": (got.at[2, at], t_recv.at[turn, 2, at], {"fs": fs_y, "tp": core}),
        }[kind]
        return pltpu.make_async_remote_copy(
            src_ref=parts[turn].at[slot, block], dst_ref=dst, send_sem=r_send.at[turn, r, block],
            recv_sem=sem, device_id=device, device_id_type=MESH,
        )

    def cases(block):
        return (
            (1, "diag_x", both(away, even(block)), True),
            (1, "diag_y", both(away, jnp.logical_not(even(block))), True),
            (1, "y", both(home, jnp.logical_not(even(block))), True),
            (0, "pair", both(home, block // per != tp), True),
            (0, "x", both(away, even(block)), True),
            (1, "y", both(home, even(block)), False),
            (0, "x", both(away, jnp.logical_not(even(block))), False),
        )

    def project(turn, left, weight, block):
        size = weight.shape[1] * weight.shape[2]
        right = weight[block].reshape(size, weight.shape[3])
        for r in (1, 0):
            slot = lax.rem(y + r, 2)
            parts[turn][slot, block] = jnp.dot(
                left[slot], right, preferred_element_type=F32
            ).astype(BF16)
            for row, kind, used, now in cases(block):
                if row == r and now:
                    @pl.when(used)
                    def _():
                        r_copy(turn, r, block, kind).start()

        @pl.when(both(home, block // per == tp))
        def _():
            gots[turn][0, lax.rem(block, per)] = parts[turn][y, block]

    def join(turn, block):
        for r, kind, used, now in cases(block):
            if not now:
                @pl.when(used)
                def _():
                    landing = incs[turn].at[block]
                    pltpu.make_async_remote_copy(
                        src_ref=landing, dst_ref=landing, send_sem=r_send.at[turn, 0, 0],
                        recv_sem=i_recv.at[turn, block], device_id={"rep": 1 - rep},
                        device_id_type=MESH,
                    ).wait_recv()
                    slot = lax.rem(y + r, 2)
                    parts[turn][slot, block] = (
                        parts[turn][slot, block].astype(F32) + incs[turn][block].astype(F32)
                    ).astype(BF16)
                    r_copy(turn, r, block, kind).start()

    def landed(turn, kind, at):
        landing = gots[turn].at[kind, at]
        pltpu.make_async_remote_copy(
            src_ref=landing, dst_ref=landing, send_sem=r_send.at[turn, 0, 0],
            recv_sem=t_recv.at[turn, kind, at], device_id={"rep": 1 - rep}, device_id_type=MESH,
        ).wait_recv()

    def collect(turn, block):
        at = lax.rem(block, per)

        @pl.when(away)
        def _():
            landed(turn, 0, at)

        landed(turn, 1, at)
        landed(turn, 2, at)
        got = gots[turn]
        total = got[0, at].astype(F32) + got[1, at].astype(F32) + got[2, at].astype(F32)
        cols = pl.ds(pl.multiple_of(at * width, 128), width)
        if turn == 0:
            mid[at] = (tok[:, cols].astype(F32) + total).astype(BF16)
            ag_send(1, at)
        else:
            out[:, cols] = (mid[at].astype(F32) + total).astype(BF16)

    def scatter_loop(k, turn, left, weight, beside):
        def step(i, _):
            @pl.when(i < n)
            def _():
                need(k, plain_block(i))

            @pl.when(both(i >= 1, i < n + 1))
            def _():
                block = plain_block(i - 1)
                partner_wait(k, block)
                project(turn, left, weight, block)

            @pl.when(both(i >= 3, i < n + 3))
            def _():
                join(turn, plain_block(i - 3))

            for at, action in beside:
                pl.when(i == at)(action)

            @pl.when(i >= 5)
            def _():
                block = plain_block(i - 5)

                @pl.when(block // per == tp)
                def _():
                    collect(turn, block)

            return 0

        lax.fori_loop(0, n + 5, step, 0)

    for k in range(4):
        for copy in own_load(k):
            copy.start()
    for copy in small_local:
        copy.start()
    for target in greeted:
        pl.semaphore_signal(barrier, inc=1, device_id=target, device_id_type=MESH)
    pl.semaphore_wait(barrier, len(greeted))

    for copy in across(0, fs):
        copy.start()
    for i in range(per):
        ag_send(0, i)
    for copy in own_load(0):
        copy.wait()
    spread(0, fs)
    for copy in across(1, fs) + small_away:
        copy.start()
    uv[...] = jnp.zeros_like(uv)
    gv[...] = jnp.zeros_like(gv)
    squares[...] = jnp.zeros_like(squares)
    row_scale[...] = jnp.zeros_like(row_scale)
    cross_over(0)
    for k in range(1, 4):
        for copy in own_load(k):
            copy.wait()
    turns = [(far, at) for far in range(1, nz - 1) for at in (y, 1 - y)]
    for i in range(max(per, len(turns))):
        if i < len(turns):
            relay(0, *turns[i])
        if i < per:
            for half in range(nt):
                ag_forward(0, half * per + i)
    spread(1, fs)
    cross_over(1)
    for k in (2, 3):
        for copy in across(k, fs):
            copy.start()

    def in_block(cols, half):
        uv[half] += jnp.dot(normed[:, cols], g_in[half, cols], preferred_element_type=F32)

    gathered_loop(0, 0, mix_gain, in_block, 0, ())
    relay_from(1, 1, 2)

    for copy in small_local:
        copy.wait()
    for i, (_, dst) in enumerate(small):
        landing = (raw_mix, gain_v, bias_all, tg, tv)[i].at[1 - tp]
        pltpu.make_async_remote_copy(
            src_ref=landing, dst_ref=landing, send_sem=s_send.at[i], recv_sem=s_recv.at[i],
            device_id={"tp": 1 - tp}, device_id_type=MESH,
        ).wait_recv()
    per_half, block_len = raw_mix.shape[1], raw_mix.shape[2]
    group_width = cu // per_half
    at_row = lax.broadcasted_iota(jnp.int32, (block_len, block_len), 0)
    at_col = lax.broadcasted_iota(jnp.int32, (block_len, block_len), 1)
    for half in range(nt):
        turned = bias_all[half].T
        lane = lax.broadcasted_iota(jnp.int32, turned.shape, 1)
        for g in range(per_half):
            mix_low[half, g] = jnp.where(
                at_row >= at_col, raw_mix[half, g].astype(F32), 0.0
            ).astype(BF16)
            bias_col[half, g] = jnp.sum(
                jnp.where(lane == quarter * per_half + g, turned, 0.0), axis=1, keepdims=True
            )

    for slot in range(2):
        def mix_rows(i, _):
            own_rows = pl.ds(pl.multiple_of(i * block_len, block_len), block_len)
            rows = pl.ds(pl.multiple_of(slot * seq + i * block_len, block_len), block_len)
            scale = row_scale[slot, pl.ds(pl.multiple_of(i * block_len + 8, 8), block_len), :]
            for half in range(nt):
                for g in range(per_half):
                    at = g * group_width
                    activated = jax.nn.gelu(
                        uv[half, rows, cu + at : cu + at + group_width] * scale
                    )
                    centred = activated - jnp.mean(activated, axis=1, keepdims=True)
                    spread_sq = jnp.mean(centred * centred, axis=1, keepdims=True)
                    v_norm = (
                        centred
                        * lax.rsqrt(spread_sq + EPS_LN)
                        * gain_v[half, :, at : at + group_width]
                    ).astype(BF16)
                    mixed = (
                        jnp.dot(mix_low[half, g], v_norm, preferred_element_type=F32)
                        + bias_col[half, g]
                    )
                    hidden[slot, own_rows, half * cu + at : half * cu + at + group_width] = (
                        jax.nn.gelu(uv[half, rows, at : at + group_width] * scale) * mixed
                    ).astype(BF16)
            return 0

        lax.fori_loop(0, seq // block_len, mix_rows, 0)

    relay_from(1, 2, nz - 1)
    spread(2, fs)
    cross_over(2)
    squares[...] = jnp.zeros_like(squares)

    def start_down():
        spread(3, fs)
        cross_over(3)

    hops = (
        (n // 2 + 1, lambda: relay(2, 1, y)),
        (n // 2 + 2, lambda: relay(2, 1, 1 - y)),
        (n, lambda: relay_from(2, 2, nz - 1)),
        (n + 3, start_down),
    )
    scatter_loop(1, 0, hidden, g_out, hops)

    def up_block(cols, half):
        product = jnp.dot(normed[:, cols], g_up[half, cols], preferred_element_type=F32)
        for slot in range(2):
            gv[half, slot, 8:, :] += product[slot * seq : (slot + 1) * seq]

    gathered_loop(2, 1, ffn_gain, up_block, 1, ((nz - 1, lambda: relay_from(3, 1, 2)),))

    taps_len = tg.shape[1]
    chunk = 128
    for slot in range(2):
        for half in range(nt):
            for at in range(0, cf, chunk):
                gate = jnp.zeros((seq, chunk), F32)
                value = jnp.zeros((seq, chunk), F32)
                for k in range(taps_len):
                    first = 8 - (taps_len - 1) + k
                    rows = slice(first, first + seq)
                    scale = row_scale[slot, rows, :]
                    gate += tg[half, k : k + 1, at : at + chunk].astype(F32) * (
                        gv[half, slot, rows, at : at + chunk] * scale
                    )
                    value += tv[half, k : k + 1, at : at + chunk].astype(F32) * (
                        gv[half, slot, rows, cf + at : cf + at + chunk] * scale
                    )
                act[slot, :, half * cf + at : half * cf + at + chunk] = (
                    jax.nn.gelu(gate) * value
                ).astype(BF16)

    relay_from(3, 2, nz - 1)
    scatter_loop(3, 1, act, g_dn, ())

    for k in range(4):
        for copy in across(k, fs):
            copy.wait_send()
    for copy in small_away:
        copy.wait_send()

    def drain_block(block, _):
        for k in range(4):
            d_copy(k, block).wait_send()
        for turn in range(2):
            for r, kind, used, _now in cases(block):
                @pl.when(used)
                def _():
                    r_copy(turn, r, block, kind).wait_send()

            @pl.when(passed(turn, block))
            def _():
                ag_pass(turn, block).wait_send()
        return 0

    lax.fori_loop(0, n, drain_block, 0)

    def drain_gather(i, _):
        for turn in range(2):
            ag_copy(turn, i, 0).wait_send()
            ag_copy(turn, i, 1).wait_send()

            @pl.when(away)
            def _():
                ag_copy(turn, i, 2).wait_send()
        return 0

    lax.fori_loop(0, per, drain_gather, 0)

    def drain_line(at, _):
        for k in range(4):
            for step in (1, -1):
                @pl.when(inside(step))
                def _():
                    z_copy(k, z * ny + at, step).wait_send()
            for far in range(1, nz - 1):
                for sign, source, used in relays(far):
                    @pl.when(used)
                    def _():
                        z_copy(k, source * ny + at, sign).wait_send()
        return 0

    lax.fori_loop(0, ny, drain_line, 0)


def on_plane(
    tokens,
    mix_gain,
    w_u,
    w_v,
    norm_gain,
    mix_weight,
    mix_bias,
    w_mix_out,
    ffn_gain,
    w_gate,
    w_value,
    taps_gate,
    taps_value,
    w_down,
):
    n, nr, nt = lax.axis_size("fs"), lax.axis_size("rep"), lax.axis_size("tp")
    seq, own_width = tokens.shape
    per = n // nt
    width = own_width // per
    depth = w_u.shape[0]
    share = nr * 2
    cu, cf = w_u.shape[1] // share, w_gate.shape[1] // share
    groups, block_len = mix_weight.shape[0], mix_weight.shape[1]
    taps_len = taps_gate.shape[0]
    vmem, sem, hbm = pltpu.VMEM, pltpu.SemaphoreType.DMA, pl.ANY
    operands = (
        (tokens, vmem),
        (mix_gain[None, :], vmem),
        (w_u, hbm),
        (w_v, hbm),
        (norm_gain[None, :], hbm),
        (mix_weight, hbm),
        (mix_bias, hbm),
        (w_mix_out, hbm),
        (ffn_gain[None, :], vmem),
        (w_gate, hbm),
        (w_value, hbm),
        (taps_gate, hbm),
        (taps_value, hbm),
        (w_down, hbm),
    )
    return pl.pallas_call(
        functools.partial(plane_kernel, n, nr, nt),
        out_shape=jax.ShapeDtypeStruct((seq, own_width), BF16),
        in_specs=[pl.BlockSpec(memory_space=space) for _, space in operands],
        out_specs=pl.BlockSpec(memory_space=vmem),
        scratch_shapes=[
            vmem((nt, n * depth, 2 * cu), BF16),
            vmem((n, nt, cu, width), BF16),
            vmem((nt, n * depth, 2 * cf), BF16),
            vmem((n, nt, cf, width), BF16),
            vmem((2, n, seq, width), BF16),
            vmem((2, n, seq, width), BF16),
            vmem((per, seq, width), BF16),
            vmem((2 * seq, n * width), BF16),
            vmem((nt, 2 * seq, 2 * cu), F32),
            vmem((2, seq, nt * cu), BF16),
            vmem((nt, 2, seq + 8, 2 * cf), F32),
            vmem((2, seq, nt * cf), BF16),
            vmem((2, seq + 8, 1), F32),
            vmem((2, seq, 128), F32),
            vmem((2, n, seq, width), BF16),
            vmem((2, n, seq, width), BF16),
            vmem((n, seq, width), BF16),
            vmem((n, seq, width), BF16),
            vmem((3, per, seq, width), BF16),
            vmem((3, per, seq, width), BF16),
            vmem((nt, groups // share, block_len, block_len), BF16),
            vmem((nt, groups // share, block_len, block_len), BF16),
            vmem((nt, 1, cu), F32),
            vmem((nt, groups, block_len), F32),
            vmem((nt, groups // share, block_len, 1), F32),
            vmem((nt, taps_len, cf), BF16),
            vmem((nt, taps_len, cf), BF16),
            sem((4, 2)),
            sem((4, 2)),
            sem((4, 2)),
            sem((4, n, 2)),
            sem((4, n)),
            sem((4, n)),
            sem((4, n)),
            sem((5,)),
            sem((5,)),
            sem((5,)),
            sem((2, 3, per)),
            sem((2, 2, n)),
            sem((2, n)),
            sem((2, 2, n)),
            sem((2, n)),
            sem((2, 3, per)),
        ],
        compiler_params=pltpu.CompilerParams(
            collective_id=0, has_side_effects=True, vmem_limit_bytes=67043328
        ),
    )(*(array for array, _ in operands))


def by_shape(*arrays):
    n, nr, nt = lax.axis_size("fs"), lax.axis_size("rep"), lax.axis_size("tp")
    groups, units = arrays[5].shape[0], arrays[9].shape[1]
    share = nr * 2
    fits = nr == 2 and nt == 2 and n % 2 == 0 and groups % share == 0 and units % (share * 128) == 0
    return on_plane(*arrays) if fits else on_device(*arrays)


def solution(mesh):
    placed = (
        P(("rep", "fs"), "tp"),
        P(),
        P("fs", "tp"),
        P("fs", "tp"),
        P("tp"),
        P("tp", None, None),
        P("tp", None),
        P("tp", "fs"),
        P(),
        P("fs", "tp"),
        P("fs", "tp"),
        P(None, "tp"),
        P(None, "tp"),
        P("tp", "fs"),
    )
    return jax.shard_map(
        by_shape, mesh=mesh, in_specs=placed, out_specs=P(("rep", "fs"), "tp"), check_vma=False
    )
```

```python
import functools

import jax
import jax.numpy as jnp
from jax import lax
from jax.experimental import pallas as pl
from jax.experimental.pallas import tpu as pltpu
from jax.sharding import PartitionSpec as P

EPS_RMS = 1e-06
EPS_LN = 1e-05
F32 = jnp.float32
BF16 = jnp.bfloat16
MESH = pl.DeviceIdType.MESH
STRAIGHT = (0, 1)


def own_half(array, axis):
    share = array.shape[axis] // lax.axis_size("rep")
    return lax.dynamic_slice_in_dim(array, lax.axis_index("rep") * share, share, axis)


def layer_kernel(
    n, nr, nt,
    tok, mix_gain, w_in, norm_gain, mixw, bias, w_out, ffn_gain, w_up, taps_g, taps_v, w_dn,
    out,
    g_in, g_out, g_up, g_dn, feat, feat2, normed, uv, hidden, gv, act, part1, part2, got1, got2,
    w_send, w_recv, w_local, f_send, f_recv, p_send, p_recv,
):
    rep, fs, tp = lax.axis_index("rep"), lax.axis_index("fs"), lax.axis_index("tp")
    seq, own_width = tok.shape
    nz = n // 2
    z, y = fs // 2, fs % 2
    per = n // nt
    depth = normed.shape[2]
    mine = (w_in, w_out, w_up, w_dn)
    gathered = (g_in, g_out, g_up, g_dn)
    offsets = [(a, b) for a in range(nr) for b in range(nt) if (a, b) != (0, 0)]

    def peer(a, b):
        return {"rep": lax.rem(rep + a, nr), "tp": lax.rem(tp + b, nt)}

    barrier = pltpu.get_barrier_semaphore()
    line = (lax.rem(z + 1, nz), lax.rem(z + nz - 1, nz))
    greeted = [{"fs": z * 2 + 1 - y}] + [{"fs": at * 2 + y} for at in line]
    greeted += [peer(a, b) for a, b in offsets]
    for target in greeted:
        pl.semaphore_signal(barrier, inc=1, device_id=target, device_id_type=MESH)
    pl.semaphore_wait(barrier, len(greeted))

    def hop(stage, block, way):
        target = (fs + 2, fs - 2, z * 2 + 1 - y)[way]
        return pltpu.make_async_remote_copy(
            src_ref=gathered[stage].at[block],
            dst_ref=gathered[stage].at[block],
            send_sem=w_send.at[stage, way, block],
            recv_sem=w_recv.at[stage, block],
            device_id={"fs": target},
            device_id_type=MESH,
        )

    def ways(src):
        return (
            jnp.logical_and(src <= z, z < nz - 1),
            jnp.logical_and(src >= z, z > 0),
        )

    def forward(stage, src):
        block = src * 2 + y
        hop(stage, block, 2).start()
        for way, used in enumerate(ways(src)):
            @pl.when(used)
            def _():
                hop(stage, block, way).start()

    def arrived(stage, block):
        hop(stage, block, 2).wait_recv()

    def order(i):
        near = jnp.minimum(z, nz - 1 - z)
        swing = z + ((i + 1) // 2) * (1 - 2 * (i % 2))
        rest = jnp.where(z < nz - 1 - z, i, nz - 1 - i)
        return jnp.where(i <= 2 * near, swing, rest)

    def stage_loop(stage, compute, begin, middle):
        def step(i, _):
            src = order(i)

            @pl.when(i > 0)
            def _():
                arrived(stage, src * 2 + y)
                forward(stage, src)

            compute(src * 2 + y)

            @pl.when(i > 0)
            def _():
                other = order(i - 1) * 2 + 1 - y
                arrived(stage, other)
                compute(other)

            return 0

        lax.fori_loop(begin, nz, step, 0)
        middle()
        last = order(nz - 1) * 2 + 1 - y
        arrived(stage, last)
        compute(last)

    locals_ = [
        pltpu.make_async_copy(mine[k], gathered[k].at[fs], w_local.at[k]) for k in range(4)
    ]
    own_tok = pltpu.make_async_copy(tok, feat.at[rep, tp], w_local.at[4])
    for copy in locals_ + [own_tok]:
        copy.start()

    def share(turn, slabs):
        copies = []
        for k, (a, b) in enumerate(offsets):
            copies.append(
                pltpu.make_async_remote_copy(
                    src_ref=slabs.at[rep, tp],
                    dst_ref=slabs.at[rep, tp],
                    send_sem=f_send.at[turn, k],
                    recv_sem=f_recv.at[turn, k],
                    device_id=peer(a, b),
                    device_id_type=MESH,
                )
            )
        return copies

    def share_wait(turn, slabs):
        for k, (a, b) in enumerate(offsets):
            slab = slabs.at[lax.rem(rep + nr - a, nr), lax.rem(tp + nt - b, nt)]
            pltpu.make_async_remote_copy(
                src_ref=slab, dst_ref=slab, send_sem=f_send.at[turn, k],
                recv_sem=f_recv.at[turn, k], device_id=peer(a, b), device_id_type=MESH,
            ).wait_recv()

    def norm(slabs, gain):
        for r in range(nr):
            total = jnp.zeros((seq, 1), F32)
            for t in range(nt):
                values = slabs[r, t].astype(F32)
                total += jnp.sum(values * values, axis=1, keepdims=True)
            scale = lax.rsqrt(total / (nt * own_width) + EPS_RMS)
            for t in range(nt):
                for j in range(per):
                    values = slabs[r, t, :, j * depth : (j + 1) * depth].astype(F32)
                    normed[t * per + j, r * seq : (r + 1) * seq, :] = (
                        values * scale * gain[t * per + j]
                    ).astype(BF16)

    def piece(turn, part, got, block, r):
        return pltpu.make_async_remote_copy(
            src_ref=part.at[block, r],
            dst_ref=got.at[rep * nt + tp, block % per],
            send_sem=p_send.at[turn, block, r],
            recv_sem=p_recv.at[turn, rep * nt + tp, block % per],
            device_id={"rep": r, "tp": block // per},
            device_id_type=MESH,
        )

    def abroad(block, r):
        return jnp.logical_or(block // per != tp, r != rep)

    def project(turn, left, gathered_w, part, got, block):
        for r in range(nr):
            part[block, r] = jnp.dot(
                left[r], gathered_w[block], preferred_element_type=F32
            ).astype(BF16)

            @pl.when(abroad(block, r))
            def _():
                piece(turn, part, got, block, r).start()

    def collect(turn, part, got, base, emit):
        for j in range(per):
            total = part[tp * per + j, rep].astype(F32)
            for a, b in offsets:
                slot = lax.rem(rep + a, nr) * nt + lax.rem(tp + b, nt)
                landing = got.at[slot, j]
                pltpu.make_async_remote_copy(
                    src_ref=landing, dst_ref=landing, send_sem=p_send.at[turn, 0, 0],
                    recv_sem=p_recv.at[turn, slot, j], device_id=peer(a, b),
                    device_id_type=MESH,
                ).wait_recv()
                total += got[slot, j].astype(F32)
            width = total.shape[1]
            span = slice(j * width, (j + 1) * width)
            emit(span, (base(span).astype(F32) + total).astype(BF16))

    for copy in locals_ + [own_tok]:
        copy.wait()
    for copy in share(0, feat):
        copy.start()
    forward(0, z)
    forward(1, z)
    forward(2, z)
    uv[...] = jnp.zeros_like(uv)
    gv[...] = jnp.zeros_like(gv)
    share_wait(0, feat)
    norm(feat, mix_gain)

    def in_block(block):
        for r in range(nr):
            rows = slice(r * seq, (r + 1) * seq)
            uv[rows, :] += jnp.dot(
                normed[block, rows, :], g_in[block], preferred_element_type=F32
            )

    stage_loop(0, in_block, 0, lambda: forward(3, z))

    groups, block_len = mixw.shape[0], mixw.shape[1]
    group_width = uv.shape[1] // 2 // groups

    for r in range(nr):
        def mix_rows(i, _):
            start = pl.multiple_of(i * block_len, block_len)
            rows = pl.ds(pl.multiple_of(r * seq + i * block_len, block_len), block_len)
            for g in range(groups):
                at = g * group_width
                half = groups * group_width
                activated = jax.nn.gelu(uv[rows, half + at : half + at + group_width])
                centred = activated - jnp.mean(activated, axis=1, keepdims=True)
                spread = jnp.mean(centred * centred, axis=1, keepdims=True)
                v_norm = (
                    centred * lax.rsqrt(spread + EPS_LN) * norm_gain[:, at : at + group_width]
                ).astype(BF16)
                mixed = jnp.dot(mixw[g], v_norm, preferred_element_type=F32) + bias[g]
                hidden[r, pl.ds(start, block_len), at : at + group_width] = (
                    jax.nn.gelu(uv[rows, at : at + group_width]) * mixed
                ).astype(BF16)
            return 0

        lax.fori_loop(0, seq // block_len, mix_rows, 0)

    stage_loop(
        1, functools.partial(project, 0, hidden, g_out, part1, got1), 0, lambda: None
    )

    def relay(stage, begin, end):
        def step(i, _):
            arrived(stage, order(i) * 2 + y)
            forward(stage, order(i))
            return 0

        lax.fori_loop(begin, end, step, 0)

    def put_middle(span, value):
        feat2[rep, tp, :, span] = value

    relay(2, 1, nz // 2)
    collect(0, part1, got1, lambda span: tok[:, span], put_middle)
    for copy in share(1, feat2):
        copy.start()
    relay(2, nz // 2, nz)
    share_wait(1, feat2)
    norm(feat2, ffn_gain)

    def up_block(block):
        for r in range(nr):
            gv[r, 8:, :] += jnp.dot(
                normed[block, r * seq : (r + 1) * seq, :],
                g_up[block],
                preferred_element_type=F32,
            )

    def up_step(i, _):
        up_block(order(i) * 2 + y)

        @pl.when(i > 0)
        def _():
            arrived(3, order(i) * 2 + y)
            forward(3, order(i))

        other = order(i) * 2 + 1 - y
        arrived(2, other)
        up_block(other)
        return 0

    lax.fori_loop(0, nz, up_step, 0)

    units = act.shape[2]
    taps_len = taps_g.shape[0]
    chunk = 128 if units % 128 == 0 else units
    for r in range(nr):
        for at in range(0, units, chunk):
            gate = jnp.zeros((seq, chunk), F32)
            value = jnp.zeros((seq, chunk), F32)
            for k in range(taps_len):
                first = 8 - (taps_len - 1) + k
                gate += taps_g[k : k + 1, at : at + chunk] * gv[r, first : first + seq, at : at + chunk]
                value += (
                    taps_v[k : k + 1, at : at + chunk]
                    * gv[r, first : first + seq, units + at : units + at + chunk]
                )
            act[r, :, at : at + chunk] = (jax.nn.gelu(gate) * value).astype(BF16)

    down = functools.partial(project, 1, act, g_dn, part2, got2)

    def down_own(i, _):
        down(order(i) * 2 + y)
        return 0

    def down_other(i, _):
        arrived(3, order(i) * 2 + 1 - y)
        down(order(i) * 2 + 1 - y)
        return 0

    lax.fori_loop(0, nz, down_own, 0)
    lax.fori_loop(0, nz, down_other, 0)

    def put_out(span, value):
        out[:, span] = value

    collect(1, part2, got2, lambda span: feat2[rep, tp, :, span], put_out)

    for turn, slabs in enumerate((feat, feat2)):
        for copy in share(turn, slabs):
            copy.wait_send()

    def drain_pieces(block, _):
        for r in range(nr):
            @pl.when(abroad(block, r))
            def _():
                piece(0, part1, got1, block, r).wait_send()
                piece(1, part2, got2, block, r).wait_send()
        return 0

    lax.fori_loop(0, n, drain_pieces, 0)

    def drain_hops(src, _):
        for stage in range(4):
            hop(stage, src * 2 + y, 2).wait_send()
            for way, used in enumerate(ways(src)):
                @pl.when(used)
                def _():
                    hop(stage, src * 2 + y, way).wait_send()
        return 0

    lax.fori_loop(0, nz, drain_hops, 0)


def on_device(
    tokens,
    mix_gain,
    w_u,
    w_v,
    norm_gain,
    mix_weight,
    mix_bias,
    w_mix_out,
    ffn_gain,
    w_gate,
    w_value,
    taps_gate,
    taps_value,
    w_down,
):
    n, nr, nt = lax.axis_size("fs"), lax.axis_size("rep"), lax.axis_size("tp")
    seq, own_width = tokens.shape
    depth, per = own_width * nt // n, n // nt
    block_len = mix_weight.shape[1]
    lower_mask = jnp.arange(block_len)[:, None] >= jnp.arange(block_len)[None, :]
    mixw = own_half(mix_weight, 0)
    mixw = jnp.where(lower_mask[None], mixw, jnp.zeros_like(mixw))
    w_in = jnp.concatenate((own_half(w_u, 1), own_half(w_v, 1)), 1)
    w_up = jnp.concatenate((own_half(w_gate, 1), own_half(w_value, 1)), 1)
    w_out, w_dn = own_half(w_mix_out, 0), own_half(w_down, 0)
    operands = (
        tokens,
        mix_gain.reshape(n, 1, depth),
        w_in,
        own_half(norm_gain, 0)[None, :],
        mixw,
        own_half(mix_bias, 0)[:, :, None],
        w_out,
        ffn_gain.reshape(n, 1, depth),
        w_up,
        own_half(taps_gate, 1).astype(F32),
        own_half(taps_value, 1).astype(F32),
        w_dn,
    )
    vmem, sem = pltpu.VMEM, pltpu.SemaphoreType.DMA
    others = nr * nt - 1
    return pl.pallas_call(
        functools.partial(layer_kernel, n, nr, nt),
        out_shape=jax.ShapeDtypeStruct((seq, own_width), BF16),
        in_specs=[pl.BlockSpec(memory_space=vmem)] * len(operands),
        out_specs=pl.BlockSpec(memory_space=vmem),
        scratch_shapes=[
            vmem((n,) + w_in.shape, BF16),
            vmem((n,) + w_out.shape, BF16),
            vmem((n,) + w_up.shape, BF16),
            vmem((n,) + w_dn.shape, BF16),
            vmem((nr, nt, seq, own_width), BF16),
            vmem((nr, nt, seq, own_width), BF16),
            vmem((n, nr * seq, depth), BF16),
            vmem((nr * seq, w_in.shape[1]), F32),
            vmem((nr, seq, w_out.shape[0]), BF16),
            vmem((nr, seq + 8, w_up.shape[1]), F32),
            vmem((nr, seq, w_dn.shape[0]), BF16),
            vmem((n, nr, seq, depth), BF16),
            vmem((n, nr, seq, depth), BF16),
            vmem((nr * nt, per, seq, depth), BF16),
            vmem((nr * nt, per, seq, depth), BF16),
            sem((4, 3, n)),
            sem((4, n)),
            sem((5,)),
            sem((2, others)),
            sem((2, others)),
            sem((2, n, nr)),
            sem((2, nr * nt, per)),
        ],
        compiler_params=pltpu.CompilerParams(
            collective_id=0, has_side_effects=True, vmem_limit_bytes=67043328
        ),
    )(*operands)


def plane_kernel(
    n, nr, nt,
    tok_hbm, mix_gain_hbm, w_u, w_v, norm_gain, mixw, bias, w_out, ffn_gain_hbm, w_gate, w_value, taps_g, taps_v, w_dn,
    out_hbm,
    tok, out, mix_gain, ffn_gain, g_in, g_out, g_up, g_dn, feat, feat2, mid, normed, uv, hidden, gv, act,
    row_scale, squares, extra, part1, part2, inc1, inc2, got1, got2, raw_mix, mix_low, gain_v, bias_all, bias_col, tg, tv,
    t_sem, o_sem, n_sem, l_sem, y_send, y_recv, z_send, z_recv, d_send, d_recv, s_local, s_send, s_recv,
    a_send, a_recv, f_send, r_send, i_recv, t_recv,
):
    rep, fs, tp = lax.axis_index("rep"), lax.axis_index("fs"), lax.axis_index("tp")
    seq, own_width = tok_hbm.shape
    ny, nz = 2, n // 2
    z, y = fs // ny, fs % ny
    per = n // nt
    width = own_width // per
    quarter = rep * ny + y
    other_quarter = rep * ny + 1 - y
    fs_y = z * ny + 1 - y
    home = rep == tp
    away = rep != tp
    cu, cf = g_out.shape[2], g_dn.shape[2]
    depth = w_u.shape[0]
    few = (max(1, per // 4), max(1, per // 2))
    feats = (feat, feat2)

    def both(*conditions):
        return functools.reduce(jnp.logical_and, conditions)

    barrier = pltpu.get_barrier_semaphore()
    greeted = [{"tp": 1 - tp}]
    greeted += [{"rep": 1 - rep, "tp": t} for t in range(nt)]
    greeted += [{"fs": fs_y, "tp": t} for t in range(nt)]
    greeted += [{"rep": 1 - rep, "fs": fs_y, "tp": t} for t in range(nt)]
    greeted += [{"fs": lax.rem(z + k, nz) * ny + y} for k in range(1, nz)]

    def item(k, block, half):
        if k in (0, 2):
            rows = pl.ds(pl.multiple_of(block * depth, 128), depth)
            return (g_in if k == 0 else g_up).at[half, rows]
        if k == 1:
            return g_out.at[block, half]
        return g_dn.at[block, half]

    def pieces(k, which, block):
        whole = item(k, block, tp)
        if k in (0, 2):
            first, second, size = (w_u, w_v, cu) if k == 0 else (w_gate, w_value, cf)
            cols = pl.ds(pl.multiple_of(which * size, 128), size)
            return (
                (first.at[:, cols], whole.at[:, pl.ds(0, size)]),
                (second.at[:, cols], whole.at[:, pl.ds(size, size)]),
            )
        source, size = (w_out, cu) if k == 1 else (w_dn, cf)
        rows = pl.ds(pl.multiple_of(which * size, 128), size)
        return ((source.at[rows, :], whole),)

    def own_load(k):
        return [
            pltpu.make_async_copy(src, dst, l_sem.at[k, i])
            for i, (src, dst) in enumerate(pieces(k, quarter, fs))
        ]

    def across(k, block):
        return [
            pltpu.make_async_remote_copy(
                src_ref=src, dst_ref=dst, send_sem=y_send.at[k, i], recv_sem=y_recv.at[k, i],
                device_id={"fs": fs_y}, device_id_type=MESH,
            )
            for i, (src, dst) in enumerate(pieces(k, other_quarter, block))
        ]

    def z_copy(k, block, step):
        return pltpu.make_async_remote_copy(
            src_ref=item(k, block, tp), dst_ref=item(k, block, tp),
            send_sem=z_send.at[k, block, (step + 1) // 2], recv_sem=z_recv.at[k, block],
            device_id={"fs": fs + ny * step}, device_id_type=MESH,
        )

    def d_copy(k, block):
        return pltpu.make_async_remote_copy(
            src_ref=item(k, block, tp), dst_ref=item(k, block, tp),
            send_sem=d_send.at[k, block], recv_sem=d_recv.at[k, block],
            device_id={"tp": 1 - tp}, device_id_type=MESH,
        )

    def inside(step):
        return jnp.logical_and(z + step >= 0, z + step < nz)

    def spread(k, block):
        for step in (1, -1):
            @pl.when(inside(step))
            def _():
                z_copy(k, block, step).start()
        d_copy(k, block).start()

    def arrive(k, block):
        landing = item(k, block, tp)
        pltpu.make_async_remote_copy(
            src_ref=landing, dst_ref=landing, send_sem=z_send.at[k, block, 0],
            recv_sem=z_recv.at[k, block], device_id={"tp": 1 - tp}, device_id_type=MESH,
        ).wait_recv()
        d_copy(k, block).start()

    def cross_over(k):
        for copy in across(k, fs_y):
            copy.wait_recv()
        spread(k, fs_y)

    def relays(far):
        return [
            (sign, z - sign * far, jnp.logical_and(inside(sign), inside(-sign * far)))
            for sign in (1, -1)
        ]

    def relay(k, far, at):
        for sign, source, used in relays(far):
            @pl.when(used)
            def _():
                arrive(k, source * ny + at)
                z_copy(k, source * ny + at, sign).start()

    def relay_from(k, first, last):
        for far in range(first, last):
            for at in range(ny):
                relay(k, far, at)

    def relayed(source):
        up = jnp.logical_and(z > source, inside(1))
        down = jnp.logical_and(source > z, inside(-1))
        return jnp.logical_or(up, down)

    def need(k, block):
        source = block // ny
        @pl.when(jnp.logical_and(source != z, jnp.logical_not(relayed(source))))
        def _():
            arrive(k, block)

    def partner_wait(k, block):
        landing = item(k, block, 1 - tp)
        pltpu.make_async_remote_copy(
            src_ref=landing, dst_ref=landing, send_sem=d_send.at[k, block],
            recv_sem=d_recv.at[k, block], device_id={"tp": 1 - tp}, device_id_type=MESH,
        ).wait_recv()

    def order(i):
        near = jnp.minimum(z, nz - 1 - z)
        swing = z + ((i + 1) // 2) * (1 - 2 * (i % 2))
        rest = jnp.where(z < nz - 1 - z, i, nz - 1 - i)
        return jnp.where(i <= 2 * near, swing, rest)

    def plain_block(i):
        return order(i // ny) * ny + lax.rem(i, ny)

    small = [
        (mixw.at[pl.ds(quarter * raw_mix.shape[1], raw_mix.shape[1])], raw_mix.at[tp]),
        (norm_gain.at[:, pl.ds(pl.multiple_of(quarter * cu, 128), cu)], gain_v.at[tp]),
        (bias, bias_all.at[tp]),
        (taps_g.at[:, pl.ds(pl.multiple_of(quarter * cf, 128), cf)], tg.at[tp]),
        (taps_v.at[:, pl.ds(pl.multiple_of(quarter * cf, 128), cf)], tv.at[tp]),
    ]
    small_local = [
        pltpu.make_async_copy(src, dst, s_local.at[i]) for i, (src, dst) in enumerate(small)
    ]
    small_away = [
        pltpu.make_async_remote_copy(
            src_ref=src, dst_ref=dst, send_sem=s_send.at[i], recv_sem=s_recv.at[i],
            device_id={"tp": 1 - tp}, device_id_type=MESH,
        )
        for i, (src, dst) in enumerate(small)
    ]

    def columns(i):
        return pl.ds(pl.multiple_of(i * width, 128), width)

    def tok_load(i):
        return pltpu.make_async_copy(tok_hbm.at[:, columns(i)], tok.at[i], t_sem.at[i])

    def out_store(i):
        return pltpu.make_async_copy(out.at[i], out_hbm.at[:, columns(i)], o_sem.at[i])

    def ag_source(turn, i):
        return (tok, mid)[turn].at[i]

    def ag_copy(turn, i, way):
        block = tp * per + i
        device = ({"rep": 1 - rep, "tp": rep}, {"fs": fs_y, "tp": rep}, {"tp": 1 - tp})[way]
        return pltpu.make_async_remote_copy(
            src_ref=ag_source(turn, i), dst_ref=feats[turn].at[y, block],
            send_sem=a_send.at[turn, way, i], recv_sem=a_recv.at[turn, y, block],
            device_id=device, device_id_type=MESH,
        )

    def ag_send(turn, i):
        ag_copy(turn, i, 0).start()
        ag_copy(turn, i, 1).start()

        @pl.when(away)
        def _():
            ag_copy(turn, i, 2).start()

        @pl.when(home)
        def _():
            feats[turn][y, tp * per + i] = ag_source(turn, i)[...]

    def passed(turn, block):
        at = lax.rem(block, per)
        return jnp.logical_or(
            jnp.logical_and(home, at >= few[turn]), jnp.logical_and(away, at < few[turn])
        )

    def ag_pass(turn, block):
        slot = jnp.where(home, 1 - y, y)
        return pltpu.make_async_remote_copy(
            src_ref=feats[turn].at[slot, block], dst_ref=feats[turn].at[slot, block],
            send_sem=f_send.at[turn, block], recv_sem=a_recv.at[turn, slot, block],
            device_id={
                "rep": jnp.where(home, 1 - rep, rep),
                "fs": jnp.where(home, fs, fs_y),
            },
            device_id_type=MESH,
        )

    def ag_landed(turn, slot, block):
        landing = feats[turn].at[slot, block]
        pltpu.make_async_remote_copy(
            src_ref=landing, dst_ref=landing, send_sem=f_send.at[turn, 0],
            recv_sem=a_recv.at[turn, slot, block], device_id={"tp": 1 - tp}, device_id_type=MESH,
        ).wait_recv()

    def ag_forward(turn, block):
        @pl.when(passed(turn, block))
        def _():
            ag_landed(turn, jnp.where(home, 1 - y, y), block)
            ag_pass(turn, block).start()

    def ag_wait(turn, slot, block):
        local = both(home, slot == y, block // per == tp)
        sent_on = jnp.logical_and(passed(turn, block), slot == jnp.where(home, 1 - y, y))

        @pl.when(jnp.logical_not(jnp.logical_or(local, sent_on)))
        def _():
            ag_landed(turn, slot, block)

    def weigh(turn, gain, block):
        gains = gain[:, pl.ds(pl.multiple_of(block * width, 128), width)]
        for r in range(2):
            slot = lax.rem(y + r, 2)
            ag_wait(turn, slot, block)
            values = feats[turn][slot, block].astype(F32)
            rows = pl.ds(pl.multiple_of(slot * seq, 8), seq)
            normed[rows, pl.ds(pl.multiple_of(block * width, 128), width)] = (
                values * gains
            ).astype(BF16)
            for at in range(0, width, 128):
                piece = values[:, at : at + 128]
                squares[slot] += piece * piece

    def finish_scale():
        for slot in range(2):
            total = jnp.sum(squares[slot], axis=1, keepdims=True)
            row_scale[slot, 8:, :] = lax.rsqrt(total / (n * width) + EPS_RMS)

    def gathered_loop(k, turn, gain, multiply, lead, beside):
        def arrived(source, half):
            if half is tp:
                for at in range(ny):
                    weigh(turn, gain, source * ny + at)
                for at in (y, 1 - y):
                    need(k, source * ny + at)
            else:
                for at in (y, 1 - y):
                    partner_wait(k, source * ny + at)
            cols = pl.ds(pl.multiple_of(source * ny * depth, 128), ny * depth)
            multiply(cols, half)

        def step(i, _):
            if lead:
                @pl.when(i < nz)
                def _():
                    for at in range(ny):
                        ag_forward(turn, order(i) * ny + at)

            for at, action in beside:
                pl.when(i == at)(action)

            @pl.when(both(i >= lead, i < nz + lead))
            def _():
                arrived(order(i - lead), tp)

            @pl.when(i >= lead + 1)
            def _():
                arrived(order(i - lead - 1), 1 - tp)

            return 0

        lax.fori_loop(0, nz + lead + 1, step, 0)
        finish_scale()

    def even(block):
        return lax.rem(block, 2) == 0

    parts, incs, gots = (part1, part2), (inc1, inc2), (got1, got2)

    def r_copy(turn, r, block, kind):
        slot = lax.rem(y + r, 2)
        core, at = block // per, lax.rem(block, per)
        got, inc = gots[turn], incs[turn]
        dst, sem, device = {
            "diag_x": (inc.at[block], i_recv.at[turn, block], {"rep": 1 - rep}),
            "diag_y": (inc.at[block], i_recv.at[turn, block], {"fs": fs_y}),
            "pair": (got.at[0, at], t_recv.at[turn, 0, at], {"tp": 1 - tp}),
            "x": (got.at[1, at], t_recv.at[turn, 1, at], {"rep": 1 - rep, "tp": core}),
            "y": (got.at[2, at], t_recv.at[turn, 2, at], {"fs": fs_y, "tp": core}),
            "diag": (
                got.at[3, at], t_recv.at[turn, 3, at],
                {"rep": 1 - rep, "fs": fs_y, "tp": core},
            ),
        }[kind]
        return pltpu.make_async_remote_copy(
            src_ref=parts[turn].at[slot, block], dst_ref=dst, send_sem=r_send.at[turn, r, block],
            recv_sem=sem, device_id=device, device_id_type=MESH,
        )

    def straight(turn, block):
        hit = block == plain_block(n - 1)
        for i in range(n - STRAIGHT[turn], n - 1):
            hit = jnp.logical_or(hit, block == plain_block(i))
        return hit if STRAIGHT[turn] else block < 0

    def cases(turn, block):
        once = straight(turn, block)
        twice = jnp.logical_not(once)
        is_even = even(block)
        is_odd = jnp.logical_not(is_even)
        return (
            (1, "diag_x", both(away, twice, is_even), True),
            (1, "diag_y", both(away, twice, is_odd), True),
            (1, "diag", both(away, once), True),
            (1, "y", both(home, jnp.logical_or(once, is_odd)), True),
            (0, "pair", both(home, block // per != tp), True),
            (0, "x", both(away, jnp.logical_or(once, is_even)), True),
            (1, "y", both(home, twice, is_even), False),
            (0, "x", both(away, twice, is_odd), False),
        )

    def project(turn, left, weight, block, r):
        size = weight.shape[1] * weight.shape[2]
        right = weight[block].reshape(size, weight.shape[3])
        slot = lax.rem(y + r, 2)
        parts[turn][slot, block] = jnp.dot(
            left[slot], right, preferred_element_type=F32
        ).astype(BF16)
        for row, kind, used, now in cases(turn, block):
            if row == r and now:
                @pl.when(used)
                def _():
                    r_copy(turn, r, block, kind).start()

        if r == 0:
            @pl.when(both(home, block // per == tp))
            def _():
                gots[turn][0, lax.rem(block, per)] = parts[turn][y, block]

    def scatter_early(k, turn, left, weight, count):
        for i in range(count):
            need(k, plain_block(i))
        for i in range(count):
            partner_wait(k, plain_block(i))
            project(turn, left, weight, plain_block(i), 1)

    def join(turn, block):
        for r, kind, used, now in cases(turn, block):
            if not now:
                @pl.when(used)
                def _():
                    landing = incs[turn].at[block]
                    pltpu.make_async_remote_copy(
                        src_ref=landing, dst_ref=landing, send_sem=r_send.at[turn, 0, 0],
                        recv_sem=i_recv.at[turn, block], device_id={"rep": 1 - rep},
                        device_id_type=MESH,
                    ).wait_recv()
                    slot = lax.rem(y + r, 2)
                    parts[turn][slot, block] = (
                        parts[turn][slot, block].astype(F32) + incs[turn][block].astype(F32)
                    ).astype(BF16)
                    r_copy(turn, r, block, kind).start()

    def landed(turn, kind, at):
        landing = gots[turn].at[kind, at]
        pltpu.make_async_remote_copy(
            src_ref=landing, dst_ref=landing, send_sem=r_send.at[turn, 0, 0],
            recv_sem=t_recv.at[turn, kind, at], device_id={"rep": 1 - rep}, device_id_type=MESH,
        ).wait_recv()

    def collect(turn, block):
        at = lax.rem(block, per)

        @pl.when(away)
        def _():
            landed(turn, 0, at)

        landed(turn, 1, at)
        landed(turn, 2, at)
        got = gots[turn]
        total = got[0, at].astype(F32) + got[1, at].astype(F32) + got[2, at].astype(F32)
        if STRAIGHT[turn]:
            once = straight(turn, block)

            @pl.when(once)
            def _():
                landed(turn, 3, at)
                extra[...] = got[3, at].astype(F32)

            @pl.when(jnp.logical_not(once))
            def _():
                extra[...] = jnp.zeros_like(extra)

            total += extra[...]
        if turn == 0:
            mid[at] = (tok[at].astype(F32) + total).astype(BF16)
            ag_send(1, at)
        else:
            out[at] = (mid[at].astype(F32) + total).astype(BF16)
            out_store(at).start()

    def scatter_loop(k, turn, left, weight, early, lags, beside):
        join_lag, collect_lag = lags

        def step(i, _):
            @pl.when(both(i >= early, i < n))
            def _():
                need(k, plain_block(i))

            @pl.when(both(i >= join_lag, i < n + join_lag))
            def _():
                join(turn, plain_block(i - join_lag))

            @pl.when(i < n)
            def _():
                block = plain_block(i)

                @pl.when(i >= early)
                def _():
                    partner_wait(k, block)
                    project(turn, left, weight, block, 1)

                project(turn, left, weight, block, 0)

            for at, action in beside:
                pl.when(i == at)(action)

            @pl.when(i >= collect_lag)
            def _():
                block = plain_block(i - collect_lag)

                @pl.when(block // per == tp)
                def _():
                    collect(turn, block)

            return 0

        lax.fori_loop(0, n + collect_lag, step, 0)

    gain_loads = [
        pltpu.make_async_copy(mix_gain_hbm, mix_gain, n_sem.at[0]),
        pltpu.make_async_copy(ffn_gain_hbm, ffn_gain, n_sem.at[1]),
    ]
    for i in range(per):
        tok_load(i).start()
    for k in range(4):
        for copy in own_load(k):
            copy.start()
    for copy in small_local + gain_loads:
        copy.start()
    for target in greeted:
        pl.semaphore_signal(barrier, inc=1, device_id=target, device_id_type=MESH)
    pl.semaphore_wait(barrier, len(greeted))

    for copy in across(0, fs):
        copy.start()
    for i in range(per):
        tok_load(i).wait()
        ag_send(0, i)
    for k in range(2):
        for copy in own_load(k):
            copy.wait()
        spread(k, fs)
    for copy in across(1, fs) + small_away:
        copy.start()
    uv[...] = jnp.zeros_like(uv)
    gv[...] = jnp.zeros_like(gv)
    squares[...] = jnp.zeros_like(squares)
    row_scale[...] = jnp.zeros_like(row_scale)
    cross_over(0)
    for k in range(2, 4):
        for copy in own_load(k):
            copy.wait()
    for copy in gain_loads:
        copy.wait()
    turns = [(far, at) for far in range(1, nz - 1) for at in (y, 1 - y)]
    for i in range(max(per, len(turns))):
        if i < len(turns):
            relay(0, *turns[i])
        if i < per:
            for half in range(nt):
                ag_forward(0, half * per + i)
    cross_over(1)
    for k in (2, 3):
        for copy in across(k, fs):
            copy.start()

    def in_block(cols, half):
        uv[half] += jnp.dot(normed[:, cols], g_in[half, cols], preferred_element_type=F32)

    hops = ((nz // 2, lambda: relay(1, 1, 0)), (nz // 2 + 1, lambda: relay(1, 1, 1)))
    gathered_loop(0, 0, mix_gain, in_block, 0, hops)

    for copy in small_local:
        copy.wait()
    for i, (_, dst) in enumerate(small):
        landing = (raw_mix, gain_v, bias_all, tg, tv)[i].at[1 - tp]
        pltpu.make_async_remote_copy(
            src_ref=landing, dst_ref=landing, send_sem=s_send.at[i], recv_sem=s_recv.at[i],
            device_id={"tp": 1 - tp}, device_id_type=MESH,
        ).wait_recv()
    per_half, block_len = raw_mix.shape[1], raw_mix.shape[2]
    group_width = cu // per_half
    at_row = lax.broadcasted_iota(jnp.int32, (block_len, block_len), 0)
    at_col = lax.broadcasted_iota(jnp.int32, (block_len, block_len), 1)
    for half in range(nt):
        turned = bias_all[half].T
        lane = lax.broadcasted_iota(jnp.int32, turned.shape, 1)
        for g in range(per_half):
            mix_low[half, g] = jnp.where(
                at_row >= at_col, raw_mix[half, g].astype(F32), 0.0
            ).astype(BF16)
            bias_col[half, g] = jnp.sum(
                jnp.where(lane == quarter * per_half + g, turned, 0.0), axis=1, keepdims=True
            )

    for slot in range(2):
        def mix_rows(i, _):
            own_rows = pl.ds(pl.multiple_of(i * block_len, block_len), block_len)
            rows = pl.ds(pl.multiple_of(slot * seq + i * block_len, block_len), block_len)
            scale = row_scale[slot, pl.ds(pl.multiple_of(i * block_len + 8, 8), block_len), :]
            for half in range(nt):
                for g in range(per_half):
                    at = g * group_width
                    activated = jax.nn.gelu(
                        uv[half, rows, cu + at : cu + at + group_width] * scale
                    )
                    centred = activated - jnp.mean(activated, axis=1, keepdims=True)
                    spread_sq = jnp.mean(centred * centred, axis=1, keepdims=True)
                    v_norm = (
                        centred
                        * lax.rsqrt(spread_sq + EPS_LN)
                        * gain_v[half, :, at : at + group_width]
                    ).astype(BF16)
                    mixed = (
                        jnp.dot(mix_low[half, g], v_norm, preferred_element_type=F32)
                        + bias_col[half, g]
                    )
                    hidden[slot, own_rows, half * cu + at : half * cu + at + group_width] = (
                        jax.nn.gelu(uv[half, rows, at : at + group_width] * scale) * mixed
                    ).astype(BF16)
            return 0

        lax.fori_loop(0, seq // block_len, mix_rows, 0)

    def start_both(k):
        @pl.when(y == 0)
        def _():
            spread(k, fs)
            cross_over(k)

        @pl.when(y == 1)
        def _():
            cross_over(k)
            spread(k, fs)

    relay_from(1, 2, nz - 1)
    start_both(2)
    squares[...] = jnp.zeros_like(squares)

    hops = (
        (n // 2 + 2, lambda: relay(2, 1, 0)),
        (n, lambda: relay(2, 1, 1)),
        (n + 4, lambda: relay_from(2, 2, nz - 1)),
        (n + 5, lambda: start_both(3)),
    )
    scatter_loop(1, 0, hidden, g_out, 0, (3, 6), hops)

    def up_block(cols, half):
        product = jnp.dot(normed[:, cols], g_up[half, cols], preferred_element_type=F32)
        for slot in range(2):
            gv[half, slot, 8:, :] += product[slot * seq : (slot + 1) * seq]

    gathered_loop(2, 1, ffn_gain, up_block, 1, ((nz - 1, lambda: relay_from(3, 1, 2)),))

    taps_len = tg.shape[1]
    chunk = 128

    def convolve(slot):
        for half in range(nt):
            for at in range(0, cf, chunk):
                gate = jnp.zeros((seq, chunk), F32)
                value = jnp.zeros((seq, chunk), F32)
                for k in range(taps_len):
                    first = 8 - (taps_len - 1) + k
                    rows = slice(first, first + seq)
                    scale = row_scale[slot, rows, :]
                    gate += tg[half, k : k + 1, at : at + chunk].astype(F32) * (
                        gv[half, slot, rows, at : at + chunk] * scale
                    )
                    value += tv[half, k : k + 1, at : at + chunk].astype(F32) * (
                        gv[half, slot, rows, cf + at : cf + at + chunk] * scale
                    )
                act[slot, :, half * cf + at : half * cf + at + chunk] = (
                    jax.nn.gelu(gate) * value
                ).astype(BF16)

    convolve(1 - y)
    scatter_early(3, 1, act, g_dn, ny)
    convolve(y)
    relay_from(3, 2, nz - 1)
    scatter_loop(3, 1, act, g_dn, ny, (2, 4), ())

    for i in range(per):
        out_store(i).wait()
    for k in range(4):
        for copy in across(k, fs):
            copy.wait_send()
    for copy in small_away:
        copy.wait_send()

    def drain_block(block, _):
        for k in range(4):
            d_copy(k, block).wait_send()
        for turn in range(2):
            for r, kind, used, _now in cases(turn, block):
                @pl.when(used)
                def _():
                    r_copy(turn, r, block, kind).wait_send()

            @pl.when(passed(turn, block))
            def _():
                ag_pass(turn, block).wait_send()
        return 0

    lax.fori_loop(0, n, drain_block, 0)

    def drain_gather(i, _):
        for turn in range(2):
            ag_copy(turn, i, 0).wait_send()
            ag_copy(turn, i, 1).wait_send()

            @pl.when(away)
            def _():
                ag_copy(turn, i, 2).wait_send()
        return 0

    lax.fori_loop(0, per, drain_gather, 0)

    def drain_line(at, _):
        for k in range(4):
            for step in (1, -1):
                @pl.when(inside(step))
                def _():
                    z_copy(k, z * ny + at, step).wait_send()
            for far in range(1, nz - 1):
                for sign, source, used in relays(far):
                    @pl.when(used)
                    def _():
                        z_copy(k, source * ny + at, sign).wait_send()
        return 0

    lax.fori_loop(0, ny, drain_line, 0)


def on_plane(
    tokens,
    mix_gain,
    w_u,
    w_v,
    norm_gain,
    mix_weight,
    mix_bias,
    w_mix_out,
    ffn_gain,
    w_gate,
    w_value,
    taps_gate,
    taps_value,
    w_down,
):
    n, nr, nt = lax.axis_size("fs"), lax.axis_size("rep"), lax.axis_size("tp")
    seq, own_width = tokens.shape
    per = n // nt
    width = own_width // per
    depth = w_u.shape[0]
    share = nr * 2
    cu, cf = w_u.shape[1] // share, w_gate.shape[1] // share
    groups, block_len = mix_weight.shape[0], mix_weight.shape[1]
    taps_len = taps_gate.shape[0]
    vmem, sem, hbm = pltpu.VMEM, pltpu.SemaphoreType.DMA, pl.ANY
    operands = (
        (tokens, hbm),
        (mix_gain[None, :], hbm),
        (w_u, hbm),
        (w_v, hbm),
        (norm_gain[None, :], hbm),
        (mix_weight, hbm),
        (mix_bias, hbm),
        (w_mix_out, hbm),
        (ffn_gain[None, :], hbm),
        (w_gate, hbm),
        (w_value, hbm),
        (taps_gate, hbm),
        (taps_value, hbm),
        (w_down, hbm),
    )
    return pl.pallas_call(
        functools.partial(plane_kernel, n, nr, nt),
        out_shape=jax.ShapeDtypeStruct((seq, own_width), BF16),
        in_specs=[pl.BlockSpec(memory_space=space) for _, space in operands],
        out_specs=pl.BlockSpec(memory_space=hbm),
        scratch_shapes=[
            vmem((per, seq, width), BF16),
            vmem((per, seq, width), BF16),
            vmem((1, n * width), F32),
            vmem((1, n * width), F32),
            vmem((nt, n * depth, 2 * cu), BF16),
            vmem((n, nt, cu, width), BF16),
            vmem((nt, n * depth, 2 * cf), BF16),
            vmem((n, nt, cf, width), BF16),
            vmem((2, n, seq, width), BF16),
            vmem((2, n, seq, width), BF16),
            vmem((per, seq, width), BF16),
            vmem((2 * seq, n * width), BF16),
            vmem((nt, 2 * seq, 2 * cu), F32),
            vmem((2, seq, nt * cu), BF16),
            vmem((nt, 2, seq + 8, 2 * cf), F32),
            vmem((2, seq, nt * cf), BF16),
            vmem((2, seq + 8, 1), F32),
            vmem((2, seq, 128), F32),
            vmem((seq, width), F32),
            vmem((2, n, seq, width), BF16),
            vmem((2, n, seq, width), BF16),
            vmem((n, seq, width), BF16),
            vmem((n, seq, width), BF16),
            vmem((4, per, seq, width), BF16),
            vmem((4, per, seq, width), BF16),
            vmem((nt, groups // share, block_len, block_len), BF16),
            vmem((nt, groups // share, block_len, block_len), BF16),
            vmem((nt, 1, cu), F32),
            vmem((nt, groups, block_len), F32),
            vmem((nt, groups // share, block_len, 1), F32),
            vmem((nt, taps_len, cf), BF16),
            vmem((nt, taps_len, cf), BF16),
            sem((per,)),
            sem((per,)),
            sem((2,)),
            sem((4, 2)),
            sem((4, 2)),
            sem((4, 2)),
            sem((4, n, 2)),
            sem((4, n)),
            sem((4, n)),
            sem((4, n)),
            sem((5,)),
            sem((5,)),
            sem((5,)),
            sem((2, 3, per)),
            sem((2, 2, n)),
            sem((2, n)),
            sem((2, 2, n)),
            sem((2, n)),
            sem((2, 4, per)),
        ],
        compiler_params=pltpu.CompilerParams(
            collective_id=0, has_side_effects=True, vmem_limit_bytes=67043328
        ),
    )(*(array for array, _ in operands))


def by_shape(*arrays):
    n, nr, nt = lax.axis_size("fs"), lax.axis_size("rep"), lax.axis_size("tp")
    groups, units = arrays[5].shape[0], arrays[9].shape[1]
    share = nr * 2
    fits = nr == 2 and nt == 2 and n % 2 == 0 and groups % share == 0 and units % (share * 128) == 0
    return on_plane(*arrays) if fits else on_device(*arrays)


def solution(mesh):
    placed = (
        P(("rep", "fs"), "tp"),
        P(),
        P("fs", "tp"),
        P("fs", "tp"),
        P("tp"),
        P("tp", None, None),
        P("tp", None),
        P("tp", "fs"),
        P(),
        P("fs", "tp"),
        P("fs", "tp"),
        P(None, "tp"),
        P(None, "tp"),
        P("tp", "fs"),
    )
    return jax.shard_map(
        by_shape, mesh=mesh, in_specs=placed, out_specs=P(("rep", "fs"), "tp"), check_vma=False
    )
```

```python
import functools

import jax
import jax.numpy as jnp
from jax import lax
from jax.experimental import pallas as pl
from jax.experimental.pallas import tpu as pltpu
from jax.sharding import PartitionSpec as P

EPS_RMS = 1e-06
EPS_LN = 1e-05
F32 = jnp.float32
BF16 = jnp.bfloat16
MESH = pl.DeviceIdType.MESH
STRAIGHT = (0, 1)


def own_half(array, axis):
    share = array.shape[axis] // lax.axis_size("rep")
    return lax.dynamic_slice_in_dim(array, lax.axis_index("rep") * share, share, axis)


def layer_kernel(
    n, nr, nt,
    tok, mix_gain, w_in, norm_gain, mixw, bias, w_out, ffn_gain, w_up, taps_g, taps_v, w_dn,
    out,
    g_in, g_out, g_up, g_dn, feat, feat2, normed, uv, hidden, gv, act, part1, part2, got1, got2,
    w_send, w_recv, w_local, f_send, f_recv, p_send, p_recv,
):
    rep, fs, tp = lax.axis_index("rep"), lax.axis_index("fs"), lax.axis_index("tp")
    seq, own_width = tok.shape
    nz = n // 2
    z, y = fs // 2, fs % 2
    per = n // nt
    depth = normed.shape[2]
    mine = (w_in, w_out, w_up, w_dn)
    gathered = (g_in, g_out, g_up, g_dn)
    offsets = [(a, b) for a in range(nr) for b in range(nt) if (a, b) != (0, 0)]

    def peer(a, b):
        return {"rep": lax.rem(rep + a, nr), "tp": lax.rem(tp + b, nt)}

    barrier = pltpu.get_barrier_semaphore()
    line = (lax.rem(z + 1, nz), lax.rem(z + nz - 1, nz))
    greeted = [{"fs": z * 2 + 1 - y}] + [{"fs": at * 2 + y} for at in line]
    greeted += [peer(a, b) for a, b in offsets]
    for target in greeted:
        pl.semaphore_signal(barrier, inc=1, device_id=target, device_id_type=MESH)
    pl.semaphore_wait(barrier, len(greeted))

    def hop(stage, block, way):
        target = (fs + 2, fs - 2, z * 2 + 1 - y)[way]
        return pltpu.make_async_remote_copy(
            src_ref=gathered[stage].at[block],
            dst_ref=gathered[stage].at[block],
            send_sem=w_send.at[stage, way, block],
            recv_sem=w_recv.at[stage, block],
            device_id={"fs": target},
            device_id_type=MESH,
        )

    def ways(src):
        return (
            jnp.logical_and(src <= z, z < nz - 1),
            jnp.logical_and(src >= z, z > 0),
        )

    def forward(stage, src):
        block = src * 2 + y
        hop(stage, block, 2).start()
        for way, used in enumerate(ways(src)):
            @pl.when(used)
            def _():
                hop(stage, block, way).start()

    def arrived(stage, block):
        hop(stage, block, 2).wait_recv()

    def order(i):
        near = jnp.minimum(z, nz - 1 - z)
        swing = z + ((i + 1) // 2) * (1 - 2 * (i % 2))
        rest = jnp.where(z < nz - 1 - z, i, nz - 1 - i)
        return jnp.where(i <= 2 * near, swing, rest)

    def stage_loop(stage, compute, begin, middle):
        def step(i, _):
            src = order(i)

            @pl.when(i > 0)
            def _():
                arrived(stage, src * 2 + y)
                forward(stage, src)

            compute(src * 2 + y)

            @pl.when(i > 0)
            def _():
                other = order(i - 1) * 2 + 1 - y
                arrived(stage, other)
                compute(other)

            return 0

        lax.fori_loop(begin, nz, step, 0)
        middle()
        last = order(nz - 1) * 2 + 1 - y
        arrived(stage, last)
        compute(last)

    locals_ = [
        pltpu.make_async_copy(mine[k], gathered[k].at[fs], w_local.at[k]) for k in range(4)
    ]
    own_tok = pltpu.make_async_copy(tok, feat.at[rep, tp], w_local.at[4])
    for copy in locals_ + [own_tok]:
        copy.start()

    def share(turn, slabs):
        copies = []
        for k, (a, b) in enumerate(offsets):
            copies.append(
                pltpu.make_async_remote_copy(
                    src_ref=slabs.at[rep, tp],
                    dst_ref=slabs.at[rep, tp],
                    send_sem=f_send.at[turn, k],
                    recv_sem=f_recv.at[turn, k],
                    device_id=peer(a, b),
                    device_id_type=MESH,
                )
            )
        return copies

    def share_wait(turn, slabs):
        for k, (a, b) in enumerate(offsets):
            slab = slabs.at[lax.rem(rep + nr - a, nr), lax.rem(tp + nt - b, nt)]
            pltpu.make_async_remote_copy(
                src_ref=slab, dst_ref=slab, send_sem=f_send.at[turn, k],
                recv_sem=f_recv.at[turn, k], device_id=peer(a, b), device_id_type=MESH,
            ).wait_recv()

    def norm(slabs, gain):
        for r in range(nr):
            total = jnp.zeros((seq, 1), F32)
            for t in range(nt):
                values = slabs[r, t].astype(F32)
                total += jnp.sum(values * values, axis=1, keepdims=True)
            scale = lax.rsqrt(total / (nt * own_width) + EPS_RMS)
            for t in range(nt):
                for j in range(per):
                    values = slabs[r, t, :, j * depth : (j + 1) * depth].astype(F32)
                    normed[t * per + j, r * seq : (r + 1) * seq, :] = (
                        values * scale * gain[t * per + j]
                    ).astype(BF16)

    def piece(turn, part, got, block, r):
        return pltpu.make_async_remote_copy(
            src_ref=part.at[block, r],
            dst_ref=got.at[rep * nt + tp, block % per],
            send_sem=p_send.at[turn, block, r],
            recv_sem=p_recv.at[turn, rep * nt + tp, block % per],
            device_id={"rep": r, "tp": block // per},
            device_id_type=MESH,
        )

    def abroad(block, r):
        return jnp.logical_or(block // per != tp, r != rep)

    def project(turn, left, gathered_w, part, got, block):
        for r in range(nr):
            part[block, r] = jnp.dot(
                left[r], gathered_w[block], preferred_element_type=F32
            ).astype(BF16)

            @pl.when(abroad(block, r))
            def _():
                piece(turn, part, got, block, r).start()

    def collect(turn, part, got, base, emit):
        for j in range(per):
            total = part[tp * per + j, rep].astype(F32)
            for a, b in offsets:
                slot = lax.rem(rep + a, nr) * nt + lax.rem(tp + b, nt)
                landing = got.at[slot, j]
                pltpu.make_async_remote_copy(
                    src_ref=landing, dst_ref=landing, send_sem=p_send.at[turn, 0, 0],
                    recv_sem=p_recv.at[turn, slot, j], device_id=peer(a, b),
                    device_id_type=MESH,
                ).wait_recv()
                total += got[slot, j].astype(F32)
            width = total.shape[1]
            span = slice(j * width, (j + 1) * width)
            emit(span, (base(span).astype(F32) + total).astype(BF16))

    for copy in locals_ + [own_tok]:
        copy.wait()
    for copy in share(0, feat):
        copy.start()
    forward(0, z)
    forward(1, z)
    forward(2, z)
    uv[...] = jnp.zeros_like(uv)
    gv[...] = jnp.zeros_like(gv)
    share_wait(0, feat)
    norm(feat, mix_gain)

    def in_block(block):
        for r in range(nr):
            rows = slice(r * seq, (r + 1) * seq)
            uv[rows, :] += jnp.dot(
                normed[block, rows, :], g_in[block], preferred_element_type=F32
            )

    stage_loop(0, in_block, 0, lambda: forward(3, z))

    groups, block_len = mixw.shape[0], mixw.shape[1]
    group_width = uv.shape[1] // 2 // groups

    for r in range(nr):
        def mix_rows(i, _):
            start = pl.multiple_of(i * block_len, block_len)
            rows = pl.ds(pl.multiple_of(r * seq + i * block_len, block_len), block_len)
            for g in range(groups):
                at = g * group_width
                half = groups * group_width
                activated = jax.nn.gelu(uv[rows, half + at : half + at + group_width])
                centred = activated - jnp.mean(activated, axis=1, keepdims=True)
                spread = jnp.mean(centred * centred, axis=1, keepdims=True)
                v_norm = (
                    centred * lax.rsqrt(spread + EPS_LN) * norm_gain[:, at : at + group_width]
                ).astype(BF16)
                mixed = jnp.dot(mixw[g], v_norm, preferred_element_type=F32) + bias[g]
                hidden[r, pl.ds(start, block_len), at : at + group_width] = (
                    jax.nn.gelu(uv[rows, at : at + group_width]) * mixed
                ).astype(BF16)
            return 0

        lax.fori_loop(0, seq // block_len, mix_rows, 0)

    stage_loop(
        1, functools.partial(project, 0, hidden, g_out, part1, got1), 0, lambda: None
    )

    def relay(stage, begin, end):
        def step(i, _):
            arrived(stage, order(i) * 2 + y)
            forward(stage, order(i))
            return 0

        lax.fori_loop(begin, end, step, 0)

    def put_middle(span, value):
        feat2[rep, tp, :, span] = value

    relay(2, 1, nz // 2)
    collect(0, part1, got1, lambda span: tok[:, span], put_middle)
    for copy in share(1, feat2):
        copy.start()
    relay(2, nz // 2, nz)
    share_wait(1, feat2)
    norm(feat2, ffn_gain)

    def up_block(block):
        for r in range(nr):
            gv[r, 8:, :] += jnp.dot(
                normed[block, r * seq : (r + 1) * seq, :],
                g_up[block],
                preferred_element_type=F32,
            )

    def up_step(i, _):
        up_block(order(i) * 2 + y)

        @pl.when(i > 0)
        def _():
            arrived(3, order(i) * 2 + y)
            forward(3, order(i))

        other = order(i) * 2 + 1 - y
        arrived(2, other)
        up_block(other)
        return 0

    lax.fori_loop(0, nz, up_step, 0)

    units = act.shape[2]
    taps_len = taps_g.shape[0]
    chunk = 128 if units % 128 == 0 else units
    for r in range(nr):
        for at in range(0, units, chunk):
            gate = jnp.zeros((seq, chunk), F32)
            value = jnp.zeros((seq, chunk), F32)
            for k in range(taps_len):
                first = 8 - (taps_len - 1) + k
                gate += taps_g[k : k + 1, at : at + chunk] * gv[r, first : first + seq, at : at + chunk]
                value += (
                    taps_v[k : k + 1, at : at + chunk]
                    * gv[r, first : first + seq, units + at : units + at + chunk]
                )
            act[r, :, at : at + chunk] = (jax.nn.gelu(gate) * value).astype(BF16)

    down = functools.partial(project, 1, act, g_dn, part2, got2)

    def down_own(i, _):
        down(order(i) * 2 + y)
        return 0

    def down_other(i, _):
        arrived(3, order(i) * 2 + 1 - y)
        down(order(i) * 2 + 1 - y)
        return 0

    lax.fori_loop(0, nz, down_own, 0)
    lax.fori_loop(0, nz, down_other, 0)

    def put_out(span, value):
        out[:, span] = value

    collect(1, part2, got2, lambda span: feat2[rep, tp, :, span], put_out)

    for turn, slabs in enumerate((feat, feat2)):
        for copy in share(turn, slabs):
            copy.wait_send()

    def drain_pieces(block, _):
        for r in range(nr):
            @pl.when(abroad(block, r))
            def _():
                piece(0, part1, got1, block, r).wait_send()
                piece(1, part2, got2, block, r).wait_send()
        return 0

    lax.fori_loop(0, n, drain_pieces, 0)

    def drain_hops(src, _):
        for stage in range(4):
            hop(stage, src * 2 + y, 2).wait_send()
            for way, used in enumerate(ways(src)):
                @pl.when(used)
                def _():
                    hop(stage, src * 2 + y, way).wait_send()
        return 0

    lax.fori_loop(0, nz, drain_hops, 0)


def on_device(
    tokens,
    mix_gain,
    w_u,
    w_v,
    norm_gain,
    mix_weight,
    mix_bias,
    w_mix_out,
    ffn_gain,
    w_gate,
    w_value,
    taps_gate,
    taps_value,
    w_down,
):
    n, nr, nt = lax.axis_size("fs"), lax.axis_size("rep"), lax.axis_size("tp")
    seq, own_width = tokens.shape
    depth, per = own_width * nt // n, n // nt
    block_len = mix_weight.shape[1]
    lower_mask = jnp.arange(block_len)[:, None] >= jnp.arange(block_len)[None, :]
    mixw = own_half(mix_weight, 0)
    mixw = jnp.where(lower_mask[None], mixw, jnp.zeros_like(mixw))
    w_in = jnp.concatenate((own_half(w_u, 1), own_half(w_v, 1)), 1)
    w_up = jnp.concatenate((own_half(w_gate, 1), own_half(w_value, 1)), 1)
    w_out, w_dn = own_half(w_mix_out, 0), own_half(w_down, 0)
    operands = (
        tokens,
        mix_gain.reshape(n, 1, depth),
        w_in,
        own_half(norm_gain, 0)[None, :],
        mixw,
        own_half(mix_bias, 0)[:, :, None],
        w_out,
        ffn_gain.reshape(n, 1, depth),
        w_up,
        own_half(taps_gate, 1).astype(F32),
        own_half(taps_value, 1).astype(F32),
        w_dn,
    )
    vmem, sem = pltpu.VMEM, pltpu.SemaphoreType.DMA
    others = nr * nt - 1
    return pl.pallas_call(
        functools.partial(layer_kernel, n, nr, nt),
        out_shape=jax.ShapeDtypeStruct((seq, own_width), BF16),
        in_specs=[pl.BlockSpec(memory_space=vmem)] * len(operands),
        out_specs=pl.BlockSpec(memory_space=vmem),
        scratch_shapes=[
            vmem((n,) + w_in.shape, BF16),
            vmem((n,) + w_out.shape, BF16),
            vmem((n,) + w_up.shape, BF16),
            vmem((n,) + w_dn.shape, BF16),
            vmem((nr, nt, seq, own_width), BF16),
            vmem((nr, nt, seq, own_width), BF16),
            vmem((n, nr * seq, depth), BF16),
            vmem((nr * seq, w_in.shape[1]), F32),
            vmem((nr, seq, w_out.shape[0]), BF16),
            vmem((nr, seq + 8, w_up.shape[1]), F32),
            vmem((nr, seq, w_dn.shape[0]), BF16),
            vmem((n, nr, seq, depth), BF16),
            vmem((n, nr, seq, depth), BF16),
            vmem((nr * nt, per, seq, depth), BF16),
            vmem((nr * nt, per, seq, depth), BF16),
            sem((4, 3, n)),
            sem((4, n)),
            sem((5,)),
            sem((2, others)),
            sem((2, others)),
            sem((2, n, nr)),
            sem((2, nr * nt, per)),
        ],
        compiler_params=pltpu.CompilerParams(
            collective_id=0, has_side_effects=True, vmem_limit_bytes=67043328
        ),
    )(*operands)


def plane_kernel(
    n, nr, nt,
    tok_hbm, mix_gain_hbm, w_u, w_v, norm_gain, mixw, bias, w_out, ffn_gain_hbm, w_gate, w_value, taps_g, taps_v, w_dn,
    out_hbm,
    tok, out, mix_gain, ffn_gain, g_in, g_out, g_up, g_dn, feat, feat2, mid, normed, uv, hidden, gv, act,
    row_scale, squares, extra, part1, part2, inc1, inc2, got1, got2, raw_mix, mix_low, gain_v, bias_all, bias_col, tg, tv,
    t_sem, o_sem, n_sem, l_sem, y_send, y_recv, z_send, z_recv, d_send, d_recv, s_local, s_send, s_recv,
    a_send, a_recv, f_send, r_send, i_recv, t_recv,
):
    rep, fs, tp = lax.axis_index("rep"), lax.axis_index("fs"), lax.axis_index("tp")
    seq, own_width = tok_hbm.shape
    ny, nz = 2, n // 2
    z, y = fs // ny, fs % ny
    per = n // nt
    width = own_width // per
    quarter = rep * ny + y
    other_quarter = rep * ny + 1 - y
    fs_y = z * ny + 1 - y
    home = rep == tp
    away = rep != tp
    cu, cf = g_out.shape[2], g_dn.shape[2]
    depth = w_u.shape[0]
    few = (max(1, per // 4), max(1, per // 4))
    feats = (feat, feat2)

    def both(*conditions):
        return functools.reduce(jnp.logical_and, conditions)

    barrier = pltpu.get_barrier_semaphore()
    greeted = [{"tp": 1 - tp}]
    greeted += [{"rep": 1 - rep, "tp": t} for t in range(nt)]
    greeted += [{"fs": fs_y, "tp": t} for t in range(nt)]
    greeted += [{"rep": 1 - rep, "fs": fs_y, "tp": t} for t in range(nt)]
    greeted += [{"fs": lax.rem(z + k, nz) * ny + y} for k in range(1, nz)]

    def item(k, block, half):
        if k in (0, 2):
            rows = pl.ds(pl.multiple_of(block * depth, 128), depth)
            return (g_in if k == 0 else g_up).at[half, rows]
        if k == 1:
            return g_out.at[block, half]
        return g_dn.at[block, half]

    def pieces(k, which, block):
        whole = item(k, block, tp)
        if k in (0, 2):
            first, second, size = (w_u, w_v, cu) if k == 0 else (w_gate, w_value, cf)
            cols = pl.ds(pl.multiple_of(which * size, 128), size)
            return (
                (first.at[:, cols], whole.at[:, pl.ds(0, size)]),
                (second.at[:, cols], whole.at[:, pl.ds(size, size)]),
            )
        source, size = (w_out, cu) if k == 1 else (w_dn, cf)
        rows = pl.ds(pl.multiple_of(which * size, 128), size)
        return ((source.at[rows, :], whole),)

    def own_load(k):
        return [
            pltpu.make_async_copy(src, dst, l_sem.at[k, i])
            for i, (src, dst) in enumerate(pieces(k, quarter, fs))
        ]

    def across(k, block):
        return [
            pltpu.make_async_remote_copy(
                src_ref=src, dst_ref=dst, send_sem=y_send.at[k, i], recv_sem=y_recv.at[k, i],
                device_id={"fs": fs_y}, device_id_type=MESH,
            )
            for i, (src, dst) in enumerate(pieces(k, other_quarter, block))
        ]

    def z_copy(k, block, step):
        return pltpu.make_async_remote_copy(
            src_ref=item(k, block, tp), dst_ref=item(k, block, tp),
            send_sem=z_send.at[k, block, (step + 1) // 2], recv_sem=z_recv.at[k, block],
            device_id={"fs": fs + ny * step}, device_id_type=MESH,
        )

    def d_copy(k, block):
        return pltpu.make_async_remote_copy(
            src_ref=item(k, block, tp), dst_ref=item(k, block, tp),
            send_sem=d_send.at[k, block], recv_sem=d_recv.at[k, block],
            device_id={"tp": 1 - tp}, device_id_type=MESH,
        )

    def inside(step):
        return jnp.logical_and(z + step >= 0, z + step < nz)

    def spread(k, block):
        for step in (1, -1):
            @pl.when(inside(step))
            def _():
                z_copy(k, block, step).start()
        d_copy(k, block).start()

    def arrive(k, block):
        landing = item(k, block, tp)
        pltpu.make_async_remote_copy(
            src_ref=landing, dst_ref=landing, send_sem=z_send.at[k, block, 0],
            recv_sem=z_recv.at[k, block], device_id={"tp": 1 - tp}, device_id_type=MESH,
        ).wait_recv()
        d_copy(k, block).start()

    def cross_over(k):
        for copy in across(k, fs_y):
            copy.wait_recv()
        spread(k, fs_y)

    def relays(far):
        return [
            (sign, z - sign * far, jnp.logical_and(inside(sign), inside(-sign * far)))
            for sign in (1, -1)
        ]

    def relay(k, far, at):
        for sign, source, used in relays(far):
            @pl.when(used)
            def _():
                arrive(k, source * ny + at)
                z_copy(k, source * ny + at, sign).start()

    def relay_from(k, first, last):
        for far in range(first, last):
            for at in range(ny):
                relay(k, far, at)

    def relayed(source):
        up = jnp.logical_and(z > source, inside(1))
        down = jnp.logical_and(source > z, inside(-1))
        return jnp.logical_or(up, down)

    def need(k, block):
        source = block // ny
        @pl.when(jnp.logical_and(source != z, jnp.logical_not(relayed(source))))
        def _():
            arrive(k, block)

    def partner_wait(k, block):
        landing = item(k, block, 1 - tp)
        pltpu.make_async_remote_copy(
            src_ref=landing, dst_ref=landing, send_sem=d_send.at[k, block],
            recv_sem=d_recv.at[k, block], device_id={"tp": 1 - tp}, device_id_type=MESH,
        ).wait_recv()

    def order(i):
        near = jnp.minimum(z, nz - 1 - z)
        swing = z + ((i + 1) // 2) * (1 - 2 * (i % 2))
        rest = jnp.where(z < nz - 1 - z, i, nz - 1 - i)
        return jnp.where(i <= 2 * near, swing, rest)

    def plain_block(i):
        return order(i // ny) * ny + lax.rem(i, ny)

    small = [
        (mixw.at[pl.ds(quarter * raw_mix.shape[1], raw_mix.shape[1])], raw_mix.at[tp]),
        (norm_gain.at[:, pl.ds(pl.multiple_of(quarter * cu, 128), cu)], gain_v.at[tp]),
        (bias, bias_all.at[tp]),
        (taps_g.at[:, pl.ds(pl.multiple_of(quarter * cf, 128), cf)], tg.at[tp]),
        (taps_v.at[:, pl.ds(pl.multiple_of(quarter * cf, 128), cf)], tv.at[tp]),
    ]
    small_local = [
        pltpu.make_async_copy(src, dst, s_local.at[i]) for i, (src, dst) in enumerate(small)
    ]
    small_away = [
        pltpu.make_async_remote_copy(
            src_ref=src, dst_ref=dst, send_sem=s_send.at[i], recv_sem=s_recv.at[i],
            device_id={"tp": 1 - tp}, device_id_type=MESH,
        )
        for i, (src, dst) in enumerate(small)
    ]

    def columns(i):
        return pl.ds(pl.multiple_of(i * width, 128), width)

    def tok_load(i):
        return pltpu.make_async_copy(tok_hbm.at[:, columns(i)], tok.at[i], t_sem.at[i])

    def out_store(i):
        return pltpu.make_async_copy(out.at[i], out_hbm.at[:, columns(i)], o_sem.at[i])

    def ag_source(turn, i):
        return (tok, mid)[turn].at[i]

    def ag_copy(turn, i, way):
        block = tp * per + i
        device = ({"rep": 1 - rep, "tp": rep}, {"fs": fs_y, "tp": rep}, {"tp": 1 - tp})[way]
        return pltpu.make_async_remote_copy(
            src_ref=ag_source(turn, i), dst_ref=feats[turn].at[y, block],
            send_sem=a_send.at[turn, way, i], recv_sem=a_recv.at[turn, y, block],
            device_id=device, device_id_type=MESH,
        )

    def ag_send(turn, i):
        ag_copy(turn, i, 0).start()
        ag_copy(turn, i, 1).start()

        @pl.when(away)
        def _():
            ag_copy(turn, i, 2).start()

        @pl.when(home)
        def _():
            feats[turn][y, tp * per + i] = ag_source(turn, i)[...]

    def passed(turn, block):
        at = lax.rem(block, per)
        return jnp.logical_or(
            jnp.logical_and(home, at >= few[turn]), jnp.logical_and(away, at < few[turn])
        )

    def ag_pass(turn, block):
        slot = jnp.where(home, 1 - y, y)
        return pltpu.make_async_remote_copy(
            src_ref=feats[turn].at[slot, block], dst_ref=feats[turn].at[slot, block],
            send_sem=f_send.at[turn, block], recv_sem=a_recv.at[turn, slot, block],
            device_id={
                "rep": jnp.where(home, 1 - rep, rep),
                "fs": jnp.where(home, fs, fs_y),
            },
            device_id_type=MESH,
        )

    def ag_landed(turn, slot, block):
        landing = feats[turn].at[slot, block]
        pltpu.make_async_remote_copy(
            src_ref=landing, dst_ref=landing, send_sem=f_send.at[turn, 0],
            recv_sem=a_recv.at[turn, slot, block], device_id={"tp": 1 - tp}, device_id_type=MESH,
        ).wait_recv()

    def ag_forward(turn, block):
        @pl.when(passed(turn, block))
        def _():
            ag_landed(turn, jnp.where(home, 1 - y, y), block)
            ag_pass(turn, block).start()

    def ag_wait(turn, slot, block):
        local = both(home, slot == y, block // per == tp)
        sent_on = jnp.logical_and(passed(turn, block), slot == jnp.where(home, 1 - y, y))

        @pl.when(jnp.logical_not(jnp.logical_or(local, sent_on)))
        def _():
            ag_landed(turn, slot, block)

    def weigh(turn, gain, block):
        gains = gain[:, pl.ds(pl.multiple_of(block * width, 128), width)]
        for r in range(2):
            slot = lax.rem(y + r, 2)
            ag_wait(turn, slot, block)
            values = feats[turn][slot, block].astype(F32)
            rows = pl.ds(pl.multiple_of(slot * seq, 8), seq)
            normed[rows, pl.ds(pl.multiple_of(block * width, 128), width)] = (
                values * gains
            ).astype(BF16)
            for at in range(0, width, 128):
                piece = values[:, at : at + 128]
                squares[slot] += piece * piece

    def finish_scale():
        for slot in range(2):
            total = jnp.sum(squares[slot], axis=1, keepdims=True)
            row_scale[slot, 8:, :] = lax.rsqrt(total / (n * width) + EPS_RMS)

    def gathered_loop(k, turn, gain, multiply, lead, beside):
        def arrived(source, half):
            if half is tp:
                for at in range(ny):
                    weigh(turn, gain, source * ny + at)
                for at in (y, 1 - y):
                    need(k, source * ny + at)
            else:
                for at in (y, 1 - y):
                    partner_wait(k, source * ny + at)
            cols = pl.ds(pl.multiple_of(source * ny * depth, 128), ny * depth)
            multiply(cols, half)

        def step(i, _):
            if lead:
                @pl.when(i < nz)
                def _():
                    for at in range(ny):
                        ag_forward(turn, order(i) * ny + at)

            for at, action in beside:
                pl.when(i == at)(action)

            @pl.when(both(i >= lead, i < nz + lead))
            def _():
                arrived(order(i - lead), tp)

            @pl.when(i >= lead + 1)
            def _():
                arrived(order(i - lead - 1), 1 - tp)

            return 0

        lax.fori_loop(0, nz + lead + 1, step, 0)
        finish_scale()

    def even(block):
        return lax.rem(block, 2) == 0

    parts, incs, gots = (part1, part2), (inc1, inc2), (got1, got2)

    def r_copy(turn, r, block, kind):
        slot = lax.rem(y + r, 2)
        core, at = block // per, lax.rem(block, per)
        got, inc = gots[turn], incs[turn]
        dst, sem, device = {
            "diag_x": (inc.at[block], i_recv.at[turn, block], {"rep": 1 - rep}),
            "diag_y": (inc.at[block], i_recv.at[turn, block], {"fs": fs_y}),
            "pair": (got.at[0, at], t_recv.at[turn, 0, at], {"tp": 1 - tp}),
            "x": (got.at[1, at], t_recv.at[turn, 1, at], {"rep": 1 - rep, "tp": core}),
            "y": (got.at[2, at], t_recv.at[turn, 2, at], {"fs": fs_y, "tp": core}),
            "diag": (
                got.at[3, at], t_recv.at[turn, 3, at],
                {"rep": 1 - rep, "fs": fs_y, "tp": core},
            ),
        }[kind]
        return pltpu.make_async_remote_copy(
            src_ref=parts[turn].at[slot, block], dst_ref=dst, send_sem=r_send.at[turn, r, block],
            recv_sem=sem, device_id=device, device_id_type=MESH,
        )

    def straight(turn, block):
        hit = block == plain_block(n - 1)
        for i in range(n - STRAIGHT[turn], n - 1):
            hit = jnp.logical_or(hit, block == plain_block(i))
        return hit if STRAIGHT[turn] else block < 0

    def cases(turn, block):
        once = straight(turn, block)
        twice = jnp.logical_not(once)
        is_even = even(block)
        is_odd = jnp.logical_not(is_even)
        return (
            (1, "diag_x", both(away, twice, is_even), True),
            (1, "diag_y", both(away, twice, is_odd), True),
            (1, "diag", both(away, once), True),
            (1, "y", both(home, jnp.logical_or(once, is_odd)), True),
            (0, "pair", both(home, block // per != tp), True),
            (0, "x", both(away, jnp.logical_or(once, is_even)), True),
            (1, "y", both(home, twice, is_even), False),
            (0, "x", both(away, twice, is_odd), False),
        )

    def project(turn, left, weight, block, r):
        size = weight.shape[1] * weight.shape[2]
        right = weight[block].reshape(size, weight.shape[3])
        slot = lax.rem(y + r, 2)
        parts[turn][slot, block] = jnp.dot(
            left[slot], right, preferred_element_type=F32
        ).astype(BF16)
        for row, kind, used, now in cases(turn, block):
            if row == r and now:
                @pl.when(used)
                def _():
                    r_copy(turn, r, block, kind).start()

        if r == 0:
            @pl.when(both(home, block // per == tp))
            def _():
                gots[turn][0, lax.rem(block, per)] = parts[turn][y, block]

    def scatter_early(k, turn, left, weight, count):
        for i in range(count):
            need(k, plain_block(i))
        for i in range(count):
            partner_wait(k, plain_block(i))
            project(turn, left, weight, plain_block(i), 1)

    def join(turn, block):
        for r, kind, used, now in cases(turn, block):
            if not now:
                @pl.when(used)
                def _():
                    landing = incs[turn].at[block]
                    pltpu.make_async_remote_copy(
                        src_ref=landing, dst_ref=landing, send_sem=r_send.at[turn, 0, 0],
                        recv_sem=i_recv.at[turn, block], device_id={"rep": 1 - rep},
                        device_id_type=MESH,
                    ).wait_recv()
                    slot = lax.rem(y + r, 2)
                    parts[turn][slot, block] = (
                        parts[turn][slot, block].astype(F32) + incs[turn][block].astype(F32)
                    ).astype(BF16)
                    r_copy(turn, r, block, kind).start()

    def landed(turn, kind, at):
        landing = gots[turn].at[kind, at]
        pltpu.make_async_remote_copy(
            src_ref=landing, dst_ref=landing, send_sem=r_send.at[turn, 0, 0],
            recv_sem=t_recv.at[turn, kind, at], device_id={"rep": 1 - rep}, device_id_type=MESH,
        ).wait_recv()

    def collect(turn, block):
        at = lax.rem(block, per)

        @pl.when(away)
        def _():
            landed(turn, 0, at)

        landed(turn, 1, at)
        landed(turn, 2, at)
        got = gots[turn]
        total = got[0, at].astype(F32) + got[1, at].astype(F32) + got[2, at].astype(F32)
        if STRAIGHT[turn]:
            once = straight(turn, block)

            @pl.when(once)
            def _():
                landed(turn, 3, at)
                extra[...] = got[3, at].astype(F32)

            @pl.when(jnp.logical_not(once))
            def _():
                extra[...] = jnp.zeros_like(extra)

            total += extra[...]
        if turn == 0:
            mid[at] = (tok[at].astype(F32) + total).astype(BF16)
            ag_send(1, at)
        else:
            out[at] = (mid[at].astype(F32) + total).astype(BF16)
            out_store(at).start()

    def scatter_loop(k, turn, left, weight, early, lags, beside):
        join_lag, collect_lag = lags

        def step(i, _):
            @pl.when(both(i >= early, i < n))
            def _():
                need(k, plain_block(i))

            @pl.when(both(i >= join_lag, i < n + join_lag))
            def _():
                join(turn, plain_block(i - join_lag))

            @pl.when(i < n)
            def _():
                block = plain_block(i)

                @pl.when(i >= early)
                def _():
                    partner_wait(k, block)
                    project(turn, left, weight, block, 1)

                project(turn, left, weight, block, 0)

            for at, action in beside:
                pl.when(i == at)(action)

            @pl.when(i >= collect_lag)
            def _():
                block = plain_block(i - collect_lag)

                @pl.when(block // per == tp)
                def _():
                    collect(turn, block)

            return 0

        lax.fori_loop(0, n + collect_lag, step, 0)

    gain_loads = [
        pltpu.make_async_copy(mix_gain_hbm, mix_gain, n_sem.at[0]),
        pltpu.make_async_copy(ffn_gain_hbm, ffn_gain, n_sem.at[1]),
    ]
    for i in range(per):
        tok_load(i).start()
    for k in range(4):
        for copy in own_load(k):
            copy.start()
    for copy in small_local + gain_loads:
        copy.start()
    for target in greeted:
        pl.semaphore_signal(barrier, inc=1, device_id=target, device_id_type=MESH)
    pl.semaphore_wait(barrier, len(greeted))

    for copy in across(0, fs):
        copy.start()
    for i in range(per):
        tok_load(i).wait()
        ag_send(0, i)
    for k in range(2):
        for copy in own_load(k):
            copy.wait()
        spread(k, fs)
    for copy in across(1, fs) + small_away:
        copy.start()
    uv[...] = jnp.zeros_like(uv)
    gv[...] = jnp.zeros_like(gv)
    squares[...] = jnp.zeros_like(squares)
    row_scale[...] = jnp.zeros_like(row_scale)
    cross_over(0)
    for k in range(2, 4):
        for copy in own_load(k):
            copy.wait()
    for copy in gain_loads:
        copy.wait()
    turns = [(far, at) for far in range(1, nz - 1) for at in (y, 1 - y)]
    for i in range(max(per, len(turns))):
        if i < len(turns):
            relay(0, *turns[i])
        if i < per:
            for half in range(nt):
                ag_forward(0, half * per + i)
    cross_over(1)
    for k in (2, 3):
        for copy in across(k, fs):
            copy.start()

    def in_block(cols, half):
        uv[half] += jnp.dot(normed[:, cols], g_in[half, cols], preferred_element_type=F32)

    hops = ((nz // 2, lambda: relay(1, 1, 0)), (nz // 2 + 1, lambda: relay(1, 1, 1)))
    gathered_loop(0, 0, mix_gain, in_block, 0, hops)

    for copy in small_local:
        copy.wait()
    for i, (_, dst) in enumerate(small):
        landing = (raw_mix, gain_v, bias_all, tg, tv)[i].at[1 - tp]
        pltpu.make_async_remote_copy(
            src_ref=landing, dst_ref=landing, send_sem=s_send.at[i], recv_sem=s_recv.at[i],
            device_id={"tp": 1 - tp}, device_id_type=MESH,
        ).wait_recv()
    per_half, block_len = raw_mix.shape[1], raw_mix.shape[2]
    group_width = cu // per_half
    at_row = lax.broadcasted_iota(jnp.int32, (block_len, block_len), 0)
    at_col = lax.broadcasted_iota(jnp.int32, (block_len, block_len), 1)
    for half in range(nt):
        turned = bias_all[half].T
        lane = lax.broadcasted_iota(jnp.int32, turned.shape, 1)
        for g in range(per_half):
            mix_low[half, g] = jnp.where(
                at_row >= at_col, raw_mix[half, g].astype(F32), 0.0
            ).astype(BF16)
            bias_col[half, g] = jnp.sum(
                jnp.where(lane == quarter * per_half + g, turned, 0.0), axis=1, keepdims=True
            )

    for slot in range(2):
        def mix_rows(i, _):
            own_rows = pl.ds(pl.multiple_of(i * block_len, block_len), block_len)
            rows = pl.ds(pl.multiple_of(slot * seq + i * block_len, block_len), block_len)
            scale = row_scale[slot, pl.ds(pl.multiple_of(i * block_len + 8, 8), block_len), :]
            for half in range(nt):
                for g in range(per_half):
                    at = g * group_width
                    activated = jax.nn.gelu(
                        uv[half, rows, cu + at : cu + at + group_width] * scale
                    )
                    centred = activated - jnp.mean(activated, axis=1, keepdims=True)
                    spread_sq = jnp.mean(centred * centred, axis=1, keepdims=True)
                    v_norm = (
                        centred
                        * lax.rsqrt(spread_sq + EPS_LN)
                        * gain_v[half, :, at : at + group_width]
                    ).astype(BF16)
                    mixed = (
                        jnp.dot(mix_low[half, g], v_norm, preferred_element_type=F32)
                        + bias_col[half, g]
                    )
                    hidden[slot, own_rows, half * cu + at : half * cu + at + group_width] = (
                        jax.nn.gelu(uv[half, rows, at : at + group_width] * scale) * mixed
                    ).astype(BF16)
            return 0

        lax.fori_loop(0, seq // block_len, mix_rows, 0)

    def start_both(k):
        @pl.when(y == 0)
        def _():
            spread(k, fs)
            cross_over(k)

        @pl.when(y == 1)
        def _():
            cross_over(k)
            spread(k, fs)

    relay_from(1, 2, nz - 1)
    start_both(2)
    squares[...] = jnp.zeros_like(squares)

    hops = (
        (n // 2 + 2, lambda: relay(2, 1, 0)),
        (n, lambda: relay(2, 1, 1)),
        (n + 4, lambda: relay_from(2, 2, nz - 1)),
        (n + 5, lambda: start_both(3)),
    )
    scatter_loop(1, 0, hidden, g_out, 0, (3, 6), hops)

    def up_block(cols, half):
        product = jnp.dot(normed[:, cols], g_up[half, cols], preferred_element_type=F32)
        for slot in range(2):
            gv[half, slot, 8:, :] += product[slot * seq : (slot + 1) * seq]

    gathered_loop(2, 1, ffn_gain, up_block, 1, ((nz - 1, lambda: relay_from(3, 1, 2)),))

    taps_len = tg.shape[1]
    chunk = 128

    def convolve(slot):
        for half in range(nt):
            for at in range(0, cf, chunk):
                gate = jnp.zeros((seq, chunk), F32)
                value = jnp.zeros((seq, chunk), F32)
                for k in range(taps_len):
                    first = 8 - (taps_len - 1) + k
                    rows = slice(first, first + seq)
                    scale = row_scale[slot, rows, :]
                    gate += tg[half, k : k + 1, at : at + chunk].astype(F32) * (
                        gv[half, slot, rows, at : at + chunk] * scale
                    )
                    value += tv[half, k : k + 1, at : at + chunk].astype(F32) * (
                        gv[half, slot, rows, cf + at : cf + at + chunk] * scale
                    )
                act[slot, :, half * cf + at : half * cf + at + chunk] = (
                    jax.nn.gelu(gate) * value
                ).astype(BF16)

    convolve(1 - y)
    scatter_early(3, 1, act, g_dn, ny)
    convolve(y)
    relay_from(3, 2, nz - 1)
    scatter_loop(3, 1, act, g_dn, ny, (2, 4), ())

    for i in range(per):
        out_store(i).wait()
    for k in range(4):
        for copy in across(k, fs):
            copy.wait_send()
    for copy in small_away:
        copy.wait_send()

    def drain_block(block, _):
        for k in range(4):
            d_copy(k, block).wait_send()
        for turn in range(2):
            for r, kind, used, _now in cases(turn, block):
                @pl.when(used)
                def _():
                    r_copy(turn, r, block, kind).wait_send()

            @pl.when(passed(turn, block))
            def _():
                ag_pass(turn, block).wait_send()
        return 0

    lax.fori_loop(0, n, drain_block, 0)

    def drain_gather(i, _):
        for turn in range(2):
            ag_copy(turn, i, 0).wait_send()
            ag_copy(turn, i, 1).wait_send()

            @pl.when(away)
            def _():
                ag_copy(turn, i, 2).wait_send()
        return 0

    lax.fori_loop(0, per, drain_gather, 0)

    def drain_line(at, _):
        for k in range(4):
            for step in (1, -1):
                @pl.when(inside(step))
                def _():
                    z_copy(k, z * ny + at, step).wait_send()
            for far in range(1, nz - 1):
                for sign, source, used in relays(far):
                    @pl.when(used)
                    def _():
                        z_copy(k, source * ny + at, sign).wait_send()
        return 0

    lax.fori_loop(0, ny, drain_line, 0)


def on_plane(
    tokens,
    mix_gain,
    w_u,
    w_v,
    norm_gain,
    mix_weight,
    mix_bias,
    w_mix_out,
    ffn_gain,
    w_gate,
    w_value,
    taps_gate,
    taps_value,
    w_down,
):
    n, nr, nt = lax.axis_size("fs"), lax.axis_size("rep"), lax.axis_size("tp")
    seq, own_width = tokens.shape
    per = n // nt
    width = own_width // per
    depth = w_u.shape[0]
    share = nr * 2
    cu, cf = w_u.shape[1] // share, w_gate.shape[1] // share
    groups, block_len = mix_weight.shape[0], mix_weight.shape[1]
    taps_len = taps_gate.shape[0]
    vmem, sem, hbm = pltpu.VMEM, pltpu.SemaphoreType.DMA, pl.ANY
    operands = (
        (tokens, hbm),
        (mix_gain[None, :], hbm),
        (w_u, hbm),
        (w_v, hbm),
        (norm_gain[None, :], hbm),
        (mix_weight, hbm),
        (mix_bias, hbm),
        (w_mix_out, hbm),
        (ffn_gain[None, :], hbm),
        (w_gate, hbm),
        (w_value, hbm),
        (taps_gate, hbm),
        (taps_value, hbm),
        (w_down, hbm),
    )
    return pl.pallas_call(
        functools.partial(plane_kernel, n, nr, nt),
        out_shape=jax.ShapeDtypeStruct((seq, own_width), BF16),
        in_specs=[pl.BlockSpec(memory_space=space) for _, space in operands],
        out_specs=pl.BlockSpec(memory_space=hbm),
        scratch_shapes=[
            vmem((per, seq, width), BF16),
            vmem((per, seq, width), BF16),
            vmem((1, n * width), F32),
            vmem((1, n * width), F32),
            vmem((nt, n * depth, 2 * cu), BF16),
            vmem((n, nt, cu, width), BF16),
            vmem((nt, n * depth, 2 * cf), BF16),
            vmem((n, nt, cf, width), BF16),
            vmem((2, n, seq, width), BF16),
            vmem((2, n, seq, width), BF16),
            vmem((per, seq, width), BF16),
            vmem((2 * seq, n * width), BF16),
            vmem((nt, 2 * seq, 2 * cu), F32),
            vmem((2, seq, nt * cu), BF16),
            vmem((nt, 2, seq + 8, 2 * cf), F32),
            vmem((2, seq, nt * cf), BF16),
            vmem((2, seq + 8, 1), F32),
            vmem((2, seq, 128), F32),
            vmem((seq, width), F32),
            vmem((2, n, seq, width), BF16),
            vmem((2, n, seq, width), BF16),
            vmem((n, seq, width), BF16),
            vmem((n, seq, width), BF16),
            vmem((4, per, seq, width), BF16),
            vmem((4, per, seq, width), BF16),
            vmem((nt, groups // share, block_len, block_len), BF16),
            vmem((nt, groups // share, block_len, block_len), BF16),
            vmem((nt, 1, cu), F32),
            vmem((nt, groups, block_len), F32),
            vmem((nt, groups // share, block_len, 1), F32),
            vmem((nt, taps_len, cf), BF16),
            vmem((nt, taps_len, cf), BF16),
            sem((per,)),
            sem((per,)),
            sem((2,)),
            sem((4, 2)),
            sem((4, 2)),
            sem((4, 2)),
            sem((4, n, 2)),
            sem((4, n)),
            sem((4, n)),
            sem((4, n)),
            sem((5,)),
            sem((5,)),
            sem((5,)),
            sem((2, 3, per)),
            sem((2, 2, n)),
            sem((2, n)),
            sem((2, 2, n)),
            sem((2, n)),
            sem((2, 4, per)),
        ],
        compiler_params=pltpu.CompilerParams(
            collective_id=0, has_side_effects=True, vmem_limit_bytes=67043328
        ),
    )(*(array for array, _ in operands))


def by_shape(*arrays):
    n, nr, nt = lax.axis_size("fs"), lax.axis_size("rep"), lax.axis_size("tp")
    groups, units = arrays[5].shape[0], arrays[9].shape[1]
    share = nr * 2
    fits = nr == 2 and nt == 2 and n % 2 == 0 and groups % share == 0 and units % (share * 128) == 0
    return on_plane(*arrays) if fits else on_device(*arrays)


def solution(mesh):
    placed = (
        P(("rep", "fs"), "tp"),
        P(),
        P("fs", "tp"),
        P("fs", "tp"),
        P("tp"),
        P("tp", None, None),
        P("tp", None),
        P("tp", "fs"),
        P(),
        P("fs", "tp"),
        P("fs", "tp"),
        P(None, "tp"),
        P(None, "tp"),
        P("tp", "fs"),
    )
    return jax.shard_map(
        by_shape, mesh=mesh, in_specs=placed, out_specs=P(("rep", "fs"), "tp"), check_vma=False
    )
```
